128 devices in a mesh: sp: 16 (over z, y), dp: 8 (over x, core).
Axes of the slice: x: 4, y: 4, z: 4, core: 2. Of those that a mesh axis runs over, the one named last changes fastest.
Arguments:
- tokens: bfloat16 [8, 4096, 2048], P('dp', 'sp'), may hold values from -6 to 6
- in_gain: float32 [2048], replicated, may hold values from 0.1 to 1.9
- w_query_down: bfloat16 [2048, 512], P('dp'), may hold values from -0.125 to 0.125
- w_latent_down: bfloat16 [2048, 256], P('dp'), may hold values from -0.125 to 0.125
- w_rope_key: bfloat16 [2048, 64], replicated, may hold values from -0.125 to 0.125
- query_latent_gain: float32 [512], replicated, may hold values from 0.1 to 1.9
- latent_gain: float32 [256], replicated, may hold values from 0.1 to 1.9
- w_query_up: bfloat16 [512, 3072], P('dp', 'sp'), may hold values from -0.25 to 0.25
- w_key_up: bfloat16 [256, 2048], P('dp', 'sp'), may hold values from -0.375 to 0.375
- w_value_up: bfloat16 [256, 2048], P('dp', 'sp'), may hold values from -0.375 to 0.375
- query_gain: float32 [192], replicated, may hold values from 0.5 to 14
- key_gain: float32 [192], replicated, may hold values from 0.5 to 14
- out_gain: float32 [2048], replicated, may hold values from 0.1 to 1.9
- w_out: bfloat16 [2048, 2048], P(('sp', 'dp')), may hold values from -0.125 to 0.125
Outputs:
- result: bfloat16 [8, 4096, 2048], P('dp', 'sp')
The draws below stay inside these ranges and needn't reach their ends.
All inputs are finite; a program needn't handle non-finite values.
Results may differ from the reference program's by a relative error of at most 0.034.
The reference program's roundings to bfloat16 on the way count: a program that leaves them out, or rounds other values in their place, can miss the bound.
Values may be sent and summed in bfloat16 or wider, within the bound.
A program may use at most 64 MiB of HBM per device.

```python
import jax
import jax.numpy as jnp
from jax import lax

D = 2048
HEADS = 16
NOPE = 128
ROPE = 64
VD = 128
QR = 512
KR = 256
QK = 192
LEN = 4096
SEQS = 8


def gain_vector(key, member):
    spread = jnp.clip(jax.random.normal(jax.random.fold_in(key, 11 + member), (QK,), jnp.float32), -2.5, 2.5)
    return (1.0 + 0.18 * spread).astype(jnp.float32)


def draw_query_gain(key, part):
    return gain_vector(key, 0)


def draw_key_gain(key, part):
    return gain_vector(key, 1)


def block_levels(own_key, shape, split, least, largest):
    gain, own = 1.0, jax.random.fold_in(own_key, 6)
    for dim, parts in split:
        draws = jnp.exp(jax.random.uniform(jax.random.fold_in(own, dim), (parts,), jnp.float32, least / len(split), largest / len(split)))
        gain = gain * jnp.repeat(draws, shape[dim] // parts).reshape([-1 if axis == dim else 1 for axis in range(len(shape))])
    return gain


def centred(stream_key, shape, scale, limit, split=(), kind=jnp.bfloat16):
    values = jax.random.normal(stream_key, shape, jnp.float32) * scale
    if len(split) > 0:
        values = block_levels(stream_key, shape, split, -0.22, 0.18) * values
    return jnp.clip(values, min=-limit, max=limit).astype(kind)


def setup_inputs(seed: int = 0) -> dict:
    arg_keys = jax.random.split(jax.random.key(seed), 15)
    tokens = centred(arg_keys[0], (SEQS, LEN, D), 1.0, 6.0, ((0, 8), (1, 16)))
    in_gain = jnp.clip(1.0 + 0.18 * jax.random.normal(arg_keys[1], (D,), jnp.float32), 0.1, 1.9)
    w_query_down = centred(arg_keys[2], (D, QR), D ** -0.5, 0.125, ((0, 8),))
    w_latent_down = centred(arg_keys[3], (D, KR), D ** -0.5, 0.125, ((0, 8),))
    w_rope_key = centred(arg_keys[4], (D, ROPE), D ** -0.5, 0.125)
    query_latent_gain = jnp.clip(1.0 + 0.18 * jax.random.normal(arg_keys[5], (QR,), jnp.float32), 0.1, 1.9)
    latent_gain = jnp.clip(1.0 + 0.18 * jax.random.normal(arg_keys[6], (KR,), jnp.float32), 0.1, 1.9)
    w_query_up = centred(arg_keys[7], (QR, HEADS * QK), QR ** -0.5, 0.25, ((0, 8), (1, 16)))
    w_key_up = centred(arg_keys[8], (KR, HEADS * NOPE), KR ** -0.5, 0.375, ((0, 8), (1, 16)))
    w_value_up = centred(arg_keys[9], (KR, HEADS * VD), KR ** -0.5, 0.375, ((0, 8), (1, 16)))
    query_gain = draw_query_gain(jax.random.fold_in(arg_keys[14], 71), 0)
    key_gain = draw_key_gain(jax.random.fold_in(arg_keys[14], 71), 0)
    out_gain = jnp.clip(1.0 + 0.18 * jax.random.normal(arg_keys[12], (HEADS * VD,), jnp.float32), 0.1, 1.9)
    w_out = centred(arg_keys[13], (HEADS * VD, D), (HEADS * VD) ** -0.5, 0.125, ((0, 128),))
    return dict(tokens=tokens, in_gain=in_gain, w_query_down=w_query_down, w_latent_down=w_latent_down, w_rope_key=w_rope_key, query_latent_gain=query_latent_gain, latent_gain=latent_gain, w_query_up=w_query_up, w_key_up=w_key_up, w_value_up=w_value_up, query_gain=query_gain, key_gain=key_gain, out_gain=out_gain, w_out=w_out)


EPS = 1e-06
THETA = 10000.0
NEG_BIG = -1e+30

def rms_scale(values, scaling):
    return values * lax.rsqrt(lax.optimization_barrier(jnp.mean(values * values, axis=-1, keepdims=True)) + EPS) * scaling

def rotate(tail_part, positions):
    half_width = tail_part.shape[-1] // 2
    frequency = THETA ** (-jnp.arange(half_width, dtype=jnp.float32) / half_width)
    angles = positions[:, None] * frequency[None, :]
    cosine = jnp.cos(angles)[:, None, :]
    sine = jnp.sin(angles)[:, None, :]
    first_half = tail_part[..., :half_width]
    second_half = tail_part[..., half_width:]
    return jnp.concatenate([first_half * cosine - second_half * sine, second_half * cosine + first_half * sine], axis=-1)

def finish_heads(joined, positions, scaling, rope_width):
    row_count = joined.shape[0]
    normal = rms_scale(joined, scaling)
    turned = rotate(normal[..., -rope_width:], positions)
    return jnp.concatenate([normal[..., :-rope_width], turned], axis=-1).astype(jnp.bfloat16).reshape(row_count, -1)

def attend(queries, keys, values, head_count):
    length = queries.shape[0]
    block_rows = min(512, length)
    query_blocks = queries.reshape(length // block_rows, block_rows, head_count, -1)
    key_heads = keys.reshape(length, head_count, -1).astype(jnp.float32)
    value_heads = values.reshape(length, head_count, -1).astype(jnp.float32)
    score_scale = key_heads.shape[-1] ** (-0.5)
    key_pos = jnp.arange(length)

    def one_block(block_args):
        query_block, block_index = block_args
        scores = jnp.einsum('qhd,khd->hqk', query_block.astype(jnp.float32), key_heads) * score_scale
        query_pos = block_index * block_rows + jnp.arange(block_rows)
        allowed = key_pos[None, :] <= query_pos[:, None]
        scores = jnp.where(allowed[None], scores, NEG_BIG)
        weights = jax.nn.softmax(scores, axis=-1).astype(jnp.bfloat16)
        return jnp.einsum('hqk,khd->qhd', weights.astype(jnp.float32), value_heads).astype(jnp.bfloat16)
    outcome = lax.map(one_block, (query_blocks, jnp.arange(length // block_rows)))
    return outcome.reshape(length, -1)

def reference(tokens, in_gain, w_query_down, w_latent_down, w_rope_key, query_latent_gain, latent_gain, w_query_up, w_key_up, w_value_up, query_gain, key_gain, out_gain, w_out):

    def one_sequence(sequence):
        normed = rms_scale(sequence.astype(jnp.float32), in_gain).astype(jnp.bfloat16)
        latent_q = rms_scale(jnp.dot(normed, w_query_down, preferred_element_type=jnp.float32), query_latent_gain).astype(jnp.bfloat16)
        latent_kv = rms_scale(jnp.dot(normed, w_latent_down, preferred_element_type=jnp.float32), latent_gain).astype(jnp.bfloat16)
        rope_key = jnp.dot(normed, w_rope_key, preferred_element_type=jnp.float32).astype(jnp.bfloat16)
        positions = jnp.arange(LEN, dtype=jnp.float32)
        query_total = jnp.dot(latent_q, w_query_up, preferred_element_type=jnp.float32)
        queries = finish_heads(query_total.reshape(LEN, HEADS, QK), positions, query_gain, ROPE)
        key_total = jnp.dot(latent_kv, w_key_up, preferred_element_type=jnp.float32).reshape(LEN, HEADS, NOPE)
        shared = jnp.broadcast_to(rope_key.astype(jnp.float32)[:, None, :], (LEN, HEADS, ROPE))
        keys = finish_heads(jnp.concatenate([key_total, shared], axis=-1), positions, key_gain, ROPE)
        values = jnp.dot(latent_kv, w_value_up, preferred_element_type=jnp.float32).astype(jnp.bfloat16)
        attended = attend(queries, keys, values, HEADS)
        mixed = rms_scale(attended.astype(jnp.float32), out_gain).astype(jnp.bfloat16)
        return jnp.dot(mixed, w_out, preferred_element_type=jnp.float32).astype(jnp.bfloat16)
    return lax.map(one_sequence, tokens)
```

```python
import functools

import jax
import jax.numpy as jnp
import numpy as np
from jax import lax
from jax.experimental import pallas as pl
from jax.experimental.pallas import tpu as pltpu
from jax.sharding import PartitionSpec as P

HEADS, NOPE, ROPE, VD, QR, KR, QK = 16, 128, 64, 128, 512, 256, 192
D = 2048
ROWS = 256
EPS = 1e-06
THETA = 10000.0
NEG_BIG = -1e30
BF, F32 = jnp.bfloat16, jnp.float32
SOFT = float(QK**-0.5 * np.log2(np.e))
GROUP = 4


def rope_tables(blocks):
    half = ROPE // 2
    freq = THETA ** (-np.arange(half) / half)
    low = np.arange(ROWS)[:, None] * freq[None, :]
    high = (np.arange(blocks) * ROWS)[:, None] * freq[None, :]
    pad = np.zeros((ROWS, 128 - ROPE))
    lowq = np.stack([np.concatenate([f(low), f(low), pad], 1) for f in (np.cos, np.sin)])
    hpad = np.zeros((blocks, 128 - ROPE))
    highq = np.stack([np.concatenate([f(high), f(high), hpad], 1) for f in (np.cos, np.sin)], 1)
    highq = np.broadcast_to(highq[:, :, None, :], (blocks, 2, 8, 128))
    lowk = np.concatenate([np.cos(low).T, np.sin(low).T], 0)
    highk = np.concatenate([np.cos(high), np.sin(high)], 1)
    highk = np.broadcast_to(highk[:, :, None], (blocks, ROPE, 128))
    return [np.ascontiguousarray(t, dtype=np.float32) for t in (lowq, highq, lowk, highk)]


def dot(a, b):
    return lax.dot_general(a, b, (((1,), (0,)), ((), ())), preferred_element_type=F32)


def dot_nt(a, b):
    return lax.dot_general(a, b, (((1,), (1,)), ((), ())), preferred_element_type=F32)


def prepare_up(u_ref, wq_ref, wkt_ref, wv_ref):
    def one(h, _):
        wq_ref[h] = u_ref[h, :, 0:64, :].reshape(QR, 256)
        kv = u_ref[h, :, 64:96, :].reshape(KR, 256)
        wkt_ref[h] = kv[:, 0:NOPE].T
        wv_ref[h] = kv[:, NOPE:256]
        return 0

    lax.fori_loop(0, HEADS, one, 0)


def make_queries(latq, block, wq_ref, qgain, lowq_ref, highq_ref, q_ref):
    ch, sh = highq_ref[block, 0, 0:1], highq_ref[block, 1, 0:1]
    cl, sl = lowq_ref[0], lowq_ref[1]
    cosine = ch * cl - sh * sl
    sine = sh * cl + ch * sl
    lane = lax.broadcasted_iota(jnp.int32, (ROWS, 128), 1)
    sine_a = jnp.where(lane < ROPE // 2, -sine, 0.0)
    sine_b = jnp.where(lane < ROPE // 2, 0.0, sine)

    def one(h, _):
        q = dot(latq, wq_ref[h])
        scale = lax.rsqrt(jnp.sum(q * q, axis=1, keepdims=True) * (1.0 / QK) + EPS)
        n = q * scale * qgain
        t = n[:, NOPE:256]
        turned = (
            t * cosine
            + pltpu.roll(t, 128 - ROPE // 2, 1) * sine_a
            + pltpu.roll(t, ROPE // 2, 1) * sine_b
        )
        q_ref[h, :, 0:NOPE] = n[:, 0:NOPE].astype(BF)
        q_ref[h, :, NOPE:256] = turned.astype(BF)
        return 0

    lax.fori_loop(0, HEADS, one, 0)


def expand(unit, block, wkt_ref, wv_ref, gk_ref, gr_ref, lowk_ref, highk_ref, kt_ref, v_ref):
    kv = unit[0:256, :]
    rope = unit[256:320, :].astype(F32)
    half = ROPE // 2
    ch = jnp.concatenate([highk_ref[block, 0:half]] * 2, axis=1)
    sh = jnp.concatenate([highk_ref[block, half:ROPE]] * 2, axis=1)
    cl, sl = lowk_ref[0:half], lowk_ref[half:ROPE]
    cosine = ch * cl - sh * sl
    sine = sh * cl + ch * sl
    rope_sq = jnp.sum(rope * rope, axis=0, keepdims=True)
    x = rope * gr_ref[...]
    a, b = x[0:half], x[half:ROPE]
    turned = jnp.concatenate([a * cosine - b * sine, b * cosine + a * sine], axis=0)

    def one(g, _):
        heads = pl.ds(g * GROUP, GROUP)
        kt = dot_nt(wkt_ref[heads].reshape(GROUP * NOPE, KR), kv)
        for i in range(GROUP):
            k = kt[i * NOPE : (i + 1) * NOPE]
            scale = lax.rsqrt(
                (jnp.sum(k * k, axis=0, keepdims=True) + rope_sq) * (1.0 / QK) + EPS
            )
            kt_ref[g * GROUP + i, 0:NOPE] = (k * scale * gk_ref[...]).astype(BF)
            kt_ref[g * GROUP + i, NOPE:QK] = (turned * scale).astype(BF)
            v_ref[g * GROUP + i, :, 0:VD] = dot(kv, wv_ref[g * GROUP + i]).astype(BF)
        return 0

    lax.fori_loop(0, HEADS // GROUP, one, 0)


def attend(diagonal, q_ref, kt_ref, v_ref, m_ref, acc_ref):
    def one(g, _):
        for i in range(GROUP):
            h = g * GROUP + i
            s = dot(q_ref[h], kt_ref[h])
            if diagonal:
                row = lax.broadcasted_iota(jnp.int32, (ROWS, ROWS), 0)
                col = lax.broadcasted_iota(jnp.int32, (ROWS, ROWS), 1)
                s = jnp.where(col <= row, s, NEG_BIG)
            top = jnp.max(s, axis=1, keepdims=True)
            if diagonal:
                p = jnp.exp2((s - top) * SOFT).astype(BF)
                m_ref[h] = jnp.broadcast_to(top, (ROWS, 128))
                acc_ref[h] = dot(p, v_ref[h])
            else:
                old = m_ref[h]
                new = jnp.maximum(old, top)
                fade = jnp.exp2((old - new) * SOFT)
                p = jnp.exp2((s - jnp.concatenate([new, new], 1)) * SOFT).astype(BF)
                m_ref[h] = new
                acc_ref[h] = acc_ref[h] * jnp.concatenate([fade, fade], 1) + dot(p, v_ref[h])
        return 0

    lax.fori_loop(0, HEADS // GROUP, one, 0)


def finish(acc_ref, mixed_ref, ogain_ref, wout_ref, out_ref):
    total = jnp.zeros((ROWS, VD), F32)
    for h in range(HEADS):
        at = (acc_ref[h, :, 0:VD] / acc_ref[h, :, VD : 2 * VD]).astype(BF)
        mixed_ref[:, h * VD : (h + 1) * VD] = at
        total = total + at.astype(F32) * at.astype(F32)
    scale = lax.rsqrt(jnp.sum(total, axis=1, keepdims=True) * (1.0 / (HEADS * VD)) + EPS)
    for h in range(HEADS):
        cols = slice(h * VD, (h + 1) * VD)
        mixed_ref[:, cols] = (mixed_ref[:, cols].astype(F32) * scale * ogain_ref[:, cols]).astype(BF)

    def one(j, _):
        cols = pl.ds(pl.multiple_of(j * 256, 256), 256)
        out_ref[:, cols] = dot(mixed_ref[...], wout_ref[:, cols]).astype(BF)
        return 0

    lax.fori_loop(0, D // 256, one, 0)


def main_kernel(
    latq_ref, kv_ref, u_ref, wout_hbm, qgain_ref, gk_ref, gr_ref, ogain_ref,
    lowq_ref, highq_ref, lowk_ref, highk_ref, out_ref,
    wq_ref, wkt_ref, wv_ref, q_ref, kt_ref, v_ref, m_ref, acc_ref, mixed_ref, wout_ref, sem,
):
    me = lax.axis_index("sp")
    load = pltpu.make_async_copy(wout_hbm, wout_ref, sem)
    load.start()
    prepare_up(u_ref, wq_ref, wkt_ref, wv_ref)
    make_queries(latq_ref[...], me, wq_ref, qgain_ref[...], lowq_ref, highq_ref, q_ref)
    kt_ref[:, QK:256, :] = jnp.zeros((HEADS, 256 - QK, 256), BF)
    v_ref[:, :, VD:256] = jnp.ones((HEADS, ROWS, 256 - VD), BF)

    def block(b):
        expand(
            kv_ref[b], b, wkt_ref, wv_ref, gk_ref, gr_ref, lowk_ref, highk_ref, kt_ref, v_ref
        )

    block(me)
    attend(True, q_ref, kt_ref, v_ref, m_ref, acc_ref)

    def one(i, _):
        block(i)
        attend(False, q_ref, kt_ref, v_ref, m_ref, acc_ref)
        return 0

    lax.fori_loop(0, me, one, 0)
    load.wait()
    finish(acc_ref, mixed_ref, ogain_ref, wout_ref, out_ref)


def rms_scale(values, scaling):
    return values * lax.rsqrt(jnp.mean(values * values, axis=-1, keepdims=True) + EPS) * scaling


def per_device(
    tokens, in_gain, w_query_down, w_latent_down, w_rope_key, query_latent_gain, latent_gain,
    w_query_up, w_key_up, w_value_up, query_gain, key_gain, out_gain, w_out,
):
    blocks = lax.axis_size("sp")
    wout = lax.all_gather(w_out, ("sp", "dp"), axis=0, tiled=True)
    up = jnp.concatenate(
        [
            jnp.pad(w_query_up, ((0, 0), (0, 256 - QK))),
            jnp.concatenate([w_key_up, w_value_up], axis=1),
        ],
        axis=0,
    )
    down = lax.all_gather(
        jnp.concatenate([w_query_down, w_latent_down], axis=1), "dp", axis=0, tiled=True
    )
    ups = lax.all_gather(up, ("sp", "dp"), axis=0, tiled=True).reshape(HEADS, 8, 96, 256)
    rows = tokens.reshape(ROWS, D)
    normed = rms_scale(rows.astype(F32), in_gain).astype(BF)
    both = dot(normed, down)
    latent_q = rms_scale(both[:, :QR], query_latent_gain).astype(BF)
    latent_kv = rms_scale(both[:, QR:], latent_gain).astype(BF)
    rope_t = dot_nt(w_rope_key.T, normed).astype(BF)
    unit = jnp.concatenate([latent_kv, rope_t], axis=0)
    units = lax.all_gather(unit, "sp", axis=0, tiled=True).reshape(blocks, 320, 256)
    tables = [jnp.asarray(t) for t in rope_tables(blocks)]
    qgain = jnp.pad(query_gain, (0, 256 - QK)).reshape(1, 256)
    gk = jnp.broadcast_to(key_gain[:NOPE, None], (NOPE, 256))
    gr = jnp.broadcast_to(key_gain[NOPE:, None], (ROPE, 256))
    vm = pl.BlockSpec(memory_space=pltpu.VMEM)
    out = pl.pallas_call(
        main_kernel,
        out_shape=jax.ShapeDtypeStruct((ROWS, D), BF),
        in_specs=[vm, vm, vm, pl.BlockSpec(memory_space=pl.ANY)] + [vm] * 8,
        out_specs=vm,
        scratch_shapes=[
            pltpu.VMEM((HEADS, QR, 256), BF),
            pltpu.VMEM((HEADS, NOPE, KR), BF),
            pltpu.VMEM((HEADS, KR, VD), BF),
            pltpu.VMEM((HEADS, ROWS, 256), BF),
            pltpu.VMEM((HEADS, 256, 256), BF),
            pltpu.VMEM((HEADS, 256, 256), BF),
            pltpu.VMEM((HEADS, ROWS, 128), F32),
            pltpu.VMEM((HEADS, ROWS, 256), F32),
            pltpu.VMEM((ROWS, D), BF),
            pltpu.VMEM((D, D), BF),
            pltpu.SemaphoreType.DMA,
        ],
        compiler_params=pltpu.CompilerParams(vmem_limit_bytes=58 * 1024 * 1024),
        cost_estimate=pl.CostEstimate(flops=20_000_000_000, bytes_accessed=20_000_000, transcendentals=0),
    )(latent_q, units, ups, wout, qgain, gk, gr, out_gain.reshape(1, D), *tables)
    return out.reshape(1, ROWS, D)


def solution(mesh):
    in_specs = (
        P("dp", "sp", None), P(), P("dp", None), P("dp", None), P(), P(), P(),
        P("dp", "sp"), P("dp", "sp"), P("dp", "sp"), P(), P(), P(), P(("sp", "dp"), None),
    )
    return jax.shard_map(
        per_device, mesh=mesh, in_specs=in_specs, out_specs=P("dp", "sp", None), check_vma=False
    )
```

```python
import functools

import jax
import jax.numpy as jnp
import numpy as np
from jax import lax
from jax.experimental import pallas as pl
from jax.experimental.pallas import tpu as pltpu
from jax.sharding import PartitionSpec as P

HEADS, NOPE, ROPE, VD, QR, KR, QK = 16, 128, 64, 128, 512, 256, 192
D = 2048
ROWS = 256
EPS = 1e-06
THETA = 10000.0
NEG_BIG = -1e30
BF, F32 = jnp.bfloat16, jnp.float32
SOFT = float(QK**-0.5 * np.log2(np.e))
LOCAL = 8


def rope_tables(blocks):
    half = ROPE // 2
    freq = THETA ** (-np.arange(half) / half)
    low = np.arange(ROWS)[:, None] * freq[None, :]
    high = (np.arange(blocks) * ROWS)[:, None] * freq[None, :]
    pad = np.zeros((ROWS, 128 - ROPE))
    lowq = np.stack([np.concatenate([f(low), f(low), pad], 1) for f in (np.cos, np.sin)])
    hpad = np.zeros((blocks, 128 - ROPE))
    highq = np.stack([np.concatenate([f(high), f(high), hpad], 1) for f in (np.cos, np.sin)], 1)
    highq = np.broadcast_to(highq[:, :, None, :], (blocks, 2, 8, 128))
    lowk = np.concatenate([np.cos(low).T, np.sin(low).T], 0)
    highk = np.concatenate([np.cos(high), np.sin(high)], 1)
    highk = np.broadcast_to(highk[:, :, None], (blocks, ROPE, 128))
    return [np.ascontiguousarray(t, dtype=np.float32) for t in (lowq, highq, lowk, highk)]


def dot(a, b):
    return lax.dot_general(a, b, (((1,), (0,)), ((), ())), preferred_element_type=F32)


def dot_nt(a, b):
    return lax.dot_general(a, b, (((1,), (1,)), ((), ())), preferred_element_type=F32)


def prepare_up(us, wq_ref, wkt_ref, wv_ref):
    def one(h, _):
        for x in range(4):
            for c in range(2):
                d = 2 * x + c
                unit = us[c, h, x]
                wq_ref[h, d * 64 : d * 64 + 64] = unit[0:64]
                kv_rows = slice(d * 32, d * 32 + 32)
                wv_ref[h, kv_rows] = unit[64:96, NOPE:256]
                wkt_ref[h, kv_rows] = unit[64:96, 0:NOPE]
        return 0

    lax.fori_loop(0, LOCAL, one, 0)


def transpose_keys(wk_ref, wkt_ref):
    def one(h, _):
        wkt_ref[h] = wk_ref[h].T
        return 0

    lax.fori_loop(0, LOCAL, one, 0)


def make_queries(latq, block, wq_ref, qgain, lowq_ref, highq_ref, q_ref, which):
    ch, sh = highq_ref[block, 0, 0:1], highq_ref[block, 1, 0:1]
    cl, sl = lowq_ref[0], lowq_ref[1]
    cosine = ch * cl - sh * sl
    sine = sh * cl + ch * sl
    lane = lax.broadcasted_iota(jnp.int32, (ROWS, 128), 1)
    sine_a = jnp.where(lane < ROPE // 2, -sine, 0.0)
    sine_b = jnp.where(lane < ROPE // 2, 0.0, sine)

    def one(g, _):
        for i in range(2):
            h = g * 2 + i
            q = dot(latq, wq_ref[h])
            scale = lax.rsqrt(jnp.sum(q * q, axis=1, keepdims=True) * (1.0 / QK) + EPS)
            n = q * scale * qgain
            t = n[:, NOPE:256]
            turned = (
                t * cosine
                + pltpu.roll(t, 128 - ROPE // 2, 1) * sine_a
                + pltpu.roll(t, ROPE // 2, 1) * sine_b
            )
            q_ref[which, h, :, 0:NOPE] = n[:, 0:NOPE].astype(BF)
            q_ref[which, h, :, NOPE:256] = turned.astype(BF)
        return 0

    lax.fori_loop(0, LOCAL // 2, one, 0)


def expand(unit, block, wkt_ref, wv_ref, gk_ref, gr_ref, lowk_ref, highk_ref, kt_ref, v_ref, slot):
    kv = unit[0:256, :]
    rope = unit[256:320, :].astype(F32)
    half = ROPE // 2
    ch = jnp.concatenate([highk_ref[block, 0:half]] * 2, axis=1)
    sh = jnp.concatenate([highk_ref[block, half:ROPE]] * 2, axis=1)
    cl, sl = lowk_ref[0:half], lowk_ref[half:ROPE]
    cosine = ch * cl - sh * sl
    sine = sh * cl + ch * sl
    rope_sq = jnp.sum(rope * rope, axis=0, keepdims=True)
    x = rope * gr_ref[...]
    a, b = x[0:half], x[half:ROPE]
    turned = jnp.concatenate([a * cosine - b * sine, b * cosine + a * sine], axis=0)
    kt = dot_nt(wkt_ref[...].reshape(LOCAL * NOPE, KR), kv)
    for h in range(LOCAL):
        k = kt[h * NOPE : (h + 1) * NOPE]
        scale = lax.rsqrt((jnp.sum(k * k, axis=0, keepdims=True) + rope_sq) * (1.0 / QK) + EPS)
        kt_ref[slot, h, 0:NOPE] = (k * scale * gk_ref[...]).astype(BF)
        kt_ref[slot, h, NOPE:QK] = (turned * scale).astype(BF)
    for h in range(LOCAL):
        v_ref[slot, h, :, 0:VD] = dot(kv, wv_ref[h]).astype(BF)


def attend(diagonal, q_ref, kt_ref, v_ref, m_ref, acc_ref, which, slot):
    for h in range(LOCAL):
        s = dot(q_ref[which, h], kt_ref[slot, h])
        if diagonal:
            row = lax.broadcasted_iota(jnp.int32, (ROWS, ROWS), 0)
            col = lax.broadcasted_iota(jnp.int32, (ROWS, ROWS), 1)
            s = jnp.where(col <= row, s, NEG_BIG)
        old = m_ref[which, h]
        new = jnp.maximum(old, jnp.max(s, axis=1, keepdims=True))
        fade = jnp.exp2((old - new) * SOFT)
        p = jnp.exp2((s - jnp.concatenate([new, new], 1)) * SOFT).astype(BF)
        m_ref[which, h] = new
        acc_ref[which, h] = acc_ref[which, h] * jnp.concatenate([fade, fade], 1) + dot(
            p, v_ref[slot, h]
        )


def close_heads(acc_ref, which, att_ref, first):
    for h in range(LOCAL):
        att_ref[first + h] = (
            acc_ref[which, h, :, 0:VD] / acc_ref[which, h, :, VD : 2 * VD]
        ).astype(BF)


def finish(att_ref, mixed_ref, ogain_ref, wo_ref, out_ref):
    total = jnp.zeros((ROWS, VD), F32)
    for h in range(HEADS):
        at = att_ref[h].astype(F32)
        total = total + at * at
    scale = lax.rsqrt(jnp.sum(total, axis=1, keepdims=True) * (1.0 / (HEADS * VD)) + EPS)
    for h in range(HEADS):
        cols = slice(h * VD, (h + 1) * VD)
        mixed_ref[:, cols] = (att_ref[h].astype(F32) * scale * ogain_ref[:, cols]).astype(BF)

    def one(j, _):
        cols = pl.ds(pl.multiple_of(j * 256, 256), 256)
        w = wo_ref[:, :, :, :, :, cols].reshape(HEADS * VD, 256)
        out_ref[:, cols] = dot(mixed_ref[...], w).astype(BF)
        return 0

    lax.fori_loop(0, D // 256, one, 0)


def rms_rows(values, scaling):
    return values * lax.rsqrt(jnp.mean(values * values, axis=-1, keepdims=True) + EPS) * scaling


SLOTS = 128
OPS = 51


def kernel(
    tok_ref, ing_ref, wqd_ref, wld_ref, wrt_ref, qlg_ref, klg_ref, wqu_ref, wku_ref, wvu_ref,
    qgain_ref, gk_ref, gr_ref, ogain_ref, wo_in_ref, lowq_ref, highq_ref, lowk_ref, highk_ref,
    out_ref,
    wd, us, wo, kvb, lq, normed, sums, wq_ref, wk_ref, wkt_ref, wv_ref, q_ref, kt_ref, v_ref,
    m_ref, acc_ref, att_ref, mixed_ref, ssem, rsem,
):
    sp, dp = lax.axis_index("sp"), lax.axis_index("dp")
    z, y = sp // 4, sp % 4
    x, c = dp // 2, dp % 2
    xl, xr, xo = (x + 3) % 4, (x + 1) % 4, (x + 2) % 4
    yl, yr, yo = (y + 3) % 4, (y + 1) % 4, (y + 2) % 4
    zl, zr, zo = (z + 3) % 4, (z + 1) % 4, (z + 2) % 4
    co = 1 - c
    zb = z % 2
    zpair = z + 1 - 2 * zb
    zmate = 3 - z

    def dev(xx=x, yy=y, zz=z, cc=c):
        return {"sp": zz * 4 + yy, "dp": xx * 2 + cc}

    X_R, X_L, Y_R, Y_L, Z_R, Z_L, CORE = (
        dev(xx=xr), dev(xx=xl), dev(yy=yr), dev(yy=yl), dev(zz=zr), dev(zz=zl), dev(cc=co)
    )
    names, sent = {}, []

    def number(name):
        return names.setdefault(name, len(names))

    def push(name, view, to, dst=None):
        i = number(name)
        again = view if callable(view) else functools.partial(lambda v: v, view)
        view = again()
        pltpu.make_async_remote_copy(
            src_ref=view, dst_ref=view if dst is None else dst, send_sem=ssem.at[i],
            recv_sem=rsem.at[i], device_id=to, device_id_type=pl.DeviceIdType.MESH,
        ).start()
        sent.append((i, again))

    def got(name, view):
        pltpu.make_async_copy(view, view, rsem.at[number(name)]).wait()

    barrier = pltpu.get_barrier_semaphore()
    for to in (X_R, X_L, Y_R, Y_L, Z_R, Z_L, CORE):
        pl.semaphore_signal(barrier, 1, device_id=to, device_id_type=pl.DeviceIdType.MESH)

    hl = zb * 4 + y
    us[c, hl, x, 0:64, 0:NOPE] = wqu_ref[:, 0:NOPE]
    us[c, hl, x, 0:64, NOPE:256] = jnp.concatenate(
        [wqu_ref[:, NOPE:QK], jnp.zeros((64, 256 - QK), BF)], axis=1
    )
    us[c, hl, x, 64:96, 0:NOPE] = wku_ref[...]
    us[c, hl, x, 64:96, NOPE:256] = wvu_ref[...]
    wo[z, y, x, c] = wo_in_ref[...]
    wd[dp, :, 0:QR] = wqd_ref[...]
    wd[dp, :, QR : QR + KR] = wld_ref[...]
    pl.semaphore_wait(barrier, 7)

    uown = us.at[c, hl, x]
    push("u_r", uown, X_R)
    push("u_l", uown, X_L)
    wown = wo.at[z, y, x, c]
    push("w_yr", wown, Y_R)
    push("w_yl", wown, Y_L)
    down = wd.at[dp]
    push("d_r", down, X_R)
    push("d_l", down, X_L)
    push("d_c", down, CORE)

    for r in range(0, ROWS, 64):
        rows = slice(r, r + 64)
        n = rms_rows(tok_ref[rows].astype(F32), ing_ref[...]).astype(BF)
        for k in range(8):
            normed[k, rows] = n[:, k * 256 : (k + 1) * 256]

    got("u_r", us.at[c, hl, xl])
    push("u_or", us.at[c, hl, xl, 0:48], X_R)
    got("u_l", us.at[c, hl, xr])
    push("u_ol", us.at[c, hl, xr, 48:96], X_L)
    got("w_yr", wo.at[z, yl, x, c])
    push("w_oyr", wo.at[z, yl, x, c, :, 0:1024], Y_R)
    got("w_yl", wo.at[z, yr, x, c])
    push("w_oyl", wo.at[z, yr, x, c, :, 1024:2048], Y_L)
    got("u_or", us.at[c, hl, xo, 0:48])
    got("u_ol", us.at[c, hl, xo, 48:96])
    block0 = us.at[c, hl]
    push("u_z", block0, dev(zz=zpair))
    push("u_y0r", block0, Y_R)
    push("u_y0l", block0, Y_L)
    push("u_c0", block0, CORE)
    got("w_oyr", wo.at[z, yo, x, c, :, 0:1024])
    got("w_oyl", wo.at[z, yo, x, c, :, 1024:2048])
    push("w_zr", wo.at[z, :, x, c], Z_R)
    push("w_zl", wo.at[z, :, x, c], Z_L)

    def add(d, first=False):
        part = dot(normed[d], wd[d])
        if first:
            sums[...] = part
        else:
            sums[...] += part

    add(dp, True)
    got("d_c", wd.at[2 * x + co])
    add(2 * x + co)
    base0, base1 = zb * 4, 4 - zb * 4
    got("u_z", us.at[c, base1 + y])
    block1 = us.at[c, base1 + y]
    push("u_c1", block1, CORE)

    def ring_y(j, base):
        got(f"u_y{j}r", us.at[c, base + yl])
        push(f"u_y{j}or", us.at[c, base + yl, 0:2], Y_R)
        push(f"u_c{j}l", us.at[c, base + yl], CORE)
        got(f"u_y{j}l", us.at[c, base + yr])
        push(f"u_y{j}ol", us.at[c, base + yr, 2:4], Y_L)
        push(f"u_c{j}r", us.at[c, base + yr], CORE)

    ring_y(0, base0)
    push("u_y1r", block1, Y_R)
    push("u_y1l", block1, Y_L)
    got("d_r", wd.at[2 * xl + c])
    push("d_or", wd.at[2 * xl + c, 0:128], X_R)
    push("d_cl", wd.at[2 * xl + c], CORE)
    got("d_l", wd.at[2 * xr + c])
    push("d_ol", wd.at[2 * xr + c, 128:256], X_L)
    push("d_cr", wd.at[2 * xr + c], CORE)
    add(2 * xl + c)
    add(2 * xr + c)
    got("d_cl", wd.at[2 * xl + co])
    add(2 * xl + co)
    got("d_cr", wd.at[2 * xr + co])
    add(2 * xr + co)
    got("w_zr", wo.at[zl, :, x, c])
    push("w_ozr", wo.at[zl, 0:2, x, c], Z_R)
    got("w_zl", wo.at[zr, :, x, c])
    push("w_ozl", wo.at[zr, 2:4, x, c], Z_L)
    ring_y(1, base1)
    got("d_or", wd.at[2 * xo + c, 0:128])
    push("d_coa", wd.at[2 * xo + c, 0:128], CORE)
    got("d_ol", wd.at[2 * xo + c, 128:256])
    push("d_cob", wd.at[2 * xo + c, 128:256], CORE)
    rope_t = jnp.zeros((ROPE, ROWS), F32)
    for k in range(8):
        rope_t = rope_t + dot_nt(wrt_ref[:, k * 256 : (k + 1) * 256], normed[k])
    add(2 * xo + c)
    got("d_coa", wd.at[2 * xo + co, 0:128])
    got("d_cob", wd.at[2 * xo + co, 128:256])
    add(2 * xo + co)

    kvb[y, z, 0:256] = rms_rows(sums[:, QR : QR + KR], klg_ref[...]).astype(BF)
    kvb[y, z, 256:320] = rope_t.astype(BF)
    lq[0] = rms_rows(sums[:, 0:QR], qlg_ref[...]).astype(BF)
    own = kvb.at[y, z]
    push("k_yr", own, Y_R)
    push("k_yl", own, Y_L)
    push("k_zr", own, Z_R)
    push("k_zl", own, Z_L)
    push("q", lq.at[0], dev(zz=zmate), lq.at[1])

    for j, base in ((0, base0), (1, base1)):
        got(f"u_y{j}or", us.at[c, base + yo, 0:2])
        got(f"u_y{j}ol", us.at[c, base + yo, 2:4])
        push(f"u_c{j}o", us.at[c, base + yo], CORE)
    got("w_ozr", wo.at[zo, 0:2, x, c])
    got("w_ozl", wo.at[zo, 2:4, x, c])
    for p in range(2):
        push(f"w_xr{p}", wo.at[2 * p : 2 * p + 2, :, x, c], X_R)
        push(f"w_xl{p}", wo.at[2 * p : 2 * p + 2, :, x, c], X_L)
    for j, base in ((0, base0), (1, base1)):
        got(f"u_c{j}", us.at[co, base + y])
        got(f"u_c{j}l", us.at[co, base + yl])
        got(f"u_c{j}r", us.at[co, base + yr])
        got(f"u_c{j}o", us.at[co, base + yo])
    push("w_c", wo.at[:, :, x, c], CORE)
    prepare_up(us, wq_ref, wk_ref, wv_ref)
    transpose_keys(wk_ref, wkt_ref)
    make_queries(lq[0], sp, wq_ref, qgain_ref[...], lowq_ref, highq_ref, q_ref, 0)
    m_ref[...] = jnp.full(m_ref.shape, NEG_BIG, F32)
    acc_ref[...] = jnp.zeros(acc_ref.shape, F32)
    kt_ref[:, :, QK:256, :] = jnp.zeros((4, LOCAL, 256 - QK, 256), BF)
    v_ref[:, :, :, VD:256] = jnp.ones((4, LOCAL, ROWS, 256 - VD), BF)

    def k1():
        got("k_yr", kvb.at[yl, z])
        push("k_oyr", lambda: kvb.at[yl, z, 0:160], Y_R)
        got("k_yl", kvb.at[yr, z])
        push("k_oyl", lambda: kvb.at[yr, z, 160:320], Y_L)

    def k2():
        got("k_zr", kvb.at[y, zl])
        push("k_ozr", lambda: kvb.at[y, zl, 0:160], Z_R)
        push("k_y1r", lambda: kvb.at[y, zl], Y_R)
        push("k_y1l", lambda: kvb.at[y, zl], Y_L)
        got("k_zl", kvb.at[y, zr])
        push("k_ozl", lambda: kvb.at[y, zr, 160:320], Z_L)
        push("k_y2r", lambda: kvb.at[y, zr], Y_R)
        push("k_y2l", lambda: kvb.at[y, zr], Y_L)

    def k3():
        got("k_oyr", kvb.at[yo, z, 0:160])
        got("k_oyl", kvb.at[yo, z, 160:320])
        push("k_pzr", lambda: kvb.at[yo, z], Z_R)
        push("k_pzl", lambda: kvb.at[yo, z], Z_L)
        got("k_ozr", kvb.at[y, zo, 0:160])
        got("k_ozl", kvb.at[y, zo, 160:320])
        push("k_y3r", lambda: kvb.at[y, zo], Y_R)
        push("k_y3l", lambda: kvb.at[y, zo], Y_L)

    def k7():
        got("k_y1r", kvb.at[yl, zl])
        got("k_y1l", kvb.at[yr, zl])

    def k9():
        got("k_y2r", kvb.at[yl, zr])
        got("k_y2l", kvb.at[yr, zr])
        got("k_pzr", kvb.at[yo, zl])
        push("k_pozr", lambda: kvb.at[yo, zl, 0:160], Z_R)
        got("k_pzl", kvb.at[yo, zr])
        push("k_pozl", lambda: kvb.at[yo, zr, 160:320], Z_L)

    def k13():
        got("k_y3r", kvb.at[yl, zo])
        got("k_y3l", kvb.at[yr, zo])

    def k15():
        got("k_pozr", kvb.at[yo, zo, 0:160])
        got("k_pozl", kvb.at[yo, zo, 160:320])

    def queries_mate():
        got("q", lq.at[1])
        make_queries(
            lq[1], zmate * 4 + y, wq_ref, qgain_ref[...], lowq_ref, highq_ref, q_ref, 1
        )

    def wx(p):
        def go():
            rng = slice(2 * p, 2 * p + 2)
            got(f"w_xr{p}", wo.at[rng, :, xl, c])
            push(f"w_oxr{p}", lambda: wo.at[2 * p, :, xl, c], X_R)
            push(f"w_cl{p}", lambda: wo.at[rng, :, xl, c], CORE)
            got(f"w_xl{p}", wo.at[rng, :, xr, c])
            push(f"w_oxl{p}", lambda: wo.at[2 * p + 1, :, xr, c], X_L)
            push(f"w_cr{p}", lambda: wo.at[rng, :, xr, c], CORE)

        return go

    def wxo(p):
        got(f"w_oxr{p}", wo.at[2 * p, :, xo, c])
        got(f"w_oxl{p}", wo.at[2 * p + 1, :, xo, c])
        push(f"w_co{p}", lambda: wo.at[2 * p : 2 * p + 2, :, xo, c], CORE)

    hfirst = (z // 2) * LOCAL
    b_own, b_mate = sp, zmate * 4 + y

    def send_mate():
        close_heads(acc_ref, 1, att_ref, HEADS)
        push("att", lambda: att_ref.at[HEADS : HEADS + LOCAL], dev(zz=zmate), att_ref.at[pl.ds(hfirst, LOCAL)])

    at_op = {3: (k1,), 6: (k2,), 9: (k3,), 11: (queries_mate,), 21: (k7,), 22: (wx(0),),
             27: (k9,), 40: (k13,), 42: (k15,), 44: (wx(1),), 47: (send_mate,)}

    def op(t, _):
        for when, todo in at_op.items():
            @pl.when(t == when)
            def _(todo=todo):
                for f in todo:
                    f()

        def pick(test, yes, no):
            return no + test.astype(jnp.int32) * (yes - no)

        late = t >= 39
        kind = pick(t < 36, t % 3, pick(late, (3 - (t - 39) // 4) % 3, 2))
        step = pick(t < 36, t // 3, pick(late, 12 + (t - 39) % 4, t - 27))
        step = step - 3 * ((kind == 2) & (t < 36)).astype(jnp.int32)
        live = step >= 0
        step = jnp.maximum(step, 0)
        dy = pick(step < 3, step, pick(step < 6, 0, pick(step == 6, 3, pick(
            step < 11, 1 + (step - 7) % 2, pick(
                step < 13, 3, pick(step < 15, step - 12, 3))))))
        dz = pick(step < 3, 0, pick(step < 6, step - 2, pick(step == 6, 0, pick(
            step < 11, 1 + (step - 7) // 2, pick(step < 13, step - 10, 3)))))
        yy = pick(dy == 0, y, pick(dy == 1, yl, pick(dy == 2, yr, yo)))
        zz = pick(dz == 0, z, pick(dz == 1, zl, pick(dz == 2, zr, zo)))
        b = zz * 4 + yy
        slot = step % 4
        which = pick(kind == 2, 1, 0)
        bq = pick(live, pick(which == 0, b_own, b_mate), -1)

        @pl.when((kind == 0) & (b <= jnp.maximum(b_own, b_mate)))
        def _():
            expand(
                kvb[yy, zz], b, wkt_ref, wv_ref, gk_ref, gr_ref, lowk_ref, highk_ref, kt_ref,
                v_ref, slot,
            )

        @pl.when((kind > 0) & (b < bq))
        def _():
            attend(False, q_ref, kt_ref, v_ref, m_ref, acc_ref, which, slot)

        @pl.when((kind > 0) & (b == bq))
        def _():
            attend(True, q_ref, kt_ref, v_ref, m_ref, acc_ref, which, slot)

        return 0

    lax.fori_loop(0, OPS, op, 0)
    close_heads(acc_ref, 0, att_ref, hfirst)
    for p in range(2):
        wxo(p)
    got("w_c", wo.at[:, :, x, co])
    for p in range(2):
        got(f"w_cl{p}", wo.at[2 * p : 2 * p + 2, :, xl, co])
        got(f"w_cr{p}", wo.at[2 * p : 2 * p + 2, :, xr, co])
        got(f"w_co{p}", wo.at[2 * p : 2 * p + 2, :, xo, co])
    got("att", att_ref.at[pl.ds(LOCAL - hfirst, LOCAL)])
    finish(att_ref, mixed_ref, ogain_ref, wo, out_ref)
    for i, again in sent:
        view = again()
        pltpu.make_async_copy(view, view, ssem.at[i]).wait()
    assert len(names) <= SLOTS


def per_device(
    tokens, in_gain, w_query_down, w_latent_down, w_rope_key, query_latent_gain, latent_gain,
    w_query_up, w_key_up, w_value_up, query_gain, key_gain, out_gain, w_out,
):
    blocks = lax.axis_size("sp")
    tables = [jnp.asarray(t) for t in rope_tables(blocks)]
    qgain = jnp.pad(query_gain, (0, 256 - QK)).reshape(1, 256)
    gains = jnp.broadcast_to(key_gain[:, None], (QK, 256))
    vm = pl.BlockSpec(memory_space=pltpu.VMEM)
    args = (
        tokens.reshape(ROWS, D), in_gain.reshape(1, D), w_query_down, w_latent_down, w_rope_key.T,
        query_latent_gain.reshape(1, QR), latent_gain.reshape(1, KR), w_query_up, w_key_up,
        w_value_up, qgain, gains[:NOPE], gains[NOPE:], out_gain.reshape(1, D), w_out, *tables,
    )
    out = pl.pallas_call(
        kernel,
        out_shape=jax.ShapeDtypeStruct((ROWS, D), BF),
        in_specs=[vm] * len(args),
        out_specs=vm,
        scratch_shapes=[
            pltpu.VMEM((8, 256, QR + KR), BF),
            pltpu.VMEM((2, LOCAL, 4, 96, 256), BF),
            pltpu.VMEM((4, 4, 4, 2, 16, D), BF),
            pltpu.VMEM((4, 4, 320, 256), BF),
            pltpu.VMEM((2, ROWS, QR), BF),
            pltpu.VMEM((8, ROWS, 256), BF),
            pltpu.VMEM((ROWS, QR + KR), F32),
            pltpu.VMEM((LOCAL, QR, 256), BF),
            pltpu.VMEM((LOCAL, KR, NOPE), BF),
            pltpu.VMEM((LOCAL, NOPE, KR), BF),
            pltpu.VMEM((LOCAL, KR, VD), BF),
            pltpu.VMEM((2, LOCAL, ROWS, 256), BF),
            pltpu.VMEM((4, LOCAL, 256, 256), BF),
            pltpu.VMEM((4, LOCAL, 256, 256), BF),
            pltpu.VMEM((2, LOCAL, ROWS, 128), F32),
            pltpu.VMEM((2, LOCAL, ROWS, 256), F32),
            pltpu.VMEM((HEADS + LOCAL, ROWS, VD), BF),
            pltpu.VMEM((ROWS, D), BF),
            pltpu.SemaphoreType.DMA((SLOTS,)),
            pltpu.SemaphoreType.DMA((SLOTS,)),
        ],
        compiler_params=pltpu.CompilerParams(
            vmem_limit_bytes=60 * 1024 * 1024, collective_id=0, has_side_effects=True
        ),
    )(*args)
    return out.reshape(1, ROWS, D)


def solution(mesh):
    in_specs = (
        P("dp", "sp", None), P(), P("dp", None), P("dp", None), P(), P(), P(),
        P("dp", "sp"), P("dp", "sp"), P("dp", "sp"), P(), P(), P(), P(("sp", "dp"), None),
    )
    return jax.shard_map(
        per_device, mesh=mesh, in_specs=in_specs, out_specs=P("dp", "sp", None), check_vma=False
    )
```

```python
import functools

import jax
import jax.numpy as jnp
import numpy as np
from jax import lax
from jax.experimental import pallas as pl
from jax.experimental.pallas import tpu as pltpu
from jax.sharding import PartitionSpec as P

HEADS, NOPE, ROPE, VD, QR, KR, QK = 16, 128, 64, 128, 512, 256, 192
D = 2048
ROWS = 256
EPS = 1e-06
THETA = 10000.0
NEG_BIG = -1e30
BF, F32 = jnp.bfloat16, jnp.float32
SOFT = float(QK**-0.5 * np.log2(np.e))
LOCAL = 8


def rope_tables(blocks):
    half = ROPE // 2
    freq = THETA ** (-np.arange(half) / half)
    low = np.arange(ROWS)[:, None] * freq[None, :]
    high = (np.arange(blocks) * ROWS)[:, None] * freq[None, :]
    pad = np.zeros((ROWS, 128 - ROPE))
    lowq = np.stack([np.concatenate([f(low), f(low), pad], 1) for f in (np.cos, np.sin)])
    hpad = np.zeros((blocks, 128 - ROPE))
    highq = np.stack([np.concatenate([f(high), f(high), hpad], 1) for f in (np.cos, np.sin)], 1)
    highq = np.broadcast_to(highq[:, :, None, :], (blocks, 2, 8, 128))
    lowk = np.concatenate([np.cos(low).T, np.sin(low).T], 0)
    highk = np.concatenate([np.cos(high), np.sin(high)], 1)
    highk = np.broadcast_to(highk[:, :, None], (blocks, ROPE, 128))
    return [np.ascontiguousarray(t, dtype=np.float32) for t in (lowq, highq, lowk, highk)]


def dot(a, b):
    return lax.dot_general(a, b, (((1,), (0,)), ((), ())), preferred_element_type=F32)


def dot_nt(a, b):
    return lax.dot_general(a, b, (((1,), (1,)), ((), ())), preferred_element_type=F32)


def prepare_up(us, wq_ref, wkt_ref, wv_ref):
    def one(h, _):
        for x in range(4):
            for c in range(2):
                d = 2 * x + c
                unit = us[c, h, x]
                wq_ref[h, d * 64 : d * 64 + 64] = unit[0:64]
                kv_rows = slice(d * 32, d * 32 + 32)
                wv_ref[h, kv_rows] = unit[64:96, NOPE:256]
                wkt_ref[h, kv_rows] = unit[64:96, 0:NOPE]
        return 0

    lax.fori_loop(0, LOCAL, one, 0)


def transpose_keys(wk_ref, wkt_ref):
    def one(h, _):
        wkt_ref[h] = wk_ref[h].T
        return 0

    lax.fori_loop(0, LOCAL, one, 0)


def make_queries(latq, block, wq_ref, qgain, lowq_ref, highq_ref, q_ref, which):
    ch, sh = highq_ref[block, 0, 0:1], highq_ref[block, 1, 0:1]
    cl, sl = lowq_ref[0], lowq_ref[1]
    cosine = ch * cl - sh * sl
    sine = sh * cl + ch * sl
    lane = lax.broadcasted_iota(jnp.int32, (ROWS, 128), 1)
    sine_a = jnp.where(lane < ROPE // 2, -sine, 0.0)
    sine_b = jnp.where(lane < ROPE // 2, 0.0, sine)

    for h in range(LOCAL):
        q = dot(latq, wq_ref[h])
        scale = lax.rsqrt(jnp.sum(q * q, axis=1, keepdims=True) * (1.0 / QK) + EPS)
        n = q * scale * qgain
        t = n[:, NOPE:256]
        turned = (
            t * cosine
            + pltpu.roll(t, 128 - ROPE // 2, 1) * sine_a
            + pltpu.roll(t, ROPE // 2, 1) * sine_b
        )
        q_ref[which, h, :, 0:NOPE] = n[:, 0:NOPE].astype(BF)
        q_ref[which, h, :, NOPE:256] = turned.astype(BF)


def expand(unit, block, wkt_ref, wv_ref, gk_ref, gr_ref, lowk_ref, highk_ref, kt_ref, v_ref, slot):
    kv = unit[0:256, :]
    rope = unit[256:320, :].astype(F32)
    half = ROPE // 2
    ch = jnp.concatenate([highk_ref[block, 0:half]] * 2, axis=1)
    sh = jnp.concatenate([highk_ref[block, half:ROPE]] * 2, axis=1)
    cl, sl = lowk_ref[0:half], lowk_ref[half:ROPE]
    cosine = ch * cl - sh * sl
    sine = sh * cl + ch * sl
    rope_sq = jnp.sum(rope * rope, axis=0, keepdims=True)
    x = rope * gr_ref[...]
    a, b = x[0:half], x[half:ROPE]
    turned = jnp.concatenate([a * cosine - b * sine, b * cosine + a * sine], axis=0)
    kt = dot_nt(wkt_ref[...].reshape(LOCAL * NOPE, KR), kv)
    for h in range(LOCAL):
        k = kt[h * NOPE : (h + 1) * NOPE]
        scale = lax.rsqrt((jnp.sum(k * k, axis=0, keepdims=True) + rope_sq) * (1.0 / QK) + EPS)
        kt_ref[slot, h, 0:NOPE] = (k * scale * gk_ref[...]).astype(BF)
        kt_ref[slot, h, NOPE:QK] = (turned * scale).astype(BF)
    for h in range(LOCAL):
        v_ref[slot, h, :, 0:VD] = dot(kv, wv_ref[h]).astype(BF)


def attend(diagonal, q_ref, kt_ref, v_ref, m_ref, acc_ref, which, slot):
    for h in range(LOCAL):
        s = dot(q_ref[which, h], kt_ref[slot, h])
        if diagonal:
            row = lax.broadcasted_iota(jnp.int32, (ROWS, ROWS), 0)
            col = lax.broadcasted_iota(jnp.int32, (ROWS, ROWS), 1)
            s = jnp.where(col <= row, s, NEG_BIG)
        old = m_ref[which, h]
        new = jnp.maximum(old, jnp.max(s, axis=1, keepdims=True))
        fade = jnp.exp2((old - new) * SOFT)
        p = jnp.exp2((s - jnp.concatenate([new, new], 1)) * SOFT).astype(BF)
        m_ref[which, h] = new
        acc_ref[which, h] = acc_ref[which, h] * jnp.concatenate([fade, fade], 1) + dot(
            p, v_ref[slot, h]
        )


def close_heads(acc_ref, which, att_ref, first):
    for h in range(LOCAL):
        att_ref[first + h] = (
            acc_ref[which, h, :, 0:VD] / acc_ref[which, h, :, VD : 2 * VD]
        ).astype(BF)


def finish(att_ref, mixed_ref, ogain_ref, wo_ref, out_ref):
    total = jnp.zeros((ROWS, VD), F32)
    for h in range(HEADS):
        at = att_ref[h].astype(F32)
        total = total + at * at
    scale = lax.rsqrt(jnp.sum(total, axis=1, keepdims=True) * (1.0 / (HEADS * VD)) + EPS)
    for h in range(HEADS):
        cols = slice(h * VD, (h + 1) * VD)
        mixed_ref[:, cols] = (att_ref[h].astype(F32) * scale * ogain_ref[:, cols]).astype(BF)

    def one(j, _):
        cols = pl.ds(pl.multiple_of(j * 256, 256), 256)
        w = wo_ref[:, :, :, :, :, cols].reshape(HEADS * VD, 256)
        out_ref[:, cols] = dot(mixed_ref[...], w).astype(BF)
        return 0

    lax.fori_loop(0, D // 256, one, 0)


def rms_rows(values, scaling):
    return values * lax.rsqrt(jnp.mean(values * values, axis=-1, keepdims=True) + EPS) * scaling


SLOTS = 128
KEPT = 5


def kernel(
    tok_ref, ing_ref, wqd_ref, wld_ref, wrt_ref, qlg_ref, klg_ref, wqu_ref, wku_ref, wvu_ref,
    qg_ref, kg_ref, ogain_ref, wo_in_ref, lowq_ref, highq_ref, lowk_ref, highk_ref,
    out_ref,
    wd, us, wo, kvb, lq, normed, sums, wq_ref, wk_ref, wkt_ref, wv_ref, q_ref, kt_ref, v_ref,
    m_ref, acc_ref, att_ref, mixed_ref, qgain_ref, gk_ref, gr_ref, ssem, rsem,
):
    sp, dp = lax.axis_index("sp"), lax.axis_index("dp")
    z, y = sp // 4, sp % 4
    x, c = dp // 2, dp % 2
    xl, xr, xo = (x + 3) % 4, (x + 1) % 4, (x + 2) % 4
    yl, yr, yo = (y + 3) % 4, (y + 1) % 4, (y + 2) % 4
    zl, zr, zo = (z + 3) % 4, (z + 1) % 4, (z + 2) % 4
    co = 1 - c
    zb = z % 2
    zpair = z + 1 - 2 * zb
    zmate = 3 - z

    def dev(xx=x, yy=y, zz=z, cc=c):
        return {"sp": zz * 4 + yy, "dp": xx * 2 + cc}

    X_R, X_L, Y_R, Y_L, Z_R, Z_L, CORE = (
        dev(xx=xr), dev(xx=xl), dev(yy=yr), dev(yy=yl), dev(zz=zr), dev(zz=zl), dev(cc=co)
    )
    names, sent = {}, []

    def number(name):
        return names.setdefault(name, len(names))

    def push(name, view, to, dst=None):
        i = number(name)
        again = view if callable(view) else functools.partial(lambda v: v, view)
        view = again()
        pltpu.make_async_remote_copy(
            src_ref=view, dst_ref=view if dst is None else dst, send_sem=ssem.at[i],
            recv_sem=rsem.at[i], device_id=to, device_id_type=pl.DeviceIdType.MESH,
        ).start()
        sent.append((i, again))

    def got(name, view):
        pltpu.make_async_copy(view, view, rsem.at[number(name)]).wait()

    barrier = pltpu.get_barrier_semaphore()
    X_O, Y_O = dev(xx=xo), dev(yy=yo)
    for to in (X_R, X_L, X_O, Y_R, Y_L, Y_O, Z_R, Z_L, CORE):
        pl.semaphore_signal(barrier, 1, device_id=to, device_id_type=pl.DeviceIdType.MESH)

    hl = zb * 4 + y
    us[c, hl, x, 0:64, 0:NOPE] = wqu_ref[:, 0:NOPE]
    us[c, hl, x, 0:64, NOPE:256] = jnp.concatenate(
        [wqu_ref[:, NOPE:QK], jnp.zeros((64, 256 - QK), BF)], axis=1
    )
    us[c, hl, x, 64:96, 0:NOPE] = wku_ref[...]
    us[c, hl, x, 64:96, NOPE:256] = wvu_ref[...]
    wo[z, y, x, c] = wo_in_ref[...]
    wd[dp, :, 0:QR] = wqd_ref[...]
    wd[dp, :, QR : QR + KR] = wld_ref[...]
    pl.semaphore_wait(barrier, 9)

    uown = us.at[c, hl, x]
    push("u_r", uown, X_R)
    push("u_l", uown, X_L)
    push("u_o", uown, X_O)
    wown = wo.at[z, y, x, c]
    push("w_yr", wown, Y_R)
    push("w_yl", wown, Y_L)
    push("w_yo", wown, Y_O)
    down = wd.at[dp]
    push("d_r", down, X_R)
    push("d_l", down, X_L)
    push("d_c", down, CORE)

    for r in range(0, ROWS, 64):
        rows = slice(r, r + 64)
        n = rms_rows(tok_ref[rows].astype(F32), ing_ref[...]).astype(BF)
        for k in range(8):
            normed[k, rows] = n[:, k * 256 : (k + 1) * 256]

    qgain_ref[:, 0:NOPE] = qg_ref[:, 0:NOPE]
    qgain_ref[:, NOPE:256] = jnp.concatenate(
        [qg_ref[:, NOPE:QK], jnp.zeros((1, 256 - QK), F32)], axis=1
    )
    kg = jnp.concatenate([kg_ref[...], jnp.zeros((1, 256 - QK), F32)], axis=1)
    column = jnp.broadcast_to(kg[:, 0:NOPE], (NOPE, NOPE)).T
    gk_ref[...] = jnp.concatenate([column, column], axis=1)
    column = jnp.broadcast_to(kg[:, NOPE:256], (NOPE, NOPE)).T[0:ROPE]
    gr_ref[...] = jnp.concatenate([column, column], axis=1)

    got("u_r", us.at[c, hl, xl])
    got("u_l", us.at[c, hl, xr])
    got("u_o", us.at[c, hl, xo])
    block0 = us.at[c, hl]
    push("u_z", block0, dev(zz=zpair))
    push("u_y0r", block0, Y_R)
    push("u_y0l", block0, Y_L)
    push("u_c0", block0, CORE)
    got("w_yr", wo.at[z, yl, x, c])
    got("w_yl", wo.at[z, yr, x, c])
    got("w_yo", wo.at[z, yo, x, c])
    push("w_zr", wo.at[z, :, x, c], Z_R)
    push("w_zl", wo.at[z, :, x, c], Z_L)

    def add(d, first=False):
        part = dot(normed[d], wd[d])
        if first:
            sums[...] = part
        else:
            sums[...] += part

    add(dp, True)
    got("d_c", wd.at[2 * x + co])
    add(2 * x + co)
    m_ref[...] = jnp.full(m_ref.shape, NEG_BIG, F32)
    acc_ref[...] = jnp.zeros(acc_ref.shape, F32)
    kt_ref[:, :, QK:256, :] = jnp.zeros((KEPT, LOCAL, 256 - QK, 256), BF)
    v_ref[:, :, :, VD:256] = jnp.ones((KEPT, LOCAL, ROWS, 256 - VD), BF)
    rope_t = jnp.zeros((ROPE, ROWS), F32)
    for k in range(8):
        rope_t = rope_t + dot_nt(wrt_ref[:, k * 256 : (k + 1) * 256], normed[k])
    kvb[y, z, 256:320] = rope_t.astype(BF)
    base0, base1 = zb * 4, 4 - zb * 4
    block1 = us.at[c, base1 + y]

    def ring_y(j, base):
        got(f"u_y{j}r", us.at[c, base + yl])
        push(f"u_y{j}or", us.at[c, base + yl, 0:2], Y_R)
        push(f"u_c{j}l", us.at[c, base + yl], CORE)
        got(f"u_y{j}l", us.at[c, base + yr])
        push(f"u_y{j}ol", us.at[c, base + yr, 2:4], Y_L)
        push(f"u_c{j}r", us.at[c, base + yr], CORE)

    ring_y(0, base0)
    got("u_z", us.at[c, base1 + y])
    push("u_y1r", block1, Y_R)
    push("u_y1l", block1, Y_L)
    push("u_c1", block1, CORE)
    got("d_r", wd.at[2 * xl + c])
    push("d_or", wd.at[2 * xl + c, 0:128], X_R)
    push("d_cl", wd.at[2 * xl + c], CORE)
    got("d_l", wd.at[2 * xr + c])
    push("d_ol", wd.at[2 * xr + c, 128:256], X_L)
    push("d_cr", wd.at[2 * xr + c], CORE)
    add(2 * xl + c)
    add(2 * xr + c)
    got("d_cl", wd.at[2 * xl + co])
    add(2 * xl + co)
    got("d_cr", wd.at[2 * xr + co])
    add(2 * xr + co)
    got("w_zr", wo.at[zl, :, x, c])
    push("w_ozr", wo.at[zl, 0:2, x, c], Z_R)
    got("w_zl", wo.at[zr, :, x, c])
    push("w_ozl", wo.at[zr, 2:4, x, c], Z_L)
    ring_y(1, base1)
    got("d_or", wd.at[2 * xo + c, 0:128])
    push("d_coa", wd.at[2 * xo + c, 0:128], CORE)
    got("d_ol", wd.at[2 * xo + c, 128:256])
    push("d_cob", wd.at[2 * xo + c, 128:256], CORE)
    add(2 * xo + c)
    got("d_coa", wd.at[2 * xo + co, 0:128])
    got("d_cob", wd.at[2 * xo + co, 128:256])
    add(2 * xo + co)

    kvb[y, z, 0:256] = rms_rows(sums[:, QR : QR + KR], klg_ref[...]).astype(BF)
    lq[0] = rms_rows(sums[:, 0:QR], qlg_ref[...]).astype(BF)
    own = kvb.at[y, z]
    push("k_yr", own, Y_R)
    push("k_yl", own, Y_L)
    push("k_zr", own, Z_R)
    push("k_zl", own, Z_L)
    push("q", lq.at[0], dev(zz=zmate), lq.at[1])

    for j, base in ((0, base0), (1, base1)):
        got(f"u_y{j}or", us.at[c, base + yo, 0:2])
        got(f"u_y{j}ol", us.at[c, base + yo, 2:4])
        push(f"u_c{j}o", us.at[c, base + yo], CORE)
    got("w_ozr", wo.at[zo, 0:2, x, c])
    got("w_ozl", wo.at[zo, 2:4, x, c])
    for p in range(2):
        push(f"w_xr{p}", wo.at[2 * p : 2 * p + 2, :, x, c], X_R)
        push(f"w_xl{p}", wo.at[2 * p : 2 * p + 2, :, x, c], X_L)
    for j, base in ((0, base0), (1, base1)):
        got(f"u_c{j}", us.at[co, base + y])
        got(f"u_c{j}l", us.at[co, base + yl])
        got(f"u_c{j}r", us.at[co, base + yr])
        got(f"u_c{j}o", us.at[co, base + yo])
    push("w_c", wo.at[:, :, x, c], CORE)
    prepare_up(us, wq_ref, wk_ref, wv_ref)
    transpose_keys(wk_ref, wkt_ref)
    make_queries(lq[0], sp, wq_ref, qgain_ref[...], lowq_ref, highq_ref, q_ref, 0)
    def k1():
        got("k_yr", kvb.at[yl, z])
        push("k_oyr", lambda: kvb.at[yl, z, 0:160], Y_R)
        got("k_yl", kvb.at[yr, z])
        push("k_oyl", lambda: kvb.at[yr, z, 160:320], Y_L)

    def k2():
        got("k_zr", kvb.at[y, zl])
        push("k_ozr", lambda: kvb.at[y, zl, 0:160], Z_R)
        push("k_y1r", lambda: kvb.at[y, zl], Y_R)
        push("k_y1l", lambda: kvb.at[y, zl], Y_L)
        got("k_zl", kvb.at[y, zr])
        push("k_ozl", lambda: kvb.at[y, zr, 160:320], Z_L)
        push("k_y2r", lambda: kvb.at[y, zr], Y_R)
        push("k_y2l", lambda: kvb.at[y, zr], Y_L)

    def k3():
        got("k_oyr", kvb.at[yo, z, 0:160])
        got("k_oyl", kvb.at[yo, z, 160:320])
        push("k_pzr", lambda: kvb.at[yo, z], Z_R)
        push("k_pzl", lambda: kvb.at[yo, z], Z_L)
        got("k_ozr", kvb.at[y, zo, 0:160])
        got("k_ozl", kvb.at[y, zo, 160:320])
        push("k_y3r", lambda: kvb.at[y, zo], Y_R)
        push("k_y3l", lambda: kvb.at[y, zo], Y_L)

    def k7():
        got("k_y1r", kvb.at[yl, zl])
        got("k_y1l", kvb.at[yr, zl])

    def k9():
        got("k_y2r", kvb.at[yl, zr])
        got("k_y2l", kvb.at[yr, zr])
        got("k_pzr", kvb.at[yo, zl])
        push("k_pozr", lambda: kvb.at[yo, zl, 0:160], Z_R)
        got("k_pzl", kvb.at[yo, zr])
        push("k_pozl", lambda: kvb.at[yo, zr, 160:320], Z_L)

    def k13():
        got("k_y3r", kvb.at[yl, zo])
        got("k_y3l", kvb.at[yr, zo])

    def k15():
        got("k_pozr", kvb.at[yo, zo, 0:160])
        got("k_pozl", kvb.at[yo, zo, 160:320])

    def queries_mate():
        got("q", lq.at[1])
        make_queries(
            lq[1], zmate * 4 + y, wq_ref, qgain_ref[...], lowq_ref, highq_ref, q_ref, 1
        )

    def wx(p):
        def go():
            rng = slice(2 * p, 2 * p + 2)
            got(f"w_xr{p}", wo.at[rng, :, xl, c])
            push(f"w_oxr{p}", lambda: wo.at[2 * p, :, xl, c], X_R)
            push(f"w_cl{p}", lambda: wo.at[rng, :, xl, c], CORE)
            got(f"w_xl{p}", wo.at[rng, :, xr, c])
            push(f"w_oxl{p}", lambda: wo.at[2 * p + 1, :, xr, c], X_L)
            push(f"w_cr{p}", lambda: wo.at[rng, :, xr, c], CORE)

        return go

    def wxo(p):
        got(f"w_oxr{p}", wo.at[2 * p, :, xo, c])
        got(f"w_oxl{p}", wo.at[2 * p + 1, :, xo, c])
        push(f"w_co{p}", lambda: wo.at[2 * p : 2 * p + 2, :, xo, c], CORE)

    hfirst = (z // 2) * LOCAL
    b_own, b_mate = sp, zmate * 4 + y

    def send_mate():
        close_heads(acc_ref, 1, att_ref, HEADS)
        push("att", lambda: att_ref.at[HEADS : HEADS + LOCAL], dev(zz=zmate), att_ref.at[pl.ds(hfirst, LOCAL)])

    def pick(test, yes, no):
        return no + test.astype(jnp.int32) * (yes - no)

    def source(step):
        dy = pick(step < 3, step, pick(step < 6, 0, pick(step == 6, 3, pick(
            step < 11, 1 + (step - 7) % 2, pick(
                step < 13, 3, pick(step < 15, step - 12, 3))))))
        dz = pick(step < 3, 0, pick(step < 6, step - 2, pick(step == 6, 0, pick(
            step < 11, 1 + (step - 7) // 2, pick(step < 13, step - 10, 3)))))
        yy = pick(dy == 0, y, pick(dy == 1, yl, pick(dy == 2, yr, yo)))
        zz = pick(dz == 0, z, pick(dz == 1, zl, pick(dz == 2, zr, zo)))
        return yy, zz, zz * 4 + yy

    b_last = jnp.maximum(b_own, b_mate)

    def expand_step(step, slot):
        yy, zz, b = source(step)

        @pl.when(b <= b_last)
        def _():
            expand(
                kvb[yy, zz], b, wkt_ref, wv_ref, gk_ref, gr_ref, lowk_ref, highk_ref, kt_ref,
                v_ref, slot,
            )

    def attend_step(step, slot, which, bq, diagonal=False):
        b = source(step)[2]

        @pl.when(b == bq if diagonal else b < bq)
        def _():
            attend(diagonal, q_ref, kt_ref, v_ref, m_ref, acc_ref, which, slot)

    def start(step, _):
        @pl.when(step == 1)
        def _():
            k1()

        expand_step(step, step)
        attend_step(step, step, 0, b_own, True)
        return 0

    lax.fori_loop(0, 3, start, 0)
    k2()
    queries_mate()

    def mate_start(step, _):
        attend_step(step, step, 1, b_mate)
        return 0

    lax.fori_loop(0, 3, mate_start, 0)
    k3()
    at_step = {5: (k7,), 7: (wx(0),), 8: (k9,), 12: (k13,), 13: (wx(1),), 15: (k15,)}

    def middle(step, _):
        for when, todo in at_step.items():
            @pl.when(step == when)
            def _(todo=todo):
                for f in todo:
                    f()

        slot = pick(step == 6, 3, 4)
        expand_step(step, slot)

        @pl.when(step != 6)
        def _():
            attend_step(step, slot, 0, b_own)

        attend_step(step, slot, 1, b_mate)
        attend_step(step, slot, 1, b_mate, True)
        return 0

    lax.fori_loop(3, 16, middle, 0)
    send_mate()

    def last(i, _):
        attend_step(pick(i == 3, 6, i), i, 0, b_own)
        return 0

    lax.fori_loop(1, 4, last, 0)
    close_heads(acc_ref, 0, att_ref, hfirst)
    for p in range(2):
        wxo(p)
    got("w_c", wo.at[:, :, x, co])
    for p in range(2):
        got(f"w_cl{p}", wo.at[2 * p : 2 * p + 2, :, xl, co])
        got(f"w_cr{p}", wo.at[2 * p : 2 * p + 2, :, xr, co])
        got(f"w_co{p}", wo.at[2 * p : 2 * p + 2, :, xo, co])
    got("att", att_ref.at[pl.ds(LOCAL - hfirst, LOCAL)])
    finish(att_ref, mixed_ref, ogain_ref, wo, out_ref)
    for i, again in sent:
        view = again()
        pltpu.make_async_copy(view, view, ssem.at[i]).wait()
    assert len(names) <= SLOTS


def per_device(
    tokens, in_gain, w_query_down, w_latent_down, w_rope_key, query_latent_gain, latent_gain,
    w_query_up, w_key_up, w_value_up, query_gain, key_gain, out_gain, w_out,
):
    blocks = lax.axis_size("sp")
    tables = [jnp.asarray(t) for t in rope_tables(blocks)]
    vm = pl.BlockSpec(memory_space=pltpu.VMEM)
    args = (
        tokens.reshape(ROWS, D), in_gain.reshape(1, D), w_query_down, w_latent_down, w_rope_key.T,
        query_latent_gain.reshape(1, QR), latent_gain.reshape(1, KR), w_query_up, w_key_up,
        w_value_up, query_gain.reshape(1, QK), key_gain.reshape(1, QK), out_gain.reshape(1, D), w_out, *tables,
    )
    out = pl.pallas_call(
        kernel,
        out_shape=jax.ShapeDtypeStruct((ROWS, D), BF),
        in_specs=[vm] * len(args),
        out_specs=vm,
        scratch_shapes=[
            pltpu.VMEM((8, 256, QR + KR), BF),
            pltpu.VMEM((2, LOCAL, 4, 96, 256), BF),
            pltpu.VMEM((4, 4, 4, 2, 16, D), BF),
            pltpu.VMEM((4, 4, 320, 256), BF),
            pltpu.VMEM((2, ROWS, QR), BF),
            pltpu.VMEM((8, ROWS, 256), BF),
            pltpu.VMEM((ROWS, QR + KR), F32),
            pltpu.VMEM((LOCAL, QR, 256), BF),
            pltpu.VMEM((LOCAL, KR, NOPE), BF),
            pltpu.VMEM((LOCAL, NOPE, KR), BF),
            pltpu.VMEM((LOCAL, KR, VD), BF),
            pltpu.VMEM((2, LOCAL, ROWS, 256), BF),
            pltpu.VMEM((KEPT, LOCAL, 256, 256), BF),
            pltpu.VMEM((KEPT, LOCAL, 256, 256), BF),
            pltpu.VMEM((2, LOCAL, ROWS, 128), F32),
            pltpu.VMEM((2, LOCAL, ROWS, 256), F32),
            pltpu.VMEM((HEADS + LOCAL, ROWS, VD), BF),
            pltpu.VMEM((ROWS, D), BF),
            pltpu.VMEM((1, 256), F32),
            pltpu.VMEM((NOPE, 256), F32),
            pltpu.VMEM((ROPE, 256), F32),
            pltpu.SemaphoreType.DMA((SLOTS,)),
            pltpu.SemaphoreType.DMA((SLOTS,)),
        ],
        compiler_params=pltpu.CompilerParams(
            vmem_limit_bytes=60 * 1024 * 1024, collective_id=0, has_side_effects=True
        ),
    )(*args)
    return out.reshape(1, ROWS, D)


def solution(mesh):
    in_specs = (
        P("dp", "sp", None), P(), P("dp", None), P("dp", None), P(), P(), P(),
        P("dp", "sp"), P("dp", "sp"), P("dp", "sp"), P(), P(), P(), P(("sp", "dp"), None),
    )
    return jax.shard_map(
        per_device, mesh=mesh, in_specs=in_specs, out_specs=P("dp", "sp", None), check_vma=False
    )
```

```python
import functools

import jax
import jax.numpy as jnp
import numpy as np
from jax import lax
from jax.experimental import pallas as pl
from jax.experimental.pallas import tpu as pltpu
from jax.sharding import PartitionSpec as P

HEADS, NOPE, ROPE, VD, QR, KR, QK = 16, 128, 64, 128, 512, 256, 192
D = 2048
ROWS = 256
EPS = 1e-06
THETA = 10000.0
NEG_BIG = -1e30
BF, F32 = jnp.bfloat16, jnp.float32
SOFT = float(QK**-0.5 * np.log2(np.e))
LOCAL = 8


def rope_tables(blocks):
    half = ROPE // 2
    freq = THETA ** (-np.arange(half) / half)
    low = np.arange(ROWS)[:, None] * freq[None, :]
    high = (np.arange(blocks) * ROWS)[:, None] * freq[None, :]
    pad = np.zeros((ROWS, 128 - ROPE))
    lowq = np.stack([np.concatenate([f(low), f(low), pad], 1) for f in (np.cos, np.sin)])
    hpad = np.zeros((blocks, 128 - ROPE))
    highq = np.stack([np.concatenate([f(high), f(high), hpad], 1) for f in (np.cos, np.sin)], 1)
    highq = np.broadcast_to(highq[:, :, None, :], (blocks, 2, 8, 128))
    lowk = np.concatenate([np.cos(low).T, np.sin(low).T], 0)
    highk = np.concatenate([np.cos(high), np.sin(high)], 1)
    highk = np.broadcast_to(highk[:, :, None], (blocks, ROPE, 128))
    return [np.ascontiguousarray(t, dtype=np.float32) for t in (lowq, highq, lowk, highk)]


def dot(a, b):
    return lax.dot_general(a, b, (((1,), (0,)), ((), ())), preferred_element_type=F32)


def dot_nt(a, b):
    return lax.dot_general(a, b, (((1,), (1,)), ((), ())), preferred_element_type=F32)


def prepare_up(us, wq_ref, wk_ref, wv_ref):
    def one(h, _):
        for x in range(4):
            for c in range(2):
                d = 2 * x + c
                unit = us[c, h, x]
                rows = slice(d * 64, d * 64 + 64)
                wq_ref[h, rows, 0:NOPE] = unit[0:64]
                wq_ref[h, d * 64 : d * 64 + 32, NOPE:QK] = unit[64:96, 0:ROPE]
                wq_ref[h, d * 64 + 32 : d * 64 + 64, NOPE:QK] = unit[64:96, ROPE:128]
                kv_rows = slice(d * 32, d * 32 + 32)
                wk_ref[h, kv_rows] = unit[96:128]
                wv_ref[h, kv_rows] = unit[128:160]
        return 0

    lax.fori_loop(0, LOCAL, one, 0)


def transpose_keys(wk_ref, wkt_ref):
    def one(h, _):
        wkt_ref[h] = wk_ref[h].T
        return 0

    lax.fori_loop(0, LOCAL, one, 0)


def make_queries(latq, block, wq_ref, qgain, lowq_ref, highq_ref, q_ref, which):
    ch, sh = highq_ref[block, 0, 0:1], highq_ref[block, 1, 0:1]
    cl, sl = lowq_ref[0], lowq_ref[1]
    cosine = ch * cl - sh * sl
    sine = sh * cl + ch * sl
    lane = lax.broadcasted_iota(jnp.int32, (ROWS, 128), 1)
    sine_a = jnp.where(lane < ROPE // 2, -sine, 0.0)
    sine_b = jnp.where(lane < ROPE // 2, 0.0, sine)

    for h in range(LOCAL):
        q = dot(latq, wq_ref[h])
        scale = lax.rsqrt(jnp.sum(q * q, axis=1, keepdims=True) * (1.0 / QK) + EPS)
        n = q * scale * qgain
        t = n[:, NOPE:256]
        turned = (
            t * cosine
            + pltpu.roll(t, 128 - ROPE // 2, 1) * sine_a
            + pltpu.roll(t, ROPE // 2, 1) * sine_b
        )
        q_ref[which, h, :, 0:NOPE] = n[:, 0:NOPE].astype(BF)
        q_ref[which, h, :, NOPE:256] = turned.astype(BF)


def expand(unit, block, wkt_ref, wv_ref, gk_ref, gr_ref, lowk_ref, highk_ref, kt_ref, v_ref, slot):
    kv = unit[0:256, :]
    rope = unit[256:320, :].astype(F32)
    half = ROPE // 2
    ch = jnp.concatenate([highk_ref[block, 0:half]] * 2, axis=1)
    sh = jnp.concatenate([highk_ref[block, half:ROPE]] * 2, axis=1)
    cl, sl = lowk_ref[0:half], lowk_ref[half:ROPE]
    cosine = ch * cl - sh * sl
    sine = sh * cl + ch * sl
    rope_sq = jnp.sum(rope * rope, axis=0, keepdims=True)
    x = rope * gr_ref[...]
    a, b = x[0:half], x[half:ROPE]
    turned = jnp.concatenate([a * cosine - b * sine, b * cosine + a * sine], axis=0)
    kt = dot_nt(wkt_ref[...].reshape(LOCAL * NOPE, KR), kv)
    for h in range(LOCAL):
        k = kt[h * NOPE : (h + 1) * NOPE]
        scale = lax.rsqrt((jnp.sum(k * k, axis=0, keepdims=True) + rope_sq) * (1.0 / QK) + EPS)
        kt_ref[slot, h, 0:NOPE] = (k * scale * gk_ref[...]).astype(BF)
        kt_ref[slot, h, NOPE:QK] = (turned * scale).astype(BF)
    for h in range(LOCAL):
        v_ref[slot, h, :, 0:VD] = dot(kv, wv_ref[h]).astype(BF)


def attend(diagonal, q_ref, kt_ref, v_ref, m_ref, acc_ref, which, slot):
    for h in range(LOCAL):
        s = dot(q_ref[which, h], kt_ref[slot, h])
        if diagonal:
            row = lax.broadcasted_iota(jnp.int32, (ROWS, ROWS), 0)
            col = lax.broadcasted_iota(jnp.int32, (ROWS, ROWS), 1)
            s = jnp.where(col <= row, s, NEG_BIG)
        old = m_ref[which, h]
        new = jnp.maximum(old, jnp.max(s, axis=1, keepdims=True))
        fade = jnp.exp2((old - new) * SOFT)
        p = jnp.exp2((s - jnp.concatenate([new, new], 1)) * SOFT).astype(BF)
        m_ref[which, h] = new
        acc_ref[which, h] = acc_ref[which, h] * jnp.concatenate([fade, fade], 1) + dot(
            p, v_ref[slot, h]
        )


def close_heads(acc_ref, which, att_ref, first):
    for h in range(LOCAL):
        att_ref[first + h] = (
            acc_ref[which, h, :, 0:VD] / acc_ref[which, h, :, VD : 2 * VD]
        ).astype(BF)


def finish(att_ref, mixed_ref, ogain_ref, wo_ref, out_ref):
    total = jnp.zeros((ROWS, VD), F32)
    for h in range(HEADS):
        at = att_ref[h].astype(F32)
        total = total + at * at
    scale = lax.rsqrt(jnp.sum(total, axis=1, keepdims=True) * (1.0 / (HEADS * VD)) + EPS)
    for h in range(HEADS):
        cols = slice(h * VD, (h + 1) * VD)
        mixed_ref[:, cols] = (att_ref[h].astype(F32) * scale * ogain_ref[:, cols]).astype(BF)

    def one(j, _):
        cols = pl.ds(pl.multiple_of(j * 512, 512), 512)
        w = wo_ref[:, :, :, :, :, cols].reshape(HEADS * VD, 512)
        out_ref[:, cols] = dot(mixed_ref[...], w).astype(BF)
        return 0

    lax.fori_loop(0, D // 512, one, 0)


def rms_rows(values, scaling):
    return values * lax.rsqrt(jnp.mean(values * values, axis=-1, keepdims=True) + EPS) * scaling


SLOTS = 128
KEPT = 2


def kernel(
    tok_ref, ing_ref, wqd_ref, wld_ref, wrt_ref, qlg_ref, klg_ref, wqu_ref, wku_ref, wvu_ref,
    qg_ref, kg_ref, ogain_ref, wo_in_ref, lowq_ref, highq_ref, lowk_ref, highk_ref,
    out_ref,
    wd, us, wo, kvb, lq, normed, sums, wq_ref, wk_ref, wkt_ref, wv_ref, q_ref, kt_ref, v_ref,
    m_ref, acc_ref, att_ref, mixed_ref, qgain_ref, gk_ref, gr_ref, ssem, rsem,
):
    sp, dp = lax.axis_index("sp"), lax.axis_index("dp")
    z, y = sp // 4, sp % 4
    x, c = dp // 2, dp % 2
    xl, xr, xo = (x + 3) % 4, (x + 1) % 4, (x + 2) % 4
    yl, yr, yo = (y + 3) % 4, (y + 1) % 4, (y + 2) % 4
    zl, zr, zo = (z + 3) % 4, (z + 1) % 4, (z + 2) % 4
    co = 1 - c
    zb = z % 2
    zpair = z + 1 - 2 * zb
    zmate = 3 - z

    def dev(xx=x, yy=y, zz=z, cc=c):
        return {"sp": zz * 4 + yy, "dp": xx * 2 + cc}

    X_R, X_L, Y_R, Y_L, Z_R, Z_L, CORE = (
        dev(xx=xr), dev(xx=xl), dev(yy=yr), dev(yy=yl), dev(zz=zr), dev(zz=zl), dev(cc=co)
    )
    names, sent = {}, []

    def number(name):
        return names.setdefault(name, len(names))

    def push(name, view, to, dst=None):
        i = number(name)
        again = view if callable(view) else functools.partial(lambda v: v, view)
        view = again()
        pltpu.make_async_remote_copy(
            src_ref=view, dst_ref=view if dst is None else dst, send_sem=ssem.at[i],
            recv_sem=rsem.at[i], device_id=to, device_id_type=pl.DeviceIdType.MESH,
        ).start()
        sent.append((i, again))

    def got(name, view):
        pltpu.make_async_copy(view, view, rsem.at[number(name)]).wait()

    barrier = pltpu.get_barrier_semaphore()
    X_O, Y_O = dev(xx=xo), dev(yy=yo)
    for to in (X_R, X_L, X_O, Y_R, Y_L, Y_O, Z_R, Z_L, CORE):
        pl.semaphore_signal(barrier, 1, device_id=to, device_id_type=pl.DeviceIdType.MESH)

    hl = zb * 4 + y
    us[c, hl, x, 0:64] = wqu_ref[:, 0:NOPE]
    us[c, hl, x, 64:96] = jnp.concatenate(
        [wqu_ref[0:32, NOPE:QK], wqu_ref[32:64, NOPE:QK]], axis=1
    )
    us[c, hl, x, 96:128] = wku_ref[...]
    us[c, hl, x, 128:160] = wvu_ref[...]
    wo[z, y, x, c] = wo_in_ref[...]
    wd[dp, :, 0:QR] = wqd_ref[...]
    wd[dp, :, QR : QR + KR] = wld_ref[...]
    pl.semaphore_wait(barrier, 9)

    uown = us.at[c, hl, x]
    push("u_r", uown, X_R)
    push("u_l", uown, X_L)
    push("u_o", uown, X_O)
    wown = wo.at[z, y, x, c]
    push("w_yr", wown, Y_R)
    push("w_yl", wown, Y_L)
    push("w_yo", wown, Y_O)
    down = wd.at[dp]
    push("d_r", down, X_R)
    push("d_l", down, X_L)
    push("d_c", down, CORE)

    for r in range(0, ROWS, 64):
        rows = slice(r, r + 64)
        n = rms_rows(tok_ref[rows].astype(F32), ing_ref[...]).astype(BF)
        for k in range(8):
            normed[k, rows] = n[:, k * 256 : (k + 1) * 256]

    qgain_ref[:, 0:NOPE] = qg_ref[:, 0:NOPE]
    qgain_ref[:, NOPE:256] = jnp.concatenate(
        [qg_ref[:, NOPE:QK], jnp.zeros((1, 256 - QK), F32)], axis=1
    )
    kg = jnp.concatenate([kg_ref[...], jnp.zeros((1, 256 - QK), F32)], axis=1)
    column = jnp.broadcast_to(kg[:, 0:NOPE], (NOPE, NOPE)).T
    gk_ref[...] = jnp.concatenate([column, column], axis=1)
    column = jnp.broadcast_to(kg[:, NOPE:256], (NOPE, NOPE)).T[0:ROPE]
    gr_ref[...] = jnp.concatenate([column, column], axis=1)

    got("u_r", us.at[c, hl, xl])
    got("u_l", us.at[c, hl, xr])
    got("u_o", us.at[c, hl, xo])
    block0 = us.at[c, hl]
    push("u_z", block0, dev(zz=zpair))
    push("u_y0r", block0, Y_R)
    push("u_y0l", block0, Y_L)
    push("u_c0", block0, CORE)
    got("w_yr", wo.at[z, yl, x, c])
    got("w_yl", wo.at[z, yr, x, c])
    got("w_yo", wo.at[z, yo, x, c])
    push("w_zr", wo.at[z, :, x, c], Z_R)
    push("w_zl", wo.at[z, :, x, c], Z_L)

    def add(d, first=False):
        part = dot(normed[d], wd[d])
        if first:
            sums[...] = part
        else:
            sums[...] += part

    add(dp, True)
    got("d_c", wd.at[2 * x + co])
    add(2 * x + co)
    m_ref[...] = jnp.full(m_ref.shape, NEG_BIG, F32)
    acc_ref[...] = jnp.zeros(acc_ref.shape, F32)
    wq_ref[:, :, QK:256] = jnp.zeros((LOCAL, QR, 256 - QK), BF)
    kt_ref[:, :, QK:256, :] = jnp.zeros((KEPT, LOCAL, 256 - QK, 256), BF)
    v_ref[:, :, :, VD:256] = jnp.ones((KEPT, LOCAL, ROWS, 256 - VD), BF)
    rope_t = jnp.zeros((ROPE, ROWS), F32)
    for k in range(8):
        rope_t = rope_t + dot_nt(wrt_ref[:, k * 256 : (k + 1) * 256], normed[k])
    kvb[y, z, 256:320] = rope_t.astype(BF)
    base0, base1 = zb * 4, 4 - zb * 4
    block1 = us.at[c, base1 + y]

    def ring_y(j, base):
        got(f"u_y{j}r", us.at[c, base + yl])
        push(f"u_y{j}or", us.at[c, base + yl, 0:2], Y_R)
        push(f"u_c{j}l", us.at[c, base + yl], CORE)
        got(f"u_y{j}l", us.at[c, base + yr])
        push(f"u_y{j}ol", us.at[c, base + yr, 2:4], Y_L)
        push(f"u_c{j}r", us.at[c, base + yr], CORE)

    ring_y(0, base0)
    got("u_z", us.at[c, base1 + y])
    push("u_y1r", block1, Y_R)
    push("u_y1l", block1, Y_L)
    push("u_c1", block1, CORE)
    got("d_r", wd.at[2 * xl + c])
    push("d_or", wd.at[2 * xl + c, 0:128], X_R)
    push("d_cl", wd.at[2 * xl + c], CORE)
    got("d_l", wd.at[2 * xr + c])
    push("d_ol", wd.at[2 * xr + c, 128:256], X_L)
    push("d_cr", wd.at[2 * xr + c], CORE)
    add(2 * xl + c)
    add(2 * xr + c)
    got("d_cl", wd.at[2 * xl + co])
    add(2 * xl + co)
    got("d_cr", wd.at[2 * xr + co])
    add(2 * xr + co)
    zrow = (z, zl, zr, zo)

    def row(k):
        push(f"w_xr{k}", wo.at[zrow[k], :, x, c], X_R)
        push(f"w_xl{k}", wo.at[zrow[k], :, x, c], X_L)

    row(0)
    got("w_zr", wo.at[zl, :, x, c])
    push("w_ozr", wo.at[zl, 0:2, x, c], Z_R)
    got("w_zl", wo.at[zr, :, x, c])
    push("w_ozl", wo.at[zr, 2:4, x, c], Z_L)
    row(1)
    row(2)
    got("d_or", wd.at[2 * xo + c, 0:128])
    push("d_coa", wd.at[2 * xo + c, 0:128], CORE)
    got("d_ol", wd.at[2 * xo + c, 128:256])
    push("d_cob", wd.at[2 * xo + c, 128:256], CORE)
    add(2 * xo + c)
    got("d_coa", wd.at[2 * xo + co, 0:128])
    got("d_cob", wd.at[2 * xo + co, 128:256])
    add(2 * xo + co)

    lq[0] = rms_rows(sums[:, 0:QR], qlg_ref[...]).astype(BF)
    push("q", lq.at[0], dev(zz=zmate), lq.at[1])
    kvb[y, z, 0:256] = rms_rows(sums[:, QR : QR + KR], klg_ref[...]).astype(BF)
    own = kvb.at[y, z]
    push("k_yr", own, Y_R)
    push("k_yl", own, Y_L)
    push("k_zr", own, Z_R)
    push("k_zl", own, Z_L)

    ring_y(1, base1)
    for j, base in ((0, base0), (1, base1)):
        got(f"u_y{j}or", us.at[c, base + yo, 0:2])
        got(f"u_y{j}ol", us.at[c, base + yo, 2:4])
        push(f"u_c{j}o", us.at[c, base + yo], CORE)
    got("w_ozr", wo.at[zo, 0:2, x, c])
    got("w_ozl", wo.at[zo, 2:4, x, c])
    row(3)
    for j, base in ((0, base0), (1, base1)):
        got(f"u_c{j}", us.at[co, base + y])
        got(f"u_c{j}l", us.at[co, base + yl])
        got(f"u_c{j}r", us.at[co, base + yr])
        got(f"u_c{j}o", us.at[co, base + yo])
    push("w_c", wo.at[:, :, x, c], CORE)
    prepare_up(us, wq_ref, wk_ref, wv_ref)
    transpose_keys(wk_ref, wkt_ref)
    make_queries(lq[0], sp, wq_ref, qgain_ref[...], lowq_ref, highq_ref, q_ref, 0)
    def k1():
        got("k_yr", kvb.at[yl, z])
        push("k_oyr", lambda: kvb.at[yl, z, 0:160], Y_R)
        got("k_yl", kvb.at[yr, z])
        push("k_oyl", lambda: kvb.at[yr, z, 160:320], Y_L)

    def k2():
        got("k_zr", kvb.at[y, zl])
        push("k_ozr", lambda: kvb.at[y, zl, 0:160], Z_R)
        push("k_y1r", lambda: kvb.at[y, zl], Y_R)
        push("k_y1l", lambda: kvb.at[y, zl], Y_L)
        got("k_zl", kvb.at[y, zr])
        push("k_ozl", lambda: kvb.at[y, zr, 160:320], Z_L)
        push("k_y2r", lambda: kvb.at[y, zr], Y_R)
        push("k_y2l", lambda: kvb.at[y, zr], Y_L)

    def k3():
        got("k_oyr", kvb.at[yo, z, 0:160])
        got("k_oyl", kvb.at[yo, z, 160:320])
        push("k_pzr", lambda: kvb.at[yo, z], Z_R)
        push("k_pzl", lambda: kvb.at[yo, z], Z_L)
        got("k_ozr", kvb.at[y, zo, 0:160])
        got("k_ozl", kvb.at[y, zo, 160:320])
        push("k_y3r", lambda: kvb.at[y, zo], Y_R)
        push("k_y3l", lambda: kvb.at[y, zo], Y_L)

    def k7():
        got("k_y1r", kvb.at[yl, zl])
        got("k_y1l", kvb.at[yr, zl])

    def k9():
        got("k_y2r", kvb.at[yl, zr])
        got("k_y2l", kvb.at[yr, zr])

    def k11():
        got("k_pzr", kvb.at[yo, zl])
        push("k_pozr", lambda: kvb.at[yo, zl, 0:160], Z_R)
        got("k_pzl", kvb.at[yo, zr])
        push("k_pozl", lambda: kvb.at[yo, zr, 160:320], Z_L)

    def k13():
        got("k_y3r", kvb.at[yl, zo])
        got("k_y3l", kvb.at[yr, zo])

    def k15():
        got("k_pozr", kvb.at[yo, zo, 0:160])
        got("k_pozl", kvb.at[yo, zo, 160:320])

    def queries_mate():
        got("q", lq.at[1])
        make_queries(
            lq[1], zmate * 4 + y, wq_ref, qgain_ref[...], lowq_ref, highq_ref, q_ref, 1
        )

    def wx(k):
        def go():
            r = zrow[k]
            got(f"w_xr{k}", wo.at[r, :, xl, c])
            push(f"w_oxr{k}", lambda: wo.at[r, 0:2, xl, c], X_R)
            push(f"w_cl{k}", lambda: wo.at[r, :, xl, c], CORE)
            got(f"w_xl{k}", wo.at[r, :, xr, c])
            push(f"w_oxl{k}", lambda: wo.at[r, 2:4, xr, c], X_L)
            push(f"w_cr{k}", lambda: wo.at[r, :, xr, c], CORE)

        return go

    def wxo(k):
        r = zrow[k]
        got(f"w_oxr{k}", wo.at[r, 0:2, xo, c])
        got(f"w_oxl{k}", wo.at[r, 2:4, xo, c])
        push(f"w_co{k}", wo.at[r, :, xo, c], CORE)

    hfirst = (z // 2) * LOCAL
    b_own, b_mate = sp, zmate * 4 + y

    def send_mate():
        close_heads(acc_ref, 1, att_ref, HEADS)
        push("att", lambda: att_ref.at[HEADS : HEADS + LOCAL], dev(zz=zmate), att_ref.at[pl.ds(hfirst, LOCAL)])

    def pick(test, yes, no):
        return no + test.astype(jnp.int32) * (yes - no)

    def source(step):
        dy = pick(step < 3, step, pick(step < 6, 0, pick(step == 6, 3, pick(
            step < 11, 1 + (step - 7) % 2, pick(
                step < 13, 3, pick(step < 15, step - 12, 3))))))
        dz = pick(step < 3, 0, pick(step < 6, step - 2, pick(step == 6, 0, pick(
            step < 11, 1 + (step - 7) // 2, pick(step < 13, step - 10, 3)))))
        yy = pick(dy == 0, y, pick(dy == 1, yl, pick(dy == 2, yr, yo)))
        zz = pick(dz == 0, z, pick(dz == 1, zl, pick(dz == 2, zr, zo)))
        return yy, zz, zz * 4 + yy

    b_last = jnp.maximum(b_own, b_mate)

    def expand_step(step, slot):
        yy, zz, b = source(step)
        expand(
            kvb[yy, zz], b, wkt_ref, wv_ref, gk_ref, gr_ref, lowk_ref, highk_ref, kt_ref,
            v_ref, slot,
        )

    def attend_to(which, slot, diagonal=False):
        attend(diagonal, q_ref, kt_ref, v_ref, m_ref, acc_ref, which, slot)

    expand_step(jnp.minimum(z, 0), 0)
    attend_to(0, 0, True)
    queries_mate()
    at_pair = {0: (k1, wx(0)), 1: (k2,), 2: (k3, wx(1)), 3: (k7, k11), 4: (k9, wx(2)), 6: (k13,),
               7: (k15, wx(3))}

    def pair(i, _):
        for when, todo in at_pair.items():
            @pl.when(i == when)
            def _(todo=todo):
                for f in todo:
                    f()

        first = pick(i == 7, 0, 2 * i + 1)
        second = pick(i == 7, 15, 2 * i + 2)
        b0, b1 = source(first)[2], source(second)[2]
        own_both = (b0 < b_own) & (b1 < b_own)
        mate_both = (b0 < b_mate) & (b1 < b_mate)
        either = own_both | mate_both
        needed = (b0 <= b_last) | (b1 <= b_last)
        lead = pick(own_both, 0, 1)

        @pl.when(either)
        def _():
            expand_step(first, 0)
            expand_step(second, 1)
            attend_to(lead, 0)
            attend_to(lead, 1)

        @pl.when(jnp.logical_not(either) & needed)
        def _():
            expand_step(first, 0)
            expand_step(second, 1)

        @pl.when(own_both & mate_both)
        def _():
            attend_to(1, 0)
            attend_to(1, 1)

        def single(j, _):
            which, slot = j // 2, j % 2
            b = pick(slot == 0, b0, b1)
            bq = pick(which == 0, b_own, b_mate)
            done = pick(which == 0, own_both.astype(jnp.int32), mate_both.astype(jnp.int32))

            @pl.when((b < bq) & (done == 0))
            def _():
                attend_to(which, slot)

            @pl.when((b == bq) & (which == 1))
            def _():
                attend_to(which, slot, True)

            return 0

        @pl.when(jnp.logical_not(own_both & mate_both))
        def _():
            lax.fori_loop(0, 4, single, 0)

        return 0

    lax.fori_loop(0, 8, pair, 0)
    send_mate()
    close_heads(acc_ref, 0, att_ref, hfirst)
    for k in range(4):
        wxo(k)
    got("w_c", wo.at[:, :, x, co])
    for k in range(4):
        got(f"w_cl{k}", wo.at[zrow[k], :, xl, co])
        got(f"w_cr{k}", wo.at[zrow[k], :, xr, co])
        got(f"w_co{k}", wo.at[zrow[k], :, xo, co])
    got("att", att_ref.at[pl.ds(LOCAL - hfirst, LOCAL)])
    finish(att_ref, mixed_ref, ogain_ref, wo, out_ref)
    for i, again in sent:
        view = again()
        pltpu.make_async_copy(view, view, ssem.at[i]).wait()
    assert len(names) <= SLOTS


def per_device(
    tokens, in_gain, w_query_down, w_latent_down, w_rope_key, query_latent_gain, latent_gain,
    w_query_up, w_key_up, w_value_up, query_gain, key_gain, out_gain, w_out,
):
    blocks = lax.axis_size("sp")
    tables = [jnp.asarray(t) for t in rope_tables(blocks)]
    vm = pl.BlockSpec(memory_space=pltpu.VMEM)
    args = (
        tokens.reshape(ROWS, D), in_gain.reshape(1, D), w_query_down, w_latent_down, w_rope_key.T,
        query_latent_gain.reshape(1, QR), latent_gain.reshape(1, KR), w_query_up, w_key_up,
        w_value_up, query_gain.reshape(1, QK), key_gain.reshape(1, QK), out_gain.reshape(1, D), w_out, *tables,
    )
    out = pl.pallas_call(
        kernel,
        out_shape=jax.ShapeDtypeStruct((ROWS, D), BF),
        in_specs=[vm] * len(args),
        out_specs=vm,
        scratch_shapes=[
            pltpu.VMEM((8, 256, QR + KR), BF),
            pltpu.VMEM((2, LOCAL, 4, 160, 128), BF),
            pltpu.VMEM((4, 4, 4, 2, 16, D), BF),
            pltpu.VMEM((4, 4, 320, 256), BF),
            pltpu.VMEM((2, ROWS, QR), BF),
            pltpu.VMEM((8, ROWS, 256), BF),
            pltpu.VMEM((ROWS, QR + KR), F32),
            pltpu.VMEM((LOCAL, QR, 256), BF),
            pltpu.VMEM((LOCAL, KR, NOPE), BF),
            pltpu.VMEM((LOCAL, NOPE, KR), BF),
            pltpu.VMEM((LOCAL, KR, VD), BF),
            pltpu.VMEM((2, LOCAL, ROWS, 256), BF),
            pltpu.VMEM((KEPT, LOCAL, 256, 256), BF),
            pltpu.VMEM((KEPT, LOCAL, 256, 256), BF),
            pltpu.VMEM((2, LOCAL, ROWS, 128), F32),
            pltpu.VMEM((2, LOCAL, ROWS, 256), F32),
            pltpu.VMEM((HEADS + LOCAL, ROWS, VD), BF),
            pltpu.VMEM((ROWS, D), BF),
            pltpu.VMEM((1, 256), F32),
            pltpu.VMEM((NOPE, 256), F32),
            pltpu.VMEM((ROPE, 256), F32),
            pltpu.SemaphoreType.DMA((SLOTS,)),
            pltpu.SemaphoreType.DMA((SLOTS,)),
        ],
        compiler_params=pltpu.CompilerParams(
            vmem_limit_bytes=60 * 1024 * 1024, collective_id=0, has_side_effects=True
        ),
    )(*args)
    return out.reshape(1, ROWS, D)


def solution(mesh):
    in_specs = (
        P("dp", "sp", None), P(), P("dp", None), P("dp", None), P(), P(), P(),
        P("dp", "sp"), P("dp", "sp"), P("dp", "sp"), P(), P(), P(), P(("sp", "dp"), None),
    )
    return jax.shard_map(
        per_device, mesh=mesh, in_specs=in_specs, out_specs=P("dp", "sp", None), check_vma=False
    )
```

```python
import functools

import jax
import jax.numpy as jnp
import numpy as np
from jax import lax
from jax.experimental import pallas as pl
from jax.experimental.pallas import tpu as pltpu
from jax.sharding import PartitionSpec as P

HEADS, NOPE, ROPE, VD, QR, KR, QK = 16, 128, 64, 128, 512, 256, 192
D = 2048
ROWS = 256
EPS = 1e-06
THETA = 10000.0
NEG_BIG = -1e30
BF, F32 = jnp.bfloat16, jnp.float32
SOFT = float(QK**-0.5 * np.log2(np.e))
LOCAL = 8


def rope_tables(blocks):
    half = ROPE // 2
    freq = THETA ** (-np.arange(half) / half)
    low = np.arange(ROWS)[:, None] * freq[None, :]
    high = (np.arange(blocks) * ROWS)[:, None] * freq[None, :]
    pad = np.zeros((ROWS, 128 - ROPE))
    lowq = np.stack([np.concatenate([f(low), f(low), pad], 1) for f in (np.cos, np.sin)])
    hpad = np.zeros((blocks, 128 - ROPE))
    highq = np.stack([np.concatenate([f(high), f(high), hpad], 1) for f in (np.cos, np.sin)], 1)
    highq = np.broadcast_to(highq[:, :, None, :], (blocks, 2, 8, 128))
    lowk = np.concatenate([np.cos(low).T, np.sin(low).T], 0)
    highk = np.concatenate([np.cos(high), np.sin(high)], 1)
    highk = np.broadcast_to(highk[:, :, None], (blocks, ROPE, 128))
    return [np.ascontiguousarray(t, dtype=np.float32) for t in (lowq, highq, lowk, highk)]


def dot(a, b):
    return lax.dot_general(a, b, (((1,), (0,)), ((), ())), preferred_element_type=F32)


def dot_nt(a, b):
    return lax.dot_general(a, b, (((1,), (1,)), ((), ())), preferred_element_type=F32)


def prepare_head(us, h, wq_ref, wkt_ref, wv_ref):
    keys = []
    for x in range(4):
        for c in range(2):
            d = 2 * x + c
            unit = us[c, h, x]
            rows = slice(d * 64, d * 64 + 64)
            wq_ref[h, rows, 0:NOPE] = unit[0:64]
            wq_ref[h, d * 64 : d * 64 + 32, NOPE:QK] = unit[64:96, 0:ROPE]
            wq_ref[h, d * 64 + 32 : d * 64 + 64, NOPE:QK] = unit[64:96, ROPE:128]
            keys.append(unit[96:128])
            wv_ref[h, d * 32 : d * 32 + 32] = unit[128:160]
    wkt_ref[h] = jnp.concatenate(keys, axis=0).T


def make_queries(latq, block, wq_ref, qgain, lowq_ref, highq_ref, q_ref, which):
    ch, sh = highq_ref[block, 0, 0:1], highq_ref[block, 1, 0:1]
    cl, sl = lowq_ref[0], lowq_ref[1]
    cosine = ch * cl - sh * sl
    sine = sh * cl + ch * sl
    lane = lax.broadcasted_iota(jnp.int32, (ROWS, 128), 1)
    sine_a = jnp.where(lane < ROPE // 2, -sine, 0.0)
    sine_b = jnp.where(lane < ROPE // 2, 0.0, sine)

    for h in range(LOCAL):
        q = dot(latq, wq_ref[h])
        scale = lax.rsqrt(jnp.sum(q * q, axis=1, keepdims=True) * (1.0 / QK) + EPS)
        n = q * scale * qgain
        t = n[:, NOPE:256]
        turned = (
            t * cosine
            + pltpu.roll(t, 128 - ROPE // 2, 1) * sine_a
            + pltpu.roll(t, ROPE // 2, 1) * sine_b
        )
        q_ref[which, h, :, 0:NOPE] = n[:, 0:NOPE].astype(BF)
        q_ref[which, h, :, NOPE:256] = turned.astype(BF)


def expand(unit, block, wkt_ref, wv_ref, gk_ref, gr_ref, lowk_ref, highk_ref, kt_ref, v_ref, slot):
    kv = unit[0:256, :]
    rope = unit[256:320, :].astype(F32)
    half = ROPE // 2
    ch = jnp.concatenate([highk_ref[block, 0:half]] * 2, axis=1)
    sh = jnp.concatenate([highk_ref[block, half:ROPE]] * 2, axis=1)
    cl, sl = lowk_ref[0:half], lowk_ref[half:ROPE]
    cosine = ch * cl - sh * sl
    sine = sh * cl + ch * sl
    rope_sq = jnp.sum(rope * rope, axis=0, keepdims=True)
    x = rope * gr_ref[...]
    a, b = x[0:half], x[half:ROPE]
    turned = jnp.concatenate([a * cosine - b * sine, b * cosine + a * sine], axis=0)
    kt = dot_nt(wkt_ref[...].reshape(LOCAL * NOPE, KR), kv)
    for h in range(LOCAL):
        k = kt[h * NOPE : (h + 1) * NOPE]
        scale = lax.rsqrt((jnp.sum(k * k, axis=0, keepdims=True) + rope_sq) * (1.0 / QK) + EPS)
        kt_ref[slot, h, 0:NOPE] = (k * scale * gk_ref[...]).astype(BF)
        kt_ref[slot, h, NOPE:QK] = (turned * scale).astype(BF)
    for h in range(LOCAL):
        v_ref[slot, h, :, 0:VD] = dot(kv, wv_ref[h]).astype(BF)


def attend(diagonal, q_ref, kt_ref, v_ref, m_ref, acc_ref, which, slot):
    for h in range(LOCAL):
        s = dot(q_ref[which, h], kt_ref[slot, h])
        if diagonal:
            row = lax.broadcasted_iota(jnp.int32, (ROWS, ROWS), 0)
            col = lax.broadcasted_iota(jnp.int32, (ROWS, ROWS), 1)
            s = jnp.where(col <= row, s, NEG_BIG)
        old = m_ref[which, h]
        new = jnp.maximum(old, jnp.max(s, axis=1, keepdims=True))
        fade = jnp.exp2((old - new) * SOFT)
        p = jnp.exp2((s - jnp.concatenate([new, new], 1)) * SOFT).astype(BF)
        m_ref[which, h] = new
        acc_ref[which, h] = acc_ref[which, h] * jnp.concatenate([fade, fade], 1) + dot(
            p, v_ref[slot, h]
        )


def attend_pair(q_ref, kt_ref, v_ref, m_ref, acc_ref, which):
    for h in range(LOCAL):
        q = q_ref[which, h]
        s0, s1 = dot(q, kt_ref[0, h]), dot(q, kt_ref[1, h])
        old = m_ref[which, h]
        new = jnp.maximum(old, jnp.max(jnp.maximum(s0, s1), axis=1, keepdims=True))
        fade = jnp.exp2((old - new) * SOFT)
        wide = jnp.concatenate([new, new], 1)
        p0 = jnp.exp2((s0 - wide) * SOFT).astype(BF)
        p1 = jnp.exp2((s1 - wide) * SOFT).astype(BF)
        m_ref[which, h] = new
        acc_ref[which, h] = acc_ref[which, h] * jnp.concatenate([fade, fade], 1) + (
            dot(p0, v_ref[0, h]) + dot(p1, v_ref[1, h])
        )


def close_heads(acc_ref, which, att_ref, first):
    for h in range(LOCAL):
        att_ref[first + h] = (
            acc_ref[which, h, :, 0:VD] / acc_ref[which, h, :, VD : 2 * VD]
        ).astype(BF)


def finish(att_ref, mixed_ref, ogain_ref, wo_ref, out_ref):
    total = jnp.zeros((ROWS, VD), F32)
    for h in range(HEADS):
        at = att_ref[h].astype(F32)
        total = total + at * at
    scale = lax.rsqrt(jnp.sum(total, axis=1, keepdims=True) * (1.0 / (HEADS * VD)) + EPS)
    for h in range(HEADS):
        cols = slice(h * VD, (h + 1) * VD)
        mixed_ref[:, cols] = (att_ref[h].astype(F32) * scale * ogain_ref[:, cols]).astype(BF)

    def one(j, _):
        cols = pl.ds(pl.multiple_of(j * 512, 512), 512)
        w = wo_ref[:, :, :, :, :, cols].reshape(HEADS * VD, 512)
        out_ref[:, cols] = dot(mixed_ref[...], w).astype(BF)
        return 0

    lax.fori_loop(0, D // 512, one, 0)


def rms_rows(values, scaling):
    return values * lax.rsqrt(jnp.mean(values * values, axis=-1, keepdims=True) + EPS) * scaling


SLOTS = 128
KEPT = 2


def kernel(
    tok_ref, ing_ref, wqd_ref, wld_ref, wrt_ref, qlg_ref, klg_ref, wqu_ref, wku_ref, wvu_ref,
    qg_ref, kg_ref, ogain_ref, wo_in_ref, lowq_ref, highq_ref, lowk_ref, highk_ref,
    out_ref,
    wd, us, wo, kvb, lq, normed, sums, wq_ref, wkt_ref, wv_ref, q_ref, kt_ref, v_ref,
    m_ref, acc_ref, att_ref, mixed_ref, qgain_ref, gk_ref, gr_ref, ssem, rsem,
):
    sp, dp = lax.axis_index("sp"), lax.axis_index("dp")
    z, y = sp // 4, sp % 4
    x, c = dp // 2, dp % 2
    xl, xr, xo = (x + 3) % 4, (x + 1) % 4, (x + 2) % 4
    yl, yr, yo = (y + 3) % 4, (y + 1) % 4, (y + 2) % 4
    zl, zr, zo = (z + 3) % 4, (z + 1) % 4, (z + 2) % 4
    co = 1 - c
    zb = z % 2
    zpair = z + 1 - 2 * zb
    zmate = 3 - z

    def dev(xx=x, yy=y, zz=z, cc=c):
        return {"sp": zz * 4 + yy, "dp": xx * 2 + cc}

    X_R, X_L, Y_R, Y_L, Z_R, Z_L, CORE = (
        dev(xx=xr), dev(xx=xl), dev(yy=yr), dev(yy=yl), dev(zz=zr), dev(zz=zl), dev(cc=co)
    )
    names, sent = {}, []

    def number(name):
        return names.setdefault(name, len(names))

    def push(name, view, to, dst=None):
        i = number(name)
        again = view if callable(view) else functools.partial(lambda v: v, view)
        view = again()
        pltpu.make_async_remote_copy(
            src_ref=view, dst_ref=view if dst is None else dst, send_sem=ssem.at[i],
            recv_sem=rsem.at[i], device_id=to, device_id_type=pl.DeviceIdType.MESH,
        ).start()
        sent.append((i, again))

    def got(name, view):
        pltpu.make_async_copy(view, view, rsem.at[number(name)]).wait()

    barrier = pltpu.get_barrier_semaphore()
    X_O, Y_O = dev(xx=xo), dev(yy=yo)
    for to in (X_R, X_L, X_O, Y_R, Y_L, Y_O, Z_R, Z_L, CORE):
        pl.semaphore_signal(barrier, 1, device_id=to, device_id_type=pl.DeviceIdType.MESH)

    hl = zb * 4 + y
    us[c, hl, x, 0:64] = wqu_ref[:, 0:NOPE]
    us[c, hl, x, 64:96] = jnp.concatenate(
        [wqu_ref[0:32, NOPE:QK], wqu_ref[32:64, NOPE:QK]], axis=1
    )
    us[c, hl, x, 96:128] = wku_ref[...]
    us[c, hl, x, 128:160] = wvu_ref[...]
    wo[z, y, x, c] = wo_in_ref[...]
    wd[dp, :, 0:QR] = wqd_ref[...]
    wd[dp, :, QR : QR + KR] = wld_ref[...]
    pl.semaphore_wait(barrier, 9)

    uown = us.at[c, hl, x]
    push("u_r", uown, X_R)
    push("u_l", uown, X_L)
    push("u_o", uown, X_O)
    wown = wo.at[z, y, x, c]
    push("w_yr", wown, Y_R)
    push("w_yl", wown, Y_L)
    push("w_yo", wown, Y_O)
    down = wd.at[dp]
    push("d_r", down, X_R)
    push("d_l", down, X_L)
    push("d_c", down, CORE)

    for r in range(0, ROWS, 64):
        rows = slice(r, r + 64)
        n = rms_rows(tok_ref[rows].astype(F32), ing_ref[...]).astype(BF)
        for k in range(8):
            normed[k, rows] = n[:, k * 256 : (k + 1) * 256]

    qgain_ref[:, 0:NOPE] = qg_ref[:, 0:NOPE]
    qgain_ref[:, NOPE:256] = jnp.concatenate(
        [qg_ref[:, NOPE:QK], jnp.zeros((1, 256 - QK), F32)], axis=1
    )
    kg = jnp.concatenate([kg_ref[...], jnp.zeros((1, 256 - QK), F32)], axis=1)
    column = jnp.broadcast_to(kg[:, 0:NOPE], (NOPE, NOPE)).T
    gk_ref[...] = jnp.concatenate([column, column], axis=1)
    column = jnp.broadcast_to(kg[:, NOPE:256], (NOPE, NOPE)).T[0:ROPE]
    gr_ref[...] = jnp.concatenate([column, column], axis=1)

    got("u_r", us.at[c, hl, xl])
    got("u_l", us.at[c, hl, xr])
    got("u_o", us.at[c, hl, xo])
    block0 = us.at[c, hl]
    push("u_z", block0, dev(zz=zpair))
    push("u_y0r", block0, Y_R)
    push("u_y0l", block0, Y_L)
    push("u_c0", block0, CORE)
    got("w_yr", wo.at[z, yl, x, c])
    got("w_yl", wo.at[z, yr, x, c])
    got("w_yo", wo.at[z, yo, x, c])
    push("w_zr", wo.at[z, :, x, c], Z_R)
    push("w_zl", wo.at[z, :, x, c], Z_L)

    def add(d, first=False):
        part = dot(normed[d], wd[d])
        if first:
            sums[...] = part
        else:
            sums[...] += part

    add(dp, True)
    got("d_c", wd.at[2 * x + co])
    add(2 * x + co)
    m_ref[...] = jnp.full(m_ref.shape, NEG_BIG, F32)
    acc_ref[...] = jnp.zeros(acc_ref.shape, F32)
    wq_ref[:, :, QK:256] = jnp.zeros((LOCAL, QR, 256 - QK), BF)
    kt_ref[:, :, QK:256, :] = jnp.zeros((KEPT, LOCAL, 256 - QK, 256), BF)
    v_ref[:, :, :, VD:256] = jnp.ones((KEPT, LOCAL, ROWS, 256 - VD), BF)
    rope_t = jnp.zeros((ROPE, ROWS), F32)
    for k in range(8):
        rope_t = rope_t + dot_nt(wrt_ref[:, k * 256 : (k + 1) * 256], normed[k])
    kvb[y, z, 256:320] = rope_t.astype(BF)
    base0, base1 = zb * 4, 4 - zb * 4
    block1 = us.at[c, base1 + y]

    def ring_y(j, base):
        got(f"u_y{j}r", us.at[c, base + yl])
        push(f"u_y{j}or", us.at[c, base + yl, 0:2], Y_R)
        push(f"u_c{j}l", us.at[c, base + yl], CORE)
        got(f"u_y{j}l", us.at[c, base + yr])
        push(f"u_y{j}ol", us.at[c, base + yr, 2:4], Y_L)
        push(f"u_c{j}r", us.at[c, base + yr], CORE)

    got("u_z", us.at[c, base1 + y])
    push("u_y1r", block1, Y_R)
    push("u_y1l", block1, Y_L)
    push("u_c1", block1, CORE)
    ring_y(0, base0)
    got("d_r", wd.at[2 * xl + c])
    push("d_or", wd.at[2 * xl + c, 0:128], X_R)
    push("d_cl", wd.at[2 * xl + c], CORE)
    got("d_l", wd.at[2 * xr + c])
    push("d_ol", wd.at[2 * xr + c, 128:256], X_L)
    push("d_cr", wd.at[2 * xr + c], CORE)
    add(2 * xl + c)
    add(2 * xr + c)
    got("d_cl", wd.at[2 * xl + co])
    add(2 * xl + co)
    got("d_cr", wd.at[2 * xr + co])
    add(2 * xr + co)
    zrow = (z, zl, zr, zo)

    def row(k):
        push(f"w_xr{k}", wo.at[zrow[k], :, x, c], X_R)
        push(f"w_xl{k}", wo.at[zrow[k], :, x, c], X_L)

    row(0)
    got("w_zr", wo.at[zl, :, x, c])
    push("w_ozr", wo.at[zl, 0:2, x, c], Z_R)
    got("w_zl", wo.at[zr, :, x, c])
    push("w_ozl", wo.at[zr, 2:4, x, c], Z_L)
    row(1)
    row(2)
    got("u_c0", us.at[co, base0 + y])
    got("u_c1", us.at[co, base1 + y])
    got("u_c0l", us.at[co, base0 + yl])
    got("u_c0r", us.at[co, base0 + yr])
    for h in (base0 + y, base1 + y, base0 + yl, base0 + yr):
        prepare_head(us, h, wq_ref, wkt_ref, wv_ref)
    ring_y(1, base1)
    got("d_or", wd.at[2 * xo + c, 0:128])
    push("d_coa", wd.at[2 * xo + c, 0:128], CORE)
    got("d_ol", wd.at[2 * xo + c, 128:256])
    push("d_cob", wd.at[2 * xo + c, 128:256], CORE)
    add(2 * xo + c)
    got("d_coa", wd.at[2 * xo + co, 0:128])
    got("d_cob", wd.at[2 * xo + co, 128:256])
    add(2 * xo + co)

    lq[0] = rms_rows(sums[:, 0:QR], qlg_ref[...]).astype(BF)
    push("q", lq.at[0], dev(zz=zmate), lq.at[1])
    kvb[y, z, 0:256] = rms_rows(sums[:, QR : QR + KR], klg_ref[...]).astype(BF)
    own = kvb.at[y, z]
    push("k_yr", own, Y_R)
    push("k_yl", own, Y_L)
    push("k_zr", own, Z_R)
    push("k_zl", own, Z_L)

    for j, base in ((0, base0), (1, base1)):
        got(f"u_y{j}or", us.at[c, base + yo, 0:2])
        got(f"u_y{j}ol", us.at[c, base + yo, 2:4])
        push(f"u_c{j}o", us.at[c, base + yo], CORE)
    got("w_ozr", wo.at[zo, 0:2, x, c])
    got("w_ozl", wo.at[zo, 2:4, x, c])
    row(3)
    got("u_c1l", us.at[co, base1 + yl])
    got("u_c1r", us.at[co, base1 + yr])
    got("u_c0o", us.at[co, base0 + yo])
    got("u_c1o", us.at[co, base1 + yo])
    push("w_c", wo.at[:, :, x, c], CORE)
    for h in (base0 + yo, base1 + yl, base1 + yr, base1 + yo):
        prepare_head(us, h, wq_ref, wkt_ref, wv_ref)
    make_queries(lq[0], sp, wq_ref, qgain_ref[...], lowq_ref, highq_ref, q_ref, 0)
    def k1():
        got("k_yr", kvb.at[yl, z])
        push("k_oyr", lambda: kvb.at[yl, z, 0:160], Y_R)
        got("k_yl", kvb.at[yr, z])
        push("k_oyl", lambda: kvb.at[yr, z, 160:320], Y_L)

    def k2():
        got("k_zr", kvb.at[y, zl])
        push("k_ozr", lambda: kvb.at[y, zl, 0:160], Z_R)
        push("k_y1r", lambda: kvb.at[y, zl], Y_R)
        push("k_y1l", lambda: kvb.at[y, zl], Y_L)
        got("k_zl", kvb.at[y, zr])
        push("k_ozl", lambda: kvb.at[y, zr, 160:320], Z_L)
        push("k_y2r", lambda: kvb.at[y, zr], Y_R)
        push("k_y2l", lambda: kvb.at[y, zr], Y_L)

    def k3():
        got("k_oyr", kvb.at[yo, z, 0:160])
        got("k_oyl", kvb.at[yo, z, 160:320])
        push("k_pzr", lambda: kvb.at[yo, z], Z_R)
        push("k_pzl", lambda: kvb.at[yo, z], Z_L)
        got("k_ozr", kvb.at[y, zo, 0:160])
        got("k_ozl", kvb.at[y, zo, 160:320])
        push("k_y3r", lambda: kvb.at[y, zo], Y_R)
        push("k_y3l", lambda: kvb.at[y, zo], Y_L)

    def k7():
        got("k_y1r", kvb.at[yl, zl])
        got("k_y1l", kvb.at[yr, zl])

    def k9():
        got("k_y2r", kvb.at[yl, zr])
        got("k_y2l", kvb.at[yr, zr])

    def k11():
        got("k_pzr", kvb.at[yo, zl])
        push("k_pozr", lambda: kvb.at[yo, zl, 0:160], Z_R)
        got("k_pzl", kvb.at[yo, zr])
        push("k_pozl", lambda: kvb.at[yo, zr, 160:320], Z_L)

    def k13():
        got("k_y3r", kvb.at[yl, zo])
        got("k_y3l", kvb.at[yr, zo])

    def k15():
        got("k_pozr", kvb.at[yo, zo, 0:160])
        got("k_pozl", kvb.at[yo, zo, 160:320])

    def queries_mate():
        got("q", lq.at[1])
        make_queries(
            lq[1], zmate * 4 + y, wq_ref, qgain_ref[...], lowq_ref, highq_ref, q_ref, 1
        )

    def wx(k):
        def go():
            r = zrow[k]
            got(f"w_xr{k}", wo.at[r, :, xl, c])
            push(f"w_oxr{k}", lambda: wo.at[r, 0:2, xl, c], X_R)
            push(f"w_cl{k}", lambda: wo.at[r, :, xl, c], CORE)
            got(f"w_xl{k}", wo.at[r, :, xr, c])
            push(f"w_oxl{k}", lambda: wo.at[r, 2:4, xr, c], X_L)
            push(f"w_cr{k}", lambda: wo.at[r, :, xr, c], CORE)

        return go

    def wxo(k):
        r = zrow[k]
        got(f"w_oxr{k}", wo.at[r, 0:2, xo, c])
        got(f"w_oxl{k}", wo.at[r, 2:4, xo, c])
        push(f"w_co{k}", wo.at[r, :, xo, c], CORE)

    hfirst = (z // 2) * LOCAL
    b_own, b_mate = sp, zmate * 4 + y

    def send_mate():
        close_heads(acc_ref, 1, att_ref, HEADS)
        push("att", lambda: att_ref.at[HEADS : HEADS + LOCAL], dev(zz=zmate), att_ref.at[pl.ds(hfirst, LOCAL)])

    def pick(test, yes, no):
        return no + test.astype(jnp.int32) * (yes - no)

    def source(step):
        dy = pick(step < 3, step, pick(step < 6, 0, pick(step == 6, 3, pick(
            step < 11, 1 + (step - 7) % 2, pick(
                step < 13, 3, pick(step < 15, step - 12, 3))))))
        dz = pick(step < 3, 0, pick(step < 6, step - 2, pick(step == 6, 0, pick(
            step < 11, 1 + (step - 7) // 2, pick(step < 13, step - 10, 3)))))
        yy = pick(dy == 0, y, pick(dy == 1, yl, pick(dy == 2, yr, yo)))
        zz = pick(dz == 0, z, pick(dz == 1, zl, pick(dz == 2, zr, zo)))
        return yy, zz, zz * 4 + yy

    b_last = jnp.maximum(b_own, b_mate)

    def expand_step(step, slot):
        yy, zz, b = source(step)
        expand(
            kvb[yy, zz], b, wkt_ref, wv_ref, gk_ref, gr_ref, lowk_ref, highk_ref, kt_ref,
            v_ref, slot,
        )

    def attend_to(which, slot, diagonal=False):
        attend(diagonal, q_ref, kt_ref, v_ref, m_ref, acc_ref, which, slot)

    expand_step(jnp.minimum(z, 0), 0)
    attend_to(0, 0, True)
    queries_mate()
    at_pair = {0: (k1, wx(0)), 1: (k2,), 2: (k3, wx(1)), 3: (k7, k11), 4: (k9, wx(2)), 6: (k13,),
               7: (k15, wx(3))}

    def pair(i, _):
        for when, todo in at_pair.items():
            @pl.when(i == when)
            def _(todo=todo):
                for f in todo:
                    f()

        first = pick(i == 7, 0, 2 * i + 1)
        second = pick(i == 7, 15, 2 * i + 2)
        b0, b1 = source(first)[2], source(second)[2]
        own_both = (b0 < b_own) & (b1 < b_own)
        mate_both = (b0 < b_mate) & (b1 < b_mate)
        either = own_both | mate_both
        needed = (b0 <= b_last) | (b1 <= b_last)
        lead = pick(own_both, 0, 1)

        @pl.when(either)
        def _():
            expand_step(first, 0)
            expand_step(second, 1)
            attend_pair(q_ref, kt_ref, v_ref, m_ref, acc_ref, lead)

        @pl.when(jnp.logical_not(either) & needed)
        def _():
            expand_step(first, 0)
            expand_step(second, 1)

        @pl.when(own_both & mate_both)
        def _():
            attend_pair(q_ref, kt_ref, v_ref, m_ref, acc_ref, 1)

        def single(j, _):
            which, slot = j // 2, j % 2
            b = pick(slot == 0, b0, b1)
            bq = pick(which == 0, b_own, b_mate)
            done = pick(which == 0, own_both.astype(jnp.int32), mate_both.astype(jnp.int32))

            @pl.when((b < bq) & (done == 0))
            def _():
                attend_to(which, slot)

            @pl.when((b == bq) & (which == 1))
            def _():
                attend_to(which, slot, True)

            return 0

        @pl.when(jnp.logical_not(own_both & mate_both))
        def _():
            lax.fori_loop(0, 4, single, 0)

        return 0

    lax.fori_loop(0, 8, pair, 0)
    send_mate()
    close_heads(acc_ref, 0, att_ref, hfirst)
    for k in range(4):
        wxo(k)
    got("w_c", wo.at[:, :, x, co])
    for k in range(4):
        got(f"w_cl{k}", wo.at[zrow[k], :, xl, co])
        got(f"w_cr{k}", wo.at[zrow[k], :, xr, co])
        got(f"w_co{k}", wo.at[zrow[k], :, xo, co])
    got("att", att_ref.at[pl.ds(LOCAL - hfirst, LOCAL)])
    finish(att_ref, mixed_ref, ogain_ref, wo, out_ref)
    for i, again in sent:
        view = again()
        pltpu.make_async_copy(view, view, ssem.at[i]).wait()
    assert len(names) <= SLOTS


def per_device(
    tokens, in_gain, w_query_down, w_latent_down, w_rope_key, query_latent_gain, latent_gain,
    w_query_up, w_key_up, w_value_up, query_gain, key_gain, out_gain, w_out,
):
    blocks = lax.axis_size("sp")
    tables = [jnp.asarray(t) for t in rope_tables(blocks)]
    vm = pl.BlockSpec(memory_space=pltpu.VMEM)
    args = (
        tokens.reshape(ROWS, D), in_gain.reshape(1, D), w_query_down, w_latent_down, w_rope_key.T,
        query_latent_gain.reshape(1, QR), latent_gain.reshape(1, KR), w_query_up, w_key_up,
        w_value_up, query_gain.reshape(1, QK), key_gain.reshape(1, QK), out_gain.reshape(1, D), w_out, *tables,
    )
    out = pl.pallas_call(
        kernel,
        out_shape=pltpu.VMEM((ROWS, D), BF),
        in_specs=[vm] * len(args),
        out_specs=vm,
        scratch_shapes=[
            pltpu.VMEM((8, 256, QR + KR), BF),
            pltpu.VMEM((2, LOCAL, 4, 160, 128), BF),
            pltpu.VMEM((4, 4, 4, 2, 16, D), BF),
            pltpu.VMEM((4, 4, 320, 256), BF),
            pltpu.VMEM((2, ROWS, QR), BF),
            pltpu.VMEM((8, ROWS, 256), BF),
            pltpu.VMEM((ROWS, QR + KR), F32),
            pltpu.VMEM((LOCAL, QR, 256), BF),
            pltpu.VMEM((LOCAL, NOPE, KR), BF),
            pltpu.VMEM((LOCAL, KR, VD), BF),
            pltpu.VMEM((2, LOCAL, ROWS, 256), BF),
            pltpu.VMEM((KEPT, LOCAL, 256, 256), BF),
            pltpu.VMEM((KEPT, LOCAL, 256, 256), BF),
            pltpu.VMEM((2, LOCAL, ROWS, 128), F32),
            pltpu.VMEM((2, LOCAL, ROWS, 256), F32),
            pltpu.VMEM((HEADS + LOCAL, ROWS, VD), BF),
            pltpu.VMEM((ROWS, D), BF),
            pltpu.VMEM((1, 256), F32),
            pltpu.VMEM((NOPE, 256), F32),
            pltpu.VMEM((ROPE, 256), F32),
            pltpu.SemaphoreType.DMA((SLOTS,)),
            pltpu.SemaphoreType.DMA((SLOTS,)),
        ],
        compiler_params=pltpu.CompilerParams(
            vmem_limit_bytes=60 * 1024 * 1024, collective_id=0, has_side_effects=True
        ),
    )(*args)
    return out.reshape(1, ROWS, D)


def solution(mesh):
    in_specs = (
        P("dp", "sp", None), P(), P("dp", None), P("dp", None), P(), P(), P(),
        P("dp", "sp"), P("dp", "sp"), P("dp", "sp"), P(), P(), P(), P(("sp", "dp"), None),
    )
    return jax.shard_map(
        per_device, mesh=mesh, in_specs=in_specs, out_specs=P("dp", "sp", None), check_vma=False
    )
```

```python
import functools

import jax
import jax.numpy as jnp
import numpy as np
from jax import lax
from jax.experimental import pallas as pl
from jax.experimental.pallas import tpu as pltpu
from jax.sharding import PartitionSpec as P

HEADS, NOPE, ROPE, VD, QR, KR, QK = 16, 128, 64, 128, 512, 256, 192
D = 2048
ROWS = 256
EPS = 1e-06
THETA = 10000.0
NEG_BIG = -1e30
BF, F32 = jnp.bfloat16, jnp.float32
SOFT = float(QK**-0.5 * np.log2(np.e))
LOCAL = 8


def rope_tables(blocks):
    half = ROPE // 2
    freq = THETA ** (-np.arange(half) / half)
    low = np.arange(ROWS)[:, None] * freq[None, :]
    high = (np.arange(blocks) * ROWS)[:, None] * freq[None, :]
    pad = np.zeros((ROWS, 128 - ROPE))
    lowq = np.stack([np.concatenate([f(low), f(low), pad], 1) for f in (np.cos, np.sin)])
    hpad = np.zeros((blocks, 128 - ROPE))
    highq = np.stack([np.concatenate([f(high), f(high), hpad], 1) for f in (np.cos, np.sin)], 1)
    highq = np.broadcast_to(highq[:, :, None, :], (blocks, 2, 8, 128))
    lowk = np.concatenate([np.cos(low).T, np.sin(low).T], 0)
    highk = np.concatenate([np.cos(high), np.sin(high)], 1)
    highk = np.broadcast_to(highk[:, :, None], (blocks, ROPE, 128))
    return [np.ascontiguousarray(t, dtype=np.float32) for t in (lowq, highq, lowk, highk)]


def dot(a, b):
    return lax.dot_general(a, b, (((1,), (0,)), ((), ())), preferred_element_type=F32)


def dot_nt(a, b):
    return lax.dot_general(a, b, (((1,), (1,)), ((), ())), preferred_element_type=F32)


def prepare_head(us, h, wq_ref, wkt_ref, wv_ref):
    keys = []
    for x in range(4):
        for c in range(2):
            d = 2 * x + c
            unit = us[c, h, x]
            rows = slice(d * 64, d * 64 + 64)
            wq_ref[h, rows, 0:NOPE] = unit[0:64]
            wq_ref[h, d * 64 : d * 64 + 32, NOPE:QK] = unit[64:96, 0:ROPE]
            wq_ref[h, d * 64 + 32 : d * 64 + 64, NOPE:QK] = unit[64:96, ROPE:128]
            keys.append(unit[96:128])
            wv_ref[h, d * 32 : d * 32 + 32] = unit[128:160]
    wkt_ref[h] = jnp.concatenate(keys, axis=0).T


def make_queries(latq, block, wq_ref, qgain, lowq_ref, highq_ref, q_ref, which):
    ch, sh = highq_ref[block, 0, 0:1], highq_ref[block, 1, 0:1]
    cl, sl = lowq_ref[0], lowq_ref[1]
    cosine = ch * cl - sh * sl
    sine = sh * cl + ch * sl
    lane = lax.broadcasted_iota(jnp.int32, (ROWS, 128), 1)
    sine_a = jnp.where(lane < ROPE // 2, -sine, 0.0)
    sine_b = jnp.where(lane < ROPE // 2, 0.0, sine)

    for h in range(LOCAL):
        q = dot(latq, wq_ref[h])
        scale = lax.rsqrt(jnp.sum(q * q, axis=1, keepdims=True) * (1.0 / QK) + EPS)
        n = q * scale * qgain
        t = n[:, NOPE:256]
        turned = (
            t * cosine
            + pltpu.roll(t, 128 - ROPE // 2, 1) * sine_a
            + pltpu.roll(t, ROPE // 2, 1) * sine_b
        )
        q_ref[which, h, :, 0:NOPE] = n[:, 0:NOPE].astype(BF)
        q_ref[which, h, :, NOPE:256] = turned.astype(BF)


def expand(unit, block, wkt_ref, wv_ref, gk_ref, gr_ref, lowk_ref, highk_ref, kt_ref, v_ref, slot):
    kv = unit[0:256, :]
    rope = unit[256:320, :].astype(F32)
    half = ROPE // 2
    ch = jnp.concatenate([highk_ref[block, 0:half]] * 2, axis=1)
    sh = jnp.concatenate([highk_ref[block, half:ROPE]] * 2, axis=1)
    cl, sl = lowk_ref[0:half], lowk_ref[half:ROPE]
    cosine = ch * cl - sh * sl
    sine = sh * cl + ch * sl
    rope_sq = jnp.sum(rope * rope, axis=0, keepdims=True)
    x = rope * gr_ref[...]
    a, b = x[0:half], x[half:ROPE]
    turned = jnp.concatenate([a * cosine - b * sine, b * cosine + a * sine], axis=0)
    kt = dot_nt(wkt_ref[...].reshape(LOCAL * NOPE, KR), kv)
    for h in range(LOCAL):
        k = kt[h * NOPE : (h + 1) * NOPE]
        scale = lax.rsqrt((jnp.sum(k * k, axis=0, keepdims=True) + rope_sq) * (1.0 / QK) + EPS)
        kt_ref[slot, h, 0:NOPE] = (k * scale * gk_ref[...]).astype(BF)
        kt_ref[slot, h, NOPE:QK] = (turned * scale).astype(BF)
    for h in range(LOCAL):
        v_ref[slot, h, :, 0:VD] = dot(kv, wv_ref[h]).astype(BF)


def attend(diagonal, q_ref, kt_ref, v_ref, m_ref, acc_ref, which, slot):
    for h in range(LOCAL):
        s = dot(q_ref[which, h], kt_ref[slot, h])
        if diagonal:
            row = lax.broadcasted_iota(jnp.int32, (ROWS, ROWS), 0)
            col = lax.broadcasted_iota(jnp.int32, (ROWS, ROWS), 1)
            s = jnp.where(col <= row, s, NEG_BIG)
        old = m_ref[which, h]
        new = jnp.maximum(old, jnp.max(s, axis=1, keepdims=True))
        fade = jnp.exp2((old - new) * SOFT)
        p = jnp.exp2((s - jnp.concatenate([new, new], 1)) * SOFT).astype(BF)
        m_ref[which, h] = new
        acc_ref[which, h] = acc_ref[which, h] * jnp.concatenate([fade, fade], 1) + dot(
            p, v_ref[slot, h]
        )


def attend_pair(q_ref, kt_ref, v_ref, m_ref, acc_ref, which):
    for h in range(LOCAL):
        q = q_ref[which, h]
        s0, s1 = dot(q, kt_ref[0, h]), dot(q, kt_ref[1, h])
        old = m_ref[which, h]
        new = jnp.maximum(old, jnp.max(jnp.maximum(s0, s1), axis=1, keepdims=True))
        fade = jnp.exp2((old - new) * SOFT)
        wide = jnp.concatenate([new, new], 1)
        p0 = jnp.exp2((s0 - wide) * SOFT).astype(BF)
        p1 = jnp.exp2((s1 - wide) * SOFT).astype(BF)
        m_ref[which, h] = new
        acc_ref[which, h] = acc_ref[which, h] * jnp.concatenate([fade, fade], 1) + (
            dot(p0, v_ref[0, h]) + dot(p1, v_ref[1, h])
        )


def close_heads(acc_ref, which, att_ref, first):
    for h in range(LOCAL):
        att_ref[first + h] = (
            acc_ref[which, h, :, 0:VD] / acc_ref[which, h, :, VD : 2 * VD]
        ).astype(BF)


def finish(att_ref, mixed_ref, ogain_ref, wo_ref, out_ref):
    total = jnp.zeros((ROWS, VD), F32)
    for h in range(HEADS):
        at = att_ref[h].astype(F32)
        total = total + at * at
    scale = lax.rsqrt(jnp.sum(total, axis=1, keepdims=True) * (1.0 / (HEADS * VD)) + EPS)
    for h in range(HEADS):
        cols = slice(h * VD, (h + 1) * VD)
        mixed_ref[:, cols] = (att_ref[h].astype(F32) * scale * ogain_ref[:, cols]).astype(BF)

    def one(j, _):
        cols = pl.ds(pl.multiple_of(j * 512, 512), 512)
        w = wo_ref[:, :, :, :, :, cols].reshape(HEADS * VD, 512)
        out_ref[:, cols] = dot(mixed_ref[...], w).astype(BF)
        return 0

    lax.fori_loop(0, D // 512, one, 0)


def rms_rows(values, scaling):
    return values * lax.rsqrt(jnp.mean(values * values, axis=-1, keepdims=True) + EPS) * scaling


SLOTS = 128
KEPT = 2


def kernel(
    tok_ref, ing_ref, wqd_ref, wld_ref, wrt_ref, qlg_ref, klg_ref, wqu_ref, wku_ref, wvu_ref,
    qg_ref, kg_ref, ogain_ref, wo_in_ref, lowq_ref, highq_ref, lowk_ref, highk_ref,
    out_ref,
    wd, us, wo, kvb, lq, normed, sums, wq_ref, wkt_ref, wv_ref, q_ref, kt_ref, v_ref,
    m_ref, acc_ref, att_ref, mixed_ref, qgain_ref, gk_ref, gr_ref, ssem, rsem,
):
    sp, dp = lax.axis_index("sp"), lax.axis_index("dp")
    z, y = sp // 4, sp % 4
    x, c = dp // 2, dp % 2
    xl, xr, xo = (x + 3) % 4, (x + 1) % 4, (x + 2) % 4
    yl, yr, yo = (y + 3) % 4, (y + 1) % 4, (y + 2) % 4
    zl, zr, zo = (z + 3) % 4, (z + 1) % 4, (z + 2) % 4
    co = 1 - c
    zb = z % 2
    zpair = z + 1 - 2 * zb
    zmate = 3 - z

    def dev(xx=x, yy=y, zz=z, cc=c):
        return {"sp": zz * 4 + yy, "dp": xx * 2 + cc}

    X_R, X_L, Y_R, Y_L, Z_R, Z_L, CORE = (
        dev(xx=xr), dev(xx=xl), dev(yy=yr), dev(yy=yl), dev(zz=zr), dev(zz=zl), dev(cc=co)
    )
    zn, zm = zpair, (z + 3 + 2 * zb) % 4
    Z_N, Z_M = dev(zz=zn), dev(zz=zm)
    names, sent = {}, []

    def number(name):
        return names.setdefault(name, len(names))

    def push(name, view, to, dst=None):
        i = number(name)
        again = view if callable(view) else functools.partial(lambda v: v, view)
        view = again()
        pltpu.make_async_remote_copy(
            src_ref=view, dst_ref=view if dst is None else dst, send_sem=ssem.at[i],
            recv_sem=rsem.at[i], device_id=to, device_id_type=pl.DeviceIdType.MESH,
        ).start()
        sent.append((i, again))

    def got(name, view):
        pltpu.make_async_copy(view, view, rsem.at[number(name)]).wait()

    barrier = pltpu.get_barrier_semaphore()
    X_O, Y_O = dev(xx=xo), dev(yy=yo)
    for to in (X_R, X_L, X_O, Y_R, Y_L, Y_O, Z_R, Z_L, CORE):
        pl.semaphore_signal(barrier, 1, device_id=to, device_id_type=pl.DeviceIdType.MESH)

    hl = zb * 4 + y
    us[c, hl, x, 0:64] = wqu_ref[:, 0:NOPE]
    us[c, hl, x, 64:96] = jnp.concatenate(
        [wqu_ref[0:32, NOPE:QK], wqu_ref[32:64, NOPE:QK]], axis=1
    )
    us[c, hl, x, 96:128] = wku_ref[...]
    us[c, hl, x, 128:160] = wvu_ref[...]
    wo[z, y, x, c] = wo_in_ref[...]
    wd[dp, :, 0:QR] = wqd_ref[...]
    wd[dp, :, QR : QR + KR] = wld_ref[...]
    pl.semaphore_wait(barrier, 9)

    uown = us.at[c, hl, x]
    push("u_r", uown, X_R)
    push("u_l", uown, X_L)
    push("u_o", uown, X_O)
    wown = wo.at[z, y, x, c]
    push("w_yr", wown, Y_R)
    push("w_yl", wown, Y_L)
    push("w_yo", wown, Y_O)
    down = wd.at[dp]
    push("d_ra", wd.at[dp, 0:128], X_R)
    push("d_la", wd.at[dp, 128:256], X_L)
    push("d_rb", wd.at[dp, 128:256], X_R)
    push("d_lb", wd.at[dp, 0:128], X_L)
    push("d_c", down, CORE)

    for r in range(0, ROWS, 64):
        rows = slice(r, r + 64)
        n = rms_rows(tok_ref[rows].astype(F32), ing_ref[...]).astype(BF)
        for k in range(8):
            normed[k, rows] = n[:, k * 256 : (k + 1) * 256]

    qgain_ref[:, 0:NOPE] = qg_ref[:, 0:NOPE]
    qgain_ref[:, NOPE:256] = jnp.concatenate(
        [qg_ref[:, NOPE:QK], jnp.zeros((1, 256 - QK), F32)], axis=1
    )
    kg = jnp.concatenate([kg_ref[...], jnp.zeros((1, 256 - QK), F32)], axis=1)
    column = jnp.broadcast_to(kg[:, 0:NOPE], (NOPE, NOPE)).T
    gk_ref[...] = jnp.concatenate([column, column], axis=1)
    column = jnp.broadcast_to(kg[:, NOPE:256], (NOPE, NOPE)).T[0:ROPE]
    gr_ref[...] = jnp.concatenate([column, column], axis=1)

    got("u_r", us.at[c, hl, xl])
    got("u_l", us.at[c, hl, xr])
    got("u_o", us.at[c, hl, xo])
    block0 = us.at[c, hl]
    push("u_z", block0, dev(zz=zpair))
    push("u_y0r", block0, Y_R)
    push("u_y0l", block0, Y_L)
    push("u_c0", block0, CORE)
    got("w_yr", wo.at[z, yl, x, c])
    got("w_yl", wo.at[z, yr, x, c])
    got("w_yo", wo.at[z, yo, x, c])
    push("w_zr", wo.at[z, :, x, c], Z_R)
    push("w_zl", wo.at[z, :, x, c], Z_L)

    def add(d, first=False):
        part = dot(normed[d], wd[d])
        if first:
            sums[...] = part
        else:
            sums[...] += part

    add(dp, True)
    got("d_c", wd.at[2 * x + co])
    add(2 * x + co)
    m_ref[...] = jnp.full(m_ref.shape, NEG_BIG, F32)
    acc_ref[...] = jnp.zeros(acc_ref.shape, F32)
    wq_ref[:, :, QK:256] = jnp.zeros((LOCAL, QR, 256 - QK), BF)
    kt_ref[:, :, QK:256, :] = jnp.zeros((KEPT, LOCAL, 256 - QK, 256), BF)
    v_ref[:, :, :, VD:256] = jnp.ones((KEPT, LOCAL, ROWS, 256 - VD), BF)
    rope_t = jnp.zeros((ROPE, ROWS), F32)
    for k in range(8):
        rope_t = rope_t + dot_nt(wrt_ref[:, k * 256 : (k + 1) * 256], normed[k])
    kvb[y, z, 256:320] = rope_t.astype(BF)
    base0, base1 = zb * 4, 4 - zb * 4
    block1 = us.at[c, base1 + y]

    def ring_y(j, base):
        got(f"u_y{j}r", us.at[c, base + yl])
        push(f"u_y{j}or", us.at[c, base + yl, 0:2], Y_R)
        push(f"u_c{j}l", us.at[c, base + yl], CORE)
        got(f"u_y{j}l", us.at[c, base + yr])
        push(f"u_y{j}ol", us.at[c, base + yr, 2:4], Y_L)
        push(f"u_c{j}r", us.at[c, base + yr], CORE)

    got("d_ra", wd.at[2 * xl + c, 0:128])
    push("d_or", wd.at[2 * xl + c, 0:128], X_R)
    got("d_la", wd.at[2 * xr + c, 128:256])
    push("d_ol", wd.at[2 * xr + c, 128:256], X_L)
    got("u_z", us.at[c, base1 + y])
    push("u_y1r", block1, Y_R)
    push("u_y1l", block1, Y_L)
    push("u_c1", block1, CORE)
    ring_y(0, base0)
    got("d_rb", wd.at[2 * xl + c, 128:256])
    push("d_cl", wd.at[2 * xl + c], CORE)
    got("d_lb", wd.at[2 * xr + c, 0:128])
    push("d_cr", wd.at[2 * xr + c], CORE)
    add(2 * xl + c)
    add(2 * xr + c)
    got("d_cl", wd.at[2 * xl + co])
    add(2 * xl + co)
    got("d_cr", wd.at[2 * xr + co])
    add(2 * xr + co)
    zrow = (z, zl, zr, zo)

    def row(k):
        push(f"w_xr{k}", wo.at[zrow[k], :, x, c], X_R)
        push(f"w_xl{k}", wo.at[zrow[k], :, x, c], X_L)

    row(0)
    got("w_zr", wo.at[zl, :, x, c])
    push("w_ozr", wo.at[zl, 0:2, x, c], Z_R)
    got("w_zl", wo.at[zr, :, x, c])
    push("w_ozl", wo.at[zr, 2:4, x, c], Z_L)
    row(1)
    row(2)
    got("u_c0", us.at[co, base0 + y])
    got("u_c1", us.at[co, base1 + y])
    got("u_c0l", us.at[co, base0 + yl])
    got("u_c0r", us.at[co, base0 + yr])
    for h in (base0 + y, base1 + y, base0 + yl, base0 + yr):
        prepare_head(us, h, wq_ref, wkt_ref, wv_ref)
    ring_y(1, base1)
    got("d_or", wd.at[2 * xo + c, 0:128])
    push("d_coa", wd.at[2 * xo + c, 0:128], CORE)
    got("d_ol", wd.at[2 * xo + c, 128:256])
    push("d_cob", wd.at[2 * xo + c, 128:256], CORE)
    add(2 * xo + c)
    got("d_coa", wd.at[2 * xo + co, 0:128])
    got("d_cob", wd.at[2 * xo + co, 128:256])
    add(2 * xo + co)

    lq[0] = rms_rows(sums[:, 0:QR], qlg_ref[...]).astype(BF)
    push("q", lq.at[0], dev(zz=zmate), lq.at[1])
    kvb[y, z, 0:256] = rms_rows(sums[:, QR : QR + KR], klg_ref[...]).astype(BF)
    own = kvb.at[y, z]
    push("k_yr", own, Y_R)
    push("k_yl", own, Y_L)
    push("k_zn", own, Z_N)
    push("k_zm", own, Z_M)

    for j, base in ((0, base0), (1, base1)):
        got(f"u_y{j}or", us.at[c, base + yo, 0:2])
        got(f"u_y{j}ol", us.at[c, base + yo, 2:4])
        push(f"u_c{j}o", us.at[c, base + yo], CORE)
    got("w_ozr", wo.at[zo, 0:2, x, c])
    got("w_ozl", wo.at[zo, 2:4, x, c])
    row(3)
    got("u_c1l", us.at[co, base1 + yl])
    got("u_c1r", us.at[co, base1 + yr])
    got("u_c0o", us.at[co, base0 + yo])
    got("u_c1o", us.at[co, base1 + yo])
    push("w_c", wo.at[:, :, x, c], CORE)
    for h in (base0 + yo, base1 + yl, base1 + yr, base1 + yo):
        prepare_head(us, h, wq_ref, wkt_ref, wv_ref)
    make_queries(lq[0], sp, wq_ref, qgain_ref[...], lowq_ref, highq_ref, q_ref, 0)
    def k_y():
        got("k_yr", kvb.at[yl, z])
        push("k_oyr", lambda: kvb.at[yl, z, 0:160], Y_R)
        got("k_yl", kvb.at[yr, z])
        push("k_oyl", lambda: kvb.at[yr, z, 160:320], Y_L)

    def k_zn():
        got("k_zn", kvb.at[y, zn])
        push("k_ozm", lambda: kvb.at[y, zn, 0:160], Z_M)
        push("k_ynr", lambda: kvb.at[y, zn], Y_R)
        push("k_ynl", lambda: kvb.at[y, zn], Y_L)

    def k_zm():
        got("k_zm", kvb.at[y, zm])
        push("k_ozn", lambda: kvb.at[y, zm, 160:320], Z_N)
        push("k_ymr", lambda: kvb.at[y, zm], Y_R)
        push("k_yml", lambda: kvb.at[y, zm], Y_L)

    def k_oy():
        got("k_oyr", kvb.at[yo, z, 0:160])
        got("k_oyl", kvb.at[yo, z, 160:320])
        push("k_pzn", lambda: kvb.at[yo, z], Z_N)
        push("k_pzm", lambda: kvb.at[yo, z], Z_M)

    def k_oz():
        got("k_ozm", kvb.at[y, zo, 0:160])
        got("k_ozn", kvb.at[y, zo, 160:320])
        push("k_yor", lambda: kvb.at[y, zo], Y_R)
        push("k_yol", lambda: kvb.at[y, zo], Y_L)

    def k_pz():
        got("k_pzn", kvb.at[yo, zn])
        push("k_pozm", lambda: kvb.at[yo, zn, 0:160], Z_M)
        got("k_pzm", kvb.at[yo, zm])
        push("k_pozn", lambda: kvb.at[yo, zm, 160:320], Z_N)

    def k_yn():
        got("k_ynr", kvb.at[yl, zn])
        got("k_ynl", kvb.at[yr, zn])

    def k_ym():
        got("k_ymr", kvb.at[yl, zm])
        got("k_yml", kvb.at[yr, zm])

    def k_yo():
        got("k_yor", kvb.at[yl, zo])
        got("k_yol", kvb.at[yr, zo])

    def k_poz():
        got("k_pozm", kvb.at[yo, zo, 0:160])
        got("k_pozn", kvb.at[yo, zo, 160:320])

    def queries_mate():
        got("q", lq.at[1])
        make_queries(
            lq[1], zmate * 4 + y, wq_ref, qgain_ref[...], lowq_ref, highq_ref, q_ref, 1
        )

    def wx(k):
        def go():
            r = zrow[k]
            got(f"w_xr{k}", wo.at[r, :, xl, c])
            push(f"w_oxr{k}", lambda: wo.at[r, 0:2, xl, c], X_R)
            push(f"w_cl{k}", lambda: wo.at[r, :, xl, c], CORE)
            got(f"w_xl{k}", wo.at[r, :, xr, c])
            push(f"w_oxl{k}", lambda: wo.at[r, 2:4, xr, c], X_L)
            push(f"w_cr{k}", lambda: wo.at[r, :, xr, c], CORE)

        return go

    def wxo(k):
        r = zrow[k]
        got(f"w_oxr{k}", wo.at[r, 0:2, xo, c])
        got(f"w_oxl{k}", wo.at[r, 2:4, xo, c])
        push(f"w_co{k}", wo.at[r, :, xo, c], CORE)

    hfirst = (z // 2) * LOCAL
    b_own, b_mate = sp, zmate * 4 + y

    def send_mate():
        close_heads(acc_ref, 1, att_ref, HEADS)
        push("att", lambda: att_ref.at[HEADS : HEADS + LOCAL], dev(zz=zmate), att_ref.at[pl.ds(hfirst, LOCAL)])

    def pick(test, yes, no):
        return no + test.astype(jnp.int32) * (yes - no)

    def source(step):
        dy = pick(step < 3, step, pick(step < 5, 0, pick(step < 7, step - 4, pick(
            step == 7, 0, pick(step == 8, 3, pick(step < 11, step - 8, pick(
                step < 13, 3, pick(step < 15, step - 12, 3))))))))
        dz = pick(step < 3, 0, pick(step < 5, step - 2, pick(step < 7, 1, pick(
            step == 7, 3, pick(step == 8, 0, pick(step < 11, 2, pick(
                step < 13, step - 10, 3)))))))
        yy = pick(dy == 0, y, pick(dy == 1, yl, pick(dy == 2, yr, yo)))
        zz = pick(dz == 0, z, pick(dz == 1, zn, pick(dz == 2, zm, zo)))
        return yy, zz, zz * 4 + yy

    b_last = jnp.maximum(b_own, b_mate)

    def expand_step(step, slot):
        yy, zz, b = source(step)
        expand(
            kvb[yy, zz], b, wkt_ref, wv_ref, gk_ref, gr_ref, lowk_ref, highk_ref, kt_ref,
            v_ref, slot,
        )

    def attend_to(which, slot, diagonal=False):
        attend(diagonal, q_ref, kt_ref, v_ref, m_ref, acc_ref, which, slot)

    def singles(b0, b1, own0, own1, skip_own, skip_mate):
        def single(j, _):
            which, slot = j // 2, j % 2
            b = pick(slot == 0, b0, b1)
            mine = pick(slot == 0, own0.astype(jnp.int32), own1.astype(jnp.int32)) * (1 - skip_own)
            mates = (b < b_mate).astype(jnp.int32) * (1 - skip_mate)

            @pl.when(pick(which == 0, mine, mates) == 1)
            def _():
                attend_to(which, slot)

            @pl.when((b == b_mate) & (which == 1))
            def _():
                attend_to(which, slot, True)

            return 0

        lax.fori_loop(0, 4, single, 0)

    zero = z - z
    expand_step(zero, 0)
    attend_to(0, 0, True)
    k_y()
    k_zn()
    expand_step(zero + 1, 0)
    expand_step(zero + 2, 1)
    queries_mate()
    k_oy()
    k_zm()
    mate_both = (source(zero + 1)[2] < b_mate) & (source(zero + 2)[2] < b_mate)

    @pl.when(mate_both)
    def _():
        attend_pair(q_ref, kt_ref, v_ref, m_ref, acc_ref, 1)

    at_pair = {1: (k_oz, wx(0)), 2: (k_yn, k_pz), 3: (wx(1),), 4: (k_ym, wx(2)), 5: (wx(3),),
               6: (k_yo,), 7: (k_poz,)}

    def pair(i, _):
        for when, todo in at_pair.items():
            @pl.when(i == when)
            def _(todo=todo):
                for f in todo:
                    f()

        first = pick(i == 7, 0, 2 * i + 1)
        second = pick(i == 7, 15, 2 * i + 2)
        b0, b1 = source(first)[2], source(second)[2]
        own0 = (b0 < b_own) & (i > 0) & (first > 0)
        own1 = (b1 < b_own) & (i > 0) & (second != 8)
        own_both = own0 & own1
        mate_both = (b0 < b_mate) & (b1 < b_mate)
        either = (own_both | mate_both) & (i > 0)
        needed = ((b0 <= b_last) | (b1 <= b_last)) & (i > 0)
        lead = pick(own_both, 0, 1)

        @pl.when(either)
        def _():
            expand_step(first, 0)
            expand_step(second, 1)
            attend_pair(q_ref, kt_ref, v_ref, m_ref, acc_ref, lead)

        @pl.when(jnp.logical_not(either) & needed)
        def _():
            expand_step(first, 0)
            expand_step(second, 1)

        @pl.when(own_both & mate_both)
        def _():
            attend_pair(q_ref, kt_ref, v_ref, m_ref, acc_ref, 1)

        @pl.when(jnp.logical_not(own_both & mate_both))
        def _():
            singles(b0, b1, own0, own1, own_both.astype(jnp.int32), mate_both.astype(jnp.int32))

        return 0

    lax.fori_loop(0, 8, pair, 0)
    send_mate()

    def last(j, _):
        step = pick(j == 2, 8, j + 1)

        @pl.when(source(step)[2] < b_own)
        def _():
            expand_step(step, 0)
            attend_to(0, 0)

        return 0

    lax.fori_loop(0, 3, last, 0)
    close_heads(acc_ref, 0, att_ref, hfirst)
    for k in range(4):
        wxo(k)
    got("w_c", wo.at[:, :, x, co])
    for k in range(4):
        got(f"w_cl{k}", wo.at[zrow[k], :, xl, co])
        got(f"w_cr{k}", wo.at[zrow[k], :, xr, co])
        got(f"w_co{k}", wo.at[zrow[k], :, xo, co])
    got("att", att_ref.at[pl.ds(LOCAL - hfirst, LOCAL)])
    finish(att_ref, mixed_ref, ogain_ref, wo, out_ref)
    for i, again in sent:
        view = again()
        pltpu.make_async_copy(view, view, ssem.at[i]).wait()
    assert len(names) <= SLOTS


def per_device(
    tokens, in_gain, w_query_down, w_latent_down, w_rope_key, query_latent_gain, latent_gain,
    w_query_up, w_key_up, w_value_up, query_gain, key_gain, out_gain, w_out,
):
    blocks = lax.axis_size("sp")
    tables = [jnp.asarray(t) for t in rope_tables(blocks)]
    vm = pl.BlockSpec(memory_space=pltpu.VMEM)
    args = (
        tokens.reshape(ROWS, D), in_gain.reshape(1, D), w_query_down, w_latent_down, w_rope_key.T,
        query_latent_gain.reshape(1, QR), latent_gain.reshape(1, KR), w_query_up, w_key_up,
        w_value_up, query_gain.reshape(1, QK), key_gain.reshape(1, QK), out_gain.reshape(1, D), w_out, *tables,
    )
    out = pl.pallas_call(
        kernel,
        out_shape=pltpu.VMEM((ROWS, D), BF),
        in_specs=[vm] * len(args),
        out_specs=vm,
        scratch_shapes=[
            pltpu.VMEM((8, 256, QR + KR), BF),
            pltpu.VMEM((2, LOCAL, 4, 160, 128), BF),
            pltpu.VMEM((4, 4, 4, 2, 16, D), BF),
            pltpu.VMEM((4, 4, 320, 256), BF),
            pltpu.VMEM((2, ROWS, QR), BF),
            pltpu.VMEM((8, ROWS, 256), BF),
            pltpu.VMEM((ROWS, QR + KR), F32),
            pltpu.VMEM((LOCAL, QR, 256), BF),
            pltpu.VMEM((LOCAL, NOPE, KR), BF),
            pltpu.VMEM((LOCAL, KR, VD), BF),
            pltpu.VMEM((2, LOCAL, ROWS, 256), BF),
            pltpu.VMEM((KEPT, LOCAL, 256, 256), BF),
            pltpu.VMEM((KEPT, LOCAL, 256, 256), BF),
            pltpu.VMEM((2, LOCAL, ROWS, 128), F32),
            pltpu.VMEM((2, LOCAL, ROWS, 256), F32),
            pltpu.VMEM((HEADS + LOCAL, ROWS, VD), BF),
            pltpu.VMEM((ROWS, D), BF),
            pltpu.VMEM((1, 256), F32),
            pltpu.VMEM((NOPE, 256), F32),
            pltpu.VMEM((ROPE, 256), F32),
            pltpu.SemaphoreType.DMA((SLOTS,)),
            pltpu.SemaphoreType.DMA((SLOTS,)),
        ],
        compiler_params=pltpu.CompilerParams(
            vmem_limit_bytes=60 * 1024 * 1024, collective_id=0, has_side_effects=True
        ),
    )(*args)
    return out.reshape(1, ROWS, D)


def solution(mesh):
    in_specs = (
        P("dp", "sp", None), P(), P("dp", None), P("dp", None), P(), P(), P(),
        P("dp", "sp"), P("dp", "sp"), P("dp", "sp"), P(), P(), P(), P(("sp", "dp"), None),
    )
    return jax.shard_map(
        per_device, mesh=mesh, in_specs=in_specs, out_specs=P("dp", "sp", None), check_vma=False
    )
```

```python
import functools

import jax
import jax.numpy as jnp
import numpy as np
from jax import lax
from jax.experimental import pallas as pl
from jax.experimental.pallas import tpu as pltpu
from jax.sharding import PartitionSpec as P

HEADS, NOPE, ROPE, VD, QR, KR, QK = 16, 128, 64, 128, 512, 256, 192
D = 2048
ROWS = 256
EPS = 1e-06
THETA = 10000.0
NEG_BIG = -1e30
BF, F32 = jnp.bfloat16, jnp.float32
SOFT = float(QK**-0.5 * np.log2(np.e))
LOCAL = 8


def rope_tables(blocks):
    half = ROPE // 2
    freq = THETA ** (-np.arange(half) / half)
    low = np.arange(ROWS)[:, None] * freq[None, :]
    high = (np.arange(blocks) * ROWS)[:, None] * freq[None, :]
    pad = np.zeros((ROWS, 128 - ROPE))
    lowq = np.stack([np.concatenate([f(low), f(low), pad], 1) for f in (np.cos, np.sin)])
    hpad = np.zeros((blocks, 128 - ROPE))
    highq = np.stack([np.concatenate([f(high), f(high), hpad], 1) for f in (np.cos, np.sin)], 1)
    highq = np.broadcast_to(highq[:, :, None, :], (blocks, 2, 8, 128))
    lowk = np.concatenate([np.cos(low).T, np.sin(low).T], 0)
    highk = np.concatenate([np.cos(high), np.sin(high)], 1)
    highk = np.broadcast_to(highk[:, :, None], (blocks, ROPE, 128))
    return [np.ascontiguousarray(t, dtype=np.float32) for t in (lowq, highq, lowk, highk)]


def dot(a, b):
    return lax.dot_general(a, b, (((1,), (0,)), ((), ())), preferred_element_type=F32)


def dot_nt(a, b):
    return lax.dot_general(a, b, (((1,), (1,)), ((), ())), preferred_element_type=F32)


def prepare_head(us, h, wq_ref, wkt_ref, wv_ref):
    keys = []
    for x in range(4):
        for c in range(2):
            d = 2 * x + c
            unit = us[c, h, x]
            rows = slice(d * 64, d * 64 + 64)
            wq_ref[h, rows, 0:NOPE] = unit[0:64]
            wq_ref[h, d * 64 : d * 64 + 32, NOPE:QK] = unit[64:96, 0:ROPE]
            wq_ref[h, d * 64 + 32 : d * 64 + 64, NOPE:QK] = unit[64:96, ROPE:128]
            keys.append(unit[96:128])
            wv_ref[h // 2, d * 32 : d * 32 + 32, pl.ds(pl.multiple_of(h % 2 * VD, VD), VD)] = unit[128:160]
    wkt_ref[h] = jnp.concatenate(keys, axis=0).T


def make_queries(latq, block, wq_ref, qgain, lowq_ref, highq_ref, q_ref, which):
    ch, sh = highq_ref[block, 0, 0:1], highq_ref[block, 1, 0:1]
    cl, sl = lowq_ref[0], lowq_ref[1]
    cosine = ch * cl - sh * sl
    sine = sh * cl + ch * sl
    lane = lax.broadcasted_iota(jnp.int32, (ROWS, 128), 1)
    sine_a = jnp.where(lane < ROPE // 2, -sine, 0.0)
    sine_b = jnp.where(lane < ROPE // 2, 0.0, sine)

    for h in range(LOCAL):
        q = dot(latq, wq_ref[h])
        scale = lax.rsqrt(jnp.sum(q * q, axis=1, keepdims=True) * (1.0 / QK) + EPS)
        n = q * scale * qgain
        t = n[:, NOPE:256]
        turned = (
            t * cosine
            + pltpu.roll(t, 128 - ROPE // 2, 1) * sine_a
            + pltpu.roll(t, ROPE // 2, 1) * sine_b
        )
        q_ref[which, h, :, 0:NOPE] = n[:, 0:NOPE].astype(BF)
        q_ref[which, h, :, NOPE:256] = turned.astype(BF)


def expand(unit, block, wkt_ref, wv_ref, gk_ref, gr_ref, lowk_ref, highk_ref, kt_ref, v_ref, slot):
    kv = unit[0:256, :]
    rope = unit[256:320, :].astype(F32)
    half = ROPE // 2
    ch = jnp.concatenate([highk_ref[block, 0:half]] * 2, axis=1)
    sh = jnp.concatenate([highk_ref[block, half:ROPE]] * 2, axis=1)
    cl, sl = lowk_ref[0:half], lowk_ref[half:ROPE]
    cosine = ch * cl - sh * sl
    sine = sh * cl + ch * sl
    rope_sq = jnp.sum(rope * rope, axis=0, keepdims=True)
    x = rope * gr_ref[...]
    a, b = x[0:half], x[half:ROPE]
    turned = jnp.concatenate([a * cosine - b * sine, b * cosine + a * sine], axis=0)
    kt = dot_nt(wkt_ref[...].reshape(LOCAL * NOPE, KR), kv)
    for h in range(LOCAL):
        k = kt[h * NOPE : (h + 1) * NOPE]
        scale = lax.rsqrt((jnp.sum(k * k, axis=0, keepdims=True) + rope_sq) * (1.0 / QK) + EPS)
        kt_ref[slot, h, 0:NOPE] = (k * scale * gk_ref[...]).astype(BF)
        kt_ref[slot, h, NOPE:QK] = (turned * scale).astype(BF)
    for h in range(0, LOCAL, 2):
        v = dot(kv, wv_ref[h // 2]).astype(BF)
        v_ref[slot, h, :, 0:VD] = v[:, 0:VD]
        v_ref[slot, h + 1, :, 0:VD] = v[:, VD : 2 * VD]


def attend(diagonal, q_ref, kt_ref, v_ref, m_ref, acc_ref, which, slot):
    for h in range(LOCAL):
        s = dot(q_ref[which, h], kt_ref[slot, h])
        if diagonal:
            row = lax.broadcasted_iota(jnp.int32, (ROWS, ROWS), 0)
            col = lax.broadcasted_iota(jnp.int32, (ROWS, ROWS), 1)
            s = jnp.where(col <= row, s, NEG_BIG)
        old = m_ref[which, h]
        new = jnp.maximum(old, jnp.max(s, axis=1, keepdims=True))
        fade = jnp.exp2((old - new) * SOFT)
        p = jnp.exp2((s - jnp.concatenate([new, new], 1)) * SOFT).astype(BF)
        m_ref[which, h] = new
        acc_ref[which, h] = acc_ref[which, h] * jnp.concatenate([fade, fade], 1) + dot(
            p, v_ref[slot, h]
        )


def attend_pair(q_ref, kt_ref, v_ref, m_ref, acc_ref, which):
    for h in range(LOCAL):
        q = q_ref[which, h]
        s0, s1 = dot(q, kt_ref[0, h]), dot(q, kt_ref[1, h])
        old = m_ref[which, h]
        new = jnp.maximum(old, jnp.max(jnp.maximum(s0, s1), axis=1, keepdims=True))
        fade = jnp.exp2((old - new) * SOFT)
        wide = jnp.concatenate([new, new], 1)
        p0 = jnp.exp2((s0 - wide) * SOFT).astype(BF)
        p1 = jnp.exp2((s1 - wide) * SOFT).astype(BF)
        m_ref[which, h] = new
        acc_ref[which, h] = acc_ref[which, h] * jnp.concatenate([fade, fade], 1) + (
            dot(p0, v_ref[0, h]) + dot(p1, v_ref[1, h])
        )


def close_heads(acc_ref, which, att_ref, first):
    for h in range(LOCAL):
        att_ref[first + h] = (
            acc_ref[which, h, :, 0:VD] / acc_ref[which, h, :, VD : 2 * VD]
        ).astype(BF)


def finish(att_ref, mixed_ref, ogain_ref, wo_ref, out_ref):
    total = jnp.zeros((ROWS, VD), F32)
    for h in range(HEADS):
        at = att_ref[h].astype(F32)
        total = total + at * at
    scale = lax.rsqrt(jnp.sum(total, axis=1, keepdims=True) * (1.0 / (HEADS * VD)) + EPS)
    for h in range(HEADS):
        cols = slice(h * VD, (h + 1) * VD)
        mixed_ref[:, cols] = (att_ref[h].astype(F32) * scale * ogain_ref[:, cols]).astype(BF)

    def one(j, _):
        cols = pl.ds(pl.multiple_of(j * 512, 512), 512)
        w = wo_ref[:, :, :, :, :, cols].reshape(HEADS * VD, 512)
        out_ref[:, cols] = dot(mixed_ref[...], w).astype(BF)
        return 0

    lax.fori_loop(0, D // 512, one, 0)


def rms_rows(values, scaling):
    return values * lax.rsqrt(jnp.mean(values * values, axis=-1, keepdims=True) + EPS) * scaling


SLOTS = 128
KEPT = 2


def kernel(
    tok_in, ing_ref, wqd_in, wld_in, wrt_in, qlg_ref, klg_ref, wqu_in, wku_in, wvu_in,
    qg_ref, kg_ref, ogain_ref, wo_in, lowq_in, highq_in, lowk_in, highk_in,
    out_ref,
    wd, us, wo, kvb, lq, normed, sums, wq_ref, wkt_ref, wv_ref, q_ref, kt_ref, v_ref,
    m_ref, acc_ref, att_ref, mixed_ref, qgain_ref, gk_ref, gr_ref,
    tok_ref, wrt_ref, wqu_ref, lowq_ref, highq_ref, lowk_ref, highk_ref, lsem, ssem, rsem,
):
    sp, dp = lax.axis_index("sp"), lax.axis_index("dp")
    z, y = sp // 4, sp % 4
    x, c = dp // 2, dp % 2
    xl, xr, xo = (x + 3) % 4, (x + 1) % 4, (x + 2) % 4
    yl, yr, yo = (y + 3) % 4, (y + 1) % 4, (y + 2) % 4
    zl, zr, zo = (z + 3) % 4, (z + 1) % 4, (z + 2) % 4
    co = 1 - c
    zb = z % 2
    zpair = z + 1 - 2 * zb
    zmate = 3 - z

    def dev(xx=x, yy=y, zz=z, cc=c):
        return {"sp": zz * 4 + yy, "dp": xx * 2 + cc}

    X_R, X_L, Y_R, Y_L, Z_R, Z_L, CORE = (
        dev(xx=xr), dev(xx=xl), dev(yy=yr), dev(yy=yl), dev(zz=zr), dev(zz=zl), dev(cc=co)
    )
    zn, zm = zpair, (z + 3 + 2 * zb) % 4
    Z_N, Z_M = dev(zz=zn), dev(zz=zm)
    names, sent = {}, []

    def number(name):
        return names.setdefault(name, len(names))

    def push(name, view, to, dst=None):
        i = number(name)
        again = view if callable(view) else functools.partial(lambda v: v, view)
        view = again()
        pltpu.make_async_remote_copy(
            src_ref=view, dst_ref=view if dst is None else dst, send_sem=ssem.at[i],
            recv_sem=rsem.at[i], device_id=to, device_id_type=pl.DeviceIdType.MESH,
        ).start()
        sent.append((i, again))

    def got(name, view):
        pltpu.make_async_copy(view, view, rsem.at[number(name)]).wait()

    barrier = pltpu.get_barrier_semaphore()
    X_O, Y_O = dev(xx=xo), dev(yy=yo)
    for to in (X_R, X_L, X_O, Y_R, Y_L, Y_O, Z_R, Z_L, CORE):
        pl.semaphore_signal(barrier, 1, device_id=to, device_id_type=pl.DeviceIdType.MESH)

    hl = zb * 4 + y
    loads = [
        pltpu.make_async_copy(src, dst, lsem.at[i])
        for i, (src, dst) in enumerate((
            (wqu_in, wqu_ref), (wku_in, us.at[c, hl, x, 96:128]),
            (wvu_in, us.at[c, hl, x, 128:160]), (wo_in, wo.at[z, y, x, c]),
            (wqd_in, wd.at[dp, :, 0:QR]), (wld_in, wd.at[dp, :, QR : QR + KR]),
            (tok_in, tok_ref), (wrt_in, wrt_ref), (lowq_in, lowq_ref), (highq_in, highq_ref),
            (lowk_in, lowk_ref), (highk_in, highk_ref),
        ))
    ]
    for load in loads:
        load.start()
    loads[0].wait()
    us[c, hl, x, 0:64] = wqu_ref[:, 0:NOPE]
    us[c, hl, x, 64:96] = jnp.concatenate(
        [wqu_ref[0:32, NOPE:QK], wqu_ref[32:64, NOPE:QK]], axis=1
    )
    for load in loads[1:4]:
        load.wait()
    pl.semaphore_wait(barrier, 9)

    uown = us.at[c, hl, x]
    push("u_r", uown, X_R)
    push("u_l", uown, X_L)
    push("u_o", uown, X_O)
    wown = wo.at[z, y, x, c]
    push("w_yr", wown, Y_R)
    push("w_yl", wown, Y_L)
    push("w_yo", wown, Y_O)
    loads[4].wait()
    loads[5].wait()
    down = wd.at[dp]
    push("d_ra", wd.at[dp, 0:128], X_R)
    push("d_la", wd.at[dp, 128:256], X_L)
    push("d_rb", wd.at[dp, 128:256], X_R)
    push("d_lb", wd.at[dp, 0:128], X_L)
    push("d_c", down, CORE)

    for load in loads[6:]:
        load.wait()
    for r in range(0, ROWS, 64):
        rows = slice(r, r + 64)
        n = rms_rows(tok_ref[rows].astype(F32), ing_ref[...]).astype(BF)
        for k in range(8):
            normed[k, rows] = n[:, k * 256 : (k + 1) * 256]

    qgain_ref[:, 0:NOPE] = qg_ref[:, 0:NOPE]
    qgain_ref[:, NOPE:256] = jnp.concatenate(
        [qg_ref[:, NOPE:QK], jnp.zeros((1, 256 - QK), F32)], axis=1
    )
    kg = jnp.concatenate([kg_ref[...], jnp.zeros((1, 256 - QK), F32)], axis=1)
    column = jnp.broadcast_to(kg[:, 0:NOPE], (NOPE, NOPE)).T
    gk_ref[...] = jnp.concatenate([column, column], axis=1)
    column = jnp.broadcast_to(kg[:, NOPE:256], (NOPE, NOPE)).T[0:ROPE]
    gr_ref[...] = jnp.concatenate([column, column], axis=1)

    got("u_r", us.at[c, hl, xl])
    got("u_l", us.at[c, hl, xr])
    got("u_o", us.at[c, hl, xo])
    block0 = us.at[c, hl]
    push("u_z", block0, dev(zz=zpair))
    push("u_y0r", block0, Y_R)
    push("u_y0l", block0, Y_L)
    push("u_c0", block0, CORE)
    got("w_yr", wo.at[z, yl, x, c])
    got("w_yl", wo.at[z, yr, x, c])
    got("w_yo", wo.at[z, yo, x, c])
    push("w_zr", wo.at[z, :, x, c], Z_R)
    push("w_zl", wo.at[z, :, x, c], Z_L)

    def add(d, first=False):
        part = dot(normed[d], wd[d])
        if first:
            sums[...] = part
        else:
            sums[...] += part

    add(dp, True)
    got("d_c", wd.at[2 * x + co])
    add(2 * x + co)
    m_ref[...] = jnp.full(m_ref.shape, NEG_BIG, F32)
    acc_ref[...] = jnp.zeros(acc_ref.shape, F32)
    wq_ref[:, :, QK:256] = jnp.zeros((LOCAL, QR, 256 - QK), BF)
    kt_ref[:, :, QK:256, :] = jnp.zeros((KEPT, LOCAL, 256 - QK, 256), BF)
    v_ref[:, :, :, VD:256] = jnp.ones((KEPT, LOCAL, ROWS, 256 - VD), BF)
    rope_t = jnp.zeros((ROPE, ROWS), F32)
    for k in range(8):
        rope_t = rope_t + dot_nt(wrt_ref[:, k * 256 : (k + 1) * 256], normed[k])
    kvb[y, z, 256:320] = rope_t.astype(BF)
    base0, base1 = zb * 4, 4 - zb * 4
    block1 = us.at[c, base1 + y]

    def ring_y(j, base):
        got(f"u_y{j}r", us.at[c, base + yl])
        push(f"u_y{j}or", us.at[c, base + yl, 0:2], Y_R)
        push(f"u_c{j}l", us.at[c, base + yl], CORE)
        got(f"u_y{j}l", us.at[c, base + yr])
        push(f"u_y{j}ol", us.at[c, base + yr, 2:4], Y_L)
        push(f"u_c{j}r", us.at[c, base + yr], CORE)

    got("d_ra", wd.at[2 * xl + c, 0:128])
    push("d_or", wd.at[2 * xl + c, 0:128], X_R)
    got("d_la", wd.at[2 * xr + c, 128:256])
    push("d_ol", wd.at[2 * xr + c, 128:256], X_L)
    got("u_z", us.at[c, base1 + y])
    push("u_y1r", block1, Y_R)
    push("u_y1l", block1, Y_L)
    push("u_c1", block1, CORE)
    ring_y(0, base0)
    got("d_rb", wd.at[2 * xl + c, 128:256])
    push("d_cl", wd.at[2 * xl + c], CORE)
    got("d_lb", wd.at[2 * xr + c, 0:128])
    push("d_cr", wd.at[2 * xr + c], CORE)
    add(2 * xl + c)
    add(2 * xr + c)
    got("d_cl", wd.at[2 * xl + co])
    add(2 * xl + co)
    got("d_cr", wd.at[2 * xr + co])
    add(2 * xr + co)
    zrow = (z, zl, zr, zo)

    def row(k):
        push(f"w_xr{k}", wo.at[zrow[k], :, x, c], X_R)
        push(f"w_xl{k}", wo.at[zrow[k], :, x, c], X_L)

    row(0)
    got("w_zr", wo.at[zl, :, x, c])
    push("w_ozr", wo.at[zl, 0:2, x, c], Z_R)
    got("w_zl", wo.at[zr, :, x, c])
    push("w_ozl", wo.at[zr, 2:4, x, c], Z_L)
    row(1)
    row(2)
    got("u_c0", us.at[co, base0 + y])
    got("u_c1", us.at[co, base1 + y])
    got("u_c0l", us.at[co, base0 + yl])
    got("u_c0r", us.at[co, base0 + yr])
    for h in (base0 + y, base1 + y, base0 + yl, base0 + yr):
        prepare_head(us, h, wq_ref, wkt_ref, wv_ref)
    ring_y(1, base1)
    got("d_or", wd.at[2 * xo + c, 0:128])
    push("d_coa", wd.at[2 * xo + c, 0:128], CORE)
    got("d_ol", wd.at[2 * xo + c, 128:256])
    push("d_cob", wd.at[2 * xo + c, 128:256], CORE)
    add(2 * xo + c)
    got("d_coa", wd.at[2 * xo + co, 0:128])
    got("d_cob", wd.at[2 * xo + co, 128:256])
    add(2 * xo + co)

    lq[0] = rms_rows(sums[:, 0:QR], qlg_ref[...]).astype(BF)
    push("q", lq.at[0], dev(zz=zmate), lq.at[1])
    kvb[y, z, 0:256] = rms_rows(sums[:, QR : QR + KR], klg_ref[...]).astype(BF)
    own = kvb.at[y, z]
    push("k_yr", own, Y_R)
    push("k_yl", own, Y_L)
    push("k_zn", own, Z_N)
    push("k_zm", own, Z_M)

    for j, base in ((0, base0), (1, base1)):
        got(f"u_y{j}or", us.at[c, base + yo, 0:2])
        got(f"u_y{j}ol", us.at[c, base + yo, 2:4])
        push(f"u_c{j}o", us.at[c, base + yo], CORE)
    got("w_ozr", wo.at[zo, 0:2, x, c])
    got("w_ozl", wo.at[zo, 2:4, x, c])
    row(3)
    got("u_c1l", us.at[co, base1 + yl])
    got("u_c1r", us.at[co, base1 + yr])
    got("u_c0o", us.at[co, base0 + yo])
    got("u_c1o", us.at[co, base1 + yo])
    push("w_c", wo.at[:, :, x, c], CORE)
    for h in (base0 + yo, base1 + yl, base1 + yr, base1 + yo):
        prepare_head(us, h, wq_ref, wkt_ref, wv_ref)
    make_queries(lq[0], sp, wq_ref, qgain_ref[...], lowq_ref, highq_ref, q_ref, 0)
    def k_y():
        got("k_yr", kvb.at[yl, z])
        push("k_oyr", lambda: kvb.at[yl, z, 0:160], Y_R)
        got("k_yl", kvb.at[yr, z])
        push("k_oyl", lambda: kvb.at[yr, z, 160:320], Y_L)

    def k_zn():
        got("k_zn", kvb.at[y, zn])
        push("k_ozm", lambda: kvb.at[y, zn, 0:160], Z_M)
        push("k_ynr", lambda: kvb.at[y, zn], Y_R)
        push("k_ynl", lambda: kvb.at[y, zn], Y_L)

    def k_zm():
        got("k_zm", kvb.at[y, zm])
        push("k_ozn", lambda: kvb.at[y, zm, 160:320], Z_N)
        push("k_ymr", lambda: kvb.at[y, zm], Y_R)
        push("k_yml", lambda: kvb.at[y, zm], Y_L)

    def k_oy():
        got("k_oyr", kvb.at[yo, z, 0:160])
        got("k_oyl", kvb.at[yo, z, 160:320])
        push("k_pzn", lambda: kvb.at[yo, z], Z_N)
        push("k_pzm", lambda: kvb.at[yo, z], Z_M)

    def k_oz():
        got("k_ozm", kvb.at[y, zo, 0:160])
        got("k_ozn", kvb.at[y, zo, 160:320])
        push("k_yor", lambda: kvb.at[y, zo], Y_R)
        push("k_yol", lambda: kvb.at[y, zo], Y_L)

    def k_pz():
        got("k_pzn", kvb.at[yo, zn])
        push("k_pozm", lambda: kvb.at[yo, zn, 0:160], Z_M)
        got("k_pzm", kvb.at[yo, zm])
        push("k_pozn", lambda: kvb.at[yo, zm, 160:320], Z_N)

    def k_yn():
        got("k_ynr", kvb.at[yl, zn])
        got("k_ynl", kvb.at[yr, zn])

    def k_ym():
        got("k_ymr", kvb.at[yl, zm])
        got("k_yml", kvb.at[yr, zm])

    def k_yo():
        got("k_yor", kvb.at[yl, zo])
        got("k_yol", kvb.at[yr, zo])

    def k_poz():
        got("k_pozm", kvb.at[yo, zo, 0:160])
        got("k_pozn", kvb.at[yo, zo, 160:320])

    def queries_mate():
        got("q", lq.at[1])
        make_queries(
            lq[1], zmate * 4 + y, wq_ref, qgain_ref[...], lowq_ref, highq_ref, q_ref, 1
        )

    def wx(k):
        def go():
            r = zrow[k]
            got(f"w_xr{k}", wo.at[r, :, xl, c])
            push(f"w_oxr{k}", lambda: wo.at[r, 0:2, xl, c], X_R)
            push(f"w_cl{k}", lambda: wo.at[r, :, xl, c], CORE)
            got(f"w_xl{k}", wo.at[r, :, xr, c])
            push(f"w_oxl{k}", lambda: wo.at[r, 2:4, xr, c], X_L)
            push(f"w_cr{k}", lambda: wo.at[r, :, xr, c], CORE)

        return go

    def wxo(k):
        r = zrow[k]
        got(f"w_oxr{k}", wo.at[r, 0:2, xo, c])
        got(f"w_oxl{k}", wo.at[r, 2:4, xo, c])
        push(f"w_co{k}", wo.at[r, :, xo, c], CORE)

    hfirst = (z // 2) * LOCAL
    b_own, b_mate = sp, zmate * 4 + y

    def send_mate():
        close_heads(acc_ref, 1, att_ref, HEADS)
        push("att", lambda: att_ref.at[HEADS : HEADS + LOCAL], dev(zz=zmate), att_ref.at[pl.ds(hfirst, LOCAL)])

    def pick(test, yes, no):
        return no + test.astype(jnp.int32) * (yes - no)

    def source(step):
        dy = pick(step < 3, step, pick(step < 5, 0, pick(step < 7, step - 4, pick(
            step == 7, 0, pick(step == 8, 3, pick(step < 11, step - 8, pick(
                step < 13, 3, pick(step < 15, step - 12, 3))))))))
        dz = pick(step < 3, 0, pick(step < 5, step - 2, pick(step < 7, 1, pick(
            step == 7, 3, pick(step == 8, 0, pick(step < 11, 2, pick(
                step < 13, step - 10, 3)))))))
        yy = pick(dy == 0, y, pick(dy == 1, yl, pick(dy == 2, yr, yo)))
        zz = pick(dz == 0, z, pick(dz == 1, zn, pick(dz == 2, zm, zo)))
        return yy, zz, zz * 4 + yy

    b_last = jnp.maximum(b_own, b_mate)

    def expand_step(step, slot):
        yy, zz, b = source(step)
        expand(
            kvb[yy, zz], b, wkt_ref, wv_ref, gk_ref, gr_ref, lowk_ref, highk_ref, kt_ref,
            v_ref, slot,
        )

    def attend_to(which, slot, diagonal=False):
        attend(diagonal, q_ref, kt_ref, v_ref, m_ref, acc_ref, which, slot)

    def singles(b0, b1, own0, own1, skip_own, skip_mate):
        def single(j, _):
            which, slot = j // 2, j % 2
            b = pick(slot == 0, b0, b1)
            mine = pick(slot == 0, own0.astype(jnp.int32), own1.astype(jnp.int32)) * (1 - skip_own)
            mates = (b < b_mate).astype(jnp.int32) * (1 - skip_mate)

            @pl.when(pick(which == 0, mine, mates) == 1)
            def _():
                attend_to(which, slot)

            @pl.when((b == b_mate) & (which == 1))
            def _():
                attend_to(which, slot, True)

            return 0

        lax.fori_loop(0, 4, single, 0)

    zero = z - z
    expand_step(zero, 0)
    attend_to(0, 0, True)
    k_y()
    k_zn()
    expand_step(zero + 1, 0)
    expand_step(zero + 2, 1)
    queries_mate()
    mate_both = (source(zero + 1)[2] < b_mate) & (source(zero + 2)[2] < b_mate)

    @pl.when(mate_both)
    def _():
        attend_pair(q_ref, kt_ref, v_ref, m_ref, acc_ref, 1)

    at_pair = {1: (k_oy, k_zm, wx(0)), 2: (k_yn, k_oz), 3: (k_pz, wx(1)), 4: (k_ym, wx(2)),
               5: (wx(3),), 6: (k_yo,), 7: (k_poz,)}

    def pair(i, _):
        for when, todo in at_pair.items():
            @pl.when(i == when)
            def _(todo=todo):
                for f in todo:
                    f()

        first = pick(i == 7, 0, 2 * i + 1)
        second = pick(i == 7, 15, 2 * i + 2)
        b0, b1 = source(first)[2], source(second)[2]
        own0 = (b0 < b_own) & (i > 0) & (first > 0)
        own1 = (b1 < b_own) & (i > 0) & (second != 8)
        own_both = own0 & own1
        mate_both = (b0 < b_mate) & (b1 < b_mate)
        either = (own_both | mate_both) & (i > 0)
        needed = ((b0 <= b_last) | (b1 <= b_last)) & (i > 0)
        lead = pick(own_both, 0, 1)

        @pl.when(either)
        def _():
            expand_step(first, 0)
            expand_step(second, 1)
            attend_pair(q_ref, kt_ref, v_ref, m_ref, acc_ref, lead)

        @pl.when(jnp.logical_not(either) & needed)
        def _():
            expand_step(first, 0)
            expand_step(second, 1)

        @pl.when(own_both & mate_both)
        def _():
            attend_pair(q_ref, kt_ref, v_ref, m_ref, acc_ref, 1)

        @pl.when(jnp.logical_not(own_both & mate_both))
        def _():
            singles(b0, b1, own0, own1, own_both.astype(jnp.int32), mate_both.astype(jnp.int32))

        return 0

    lax.fori_loop(0, 8, pair, 0)
    send_mate()

    def last(j, _):
        step = pick(j == 2, 8, j + 1)

        @pl.when(source(step)[2] < b_own)
        def _():
            expand_step(step, 0)
            attend_to(0, 0)

        return 0

    lax.fori_loop(0, 3, last, 0)
    close_heads(acc_ref, 0, att_ref, hfirst)
    for k in range(4):
        wxo(k)
    got("w_c", wo.at[:, :, x, co])
    for k in range(4):
        got(f"w_cl{k}", wo.at[zrow[k], :, xl, co])
        got(f"w_cr{k}", wo.at[zrow[k], :, xr, co])
        got(f"w_co{k}", wo.at[zrow[k], :, xo, co])
    got("att", att_ref.at[pl.ds(LOCAL - hfirst, LOCAL)])
    finish(att_ref, mixed_ref, ogain_ref, wo, out_ref)
    for i, again in sent:
        view = again()
        pltpu.make_async_copy(view, view, ssem.at[i]).wait()
    assert len(names) <= SLOTS


def per_device(
    tokens, in_gain, w_query_down, w_latent_down, w_rope_key, query_latent_gain, latent_gain,
    w_query_up, w_key_up, w_value_up, query_gain, key_gain, out_gain, w_out,
):
    blocks = lax.axis_size("sp")
    tables = [jnp.asarray(t) for t in rope_tables(blocks)]
    vm = pl.BlockSpec(memory_space=pltpu.VMEM)
    hbm = pl.BlockSpec(memory_space=pl.ANY)
    args = (
        tokens.reshape(ROWS, D), in_gain.reshape(1, D), w_query_down, w_latent_down, w_rope_key.T,
        query_latent_gain.reshape(1, QR), latent_gain.reshape(1, KR), w_query_up, w_key_up,
        w_value_up, query_gain.reshape(1, QK), key_gain.reshape(1, QK), out_gain.reshape(1, D), w_out, *tables,
    )
    out = pl.pallas_call(
        kernel,
        out_shape=pltpu.VMEM((ROWS, D), BF),
        in_specs=[hbm if i in (0, 2, 3, 4, 7, 8, 9) or i > 12 else vm for i in range(len(args))],
        out_specs=vm,
        scratch_shapes=[
            pltpu.VMEM((8, 256, QR + KR), BF),
            pltpu.VMEM((2, LOCAL, 4, 160, 128), BF),
            pltpu.VMEM((4, 4, 4, 2, 16, D), BF),
            pltpu.VMEM((4, 4, 320, 256), BF),
            pltpu.VMEM((2, ROWS, QR), BF),
            pltpu.VMEM((8, ROWS, 256), BF),
            pltpu.VMEM((ROWS, QR + KR), F32),
            pltpu.VMEM((LOCAL, QR, 256), BF),
            pltpu.VMEM((LOCAL, NOPE, KR), BF),
            pltpu.VMEM((LOCAL // 2, KR, 2 * VD), BF),
            pltpu.VMEM((2, LOCAL, ROWS, 256), BF),
            pltpu.VMEM((KEPT, LOCAL, 256, 256), BF),
            pltpu.VMEM((KEPT, LOCAL, 256, 256), BF),
            pltpu.VMEM((2, LOCAL, ROWS, 128), F32),
            pltpu.VMEM((2, LOCAL, ROWS, 256), F32),
            pltpu.VMEM((HEADS + LOCAL, ROWS, VD), BF),
            pltpu.VMEM((ROWS, D), BF),
            pltpu.VMEM((1, 256), F32),
            pltpu.VMEM((NOPE, 256), F32),
            pltpu.VMEM((ROPE, 256), F32),
            pltpu.VMEM((ROWS, D), BF),
            pltpu.VMEM((ROPE, D), BF),
            pltpu.VMEM((64, QK), BF),
        ]
        + [pltpu.VMEM(t.shape, F32) for t in tables]
        + [
            pltpu.SemaphoreType.DMA((12,)),
            pltpu.SemaphoreType.DMA((SLOTS,)),
            pltpu.SemaphoreType.DMA((SLOTS,)),
        ],
        compiler_params=pltpu.CompilerParams(
            vmem_limit_bytes=60 * 1024 * 1024, collective_id=0, has_side_effects=True
        ),
    )(*args)
    return out.reshape(1, ROWS, D)


def solution(mesh):
    in_specs = (
        P("dp", "sp", None), P(), P("dp", None), P("dp", None), P(), P(), P(),
        P("dp", "sp"), P("dp", "sp"), P("dp", "sp"), P(), P(), P(), P(("sp", "dp"), None),
    )
    return jax.shard_map(
        per_device, mesh=mesh, in_specs=in_specs, out_specs=P("dp", "sp", None), check_vma=False
    )
```

```python
import functools

import jax
import jax.numpy as jnp
import numpy as np
from jax import lax
from jax.experimental import pallas as pl
from jax.experimental.pallas import tpu as pltpu
from jax.sharding import PartitionSpec as P

HEADS, NOPE, ROPE, VD, QR, KR, QK = 16, 128, 64, 128, 512, 256, 192
D = 2048
ROWS = 256
EPS = 1e-06
THETA = 10000.0
NEG_BIG = -1e30
BF, F32 = jnp.bfloat16, jnp.float32
SOFT = float(QK**-0.5 * np.log2(np.e))
LOCAL = 8


def rope_tables(blocks):
    half = ROPE // 2
    freq = THETA ** (-np.arange(half) / half)
    low = np.arange(ROWS)[:, None] * freq[None, :]
    high = (np.arange(blocks) * ROWS)[:, None] * freq[None, :]
    pad = np.zeros((ROWS, 128 - ROPE))
    lowq = np.stack([np.concatenate([f(low), f(low), pad], 1) for f in (np.cos, np.sin)])
    hpad = np.zeros((blocks, 128 - ROPE))
    highq = np.stack([np.concatenate([f(high), f(high), hpad], 1) for f in (np.cos, np.sin)], 1)
    highq = np.broadcast_to(highq[:, :, None, :], (blocks, 2, 8, 128))
    lowk = np.concatenate([np.cos(low).T, np.sin(low).T], 0)
    highk = np.concatenate([np.cos(high), np.sin(high)], 1)
    highk = np.broadcast_to(highk[:, :, None], (blocks, ROPE, 128))
    return [np.ascontiguousarray(t, dtype=np.float32) for t in (lowq, highq, lowk, highk)]


def dot(a, b):
    return lax.dot_general(a, b, (((1,), (0,)), ((), ())), preferred_element_type=F32)


def dot_nt(a, b):
    return lax.dot_general(a, b, (((1,), (1,)), ((), ())), preferred_element_type=F32)


def prepare_head(us, h, wq_ref, wkt_ref, wv_ref):
    keys = []
    for x in range(4):
        for c in range(2):
            d = 2 * x + c
            unit = us[c, h, x]
            rows = slice(d * 64, d * 64 + 64)
            wq_ref[h, rows, 0:NOPE] = unit[0:64]
            wq_ref[h, d * 64 : d * 64 + 32, NOPE:QK] = unit[64:96, 0:ROPE]
            wq_ref[h, d * 64 + 32 : d * 64 + 64, NOPE:QK] = unit[64:96, ROPE:128]
            keys.append(unit[96:128])
            wv_ref[h // 2, d * 32 : d * 32 + 32, pl.ds(pl.multiple_of(h % 2 * VD, VD), VD)] = unit[128:160]
    wkt_ref[h] = jnp.concatenate(keys, axis=0).T


def make_queries(latq, block, wq_ref, qgain, lowq_ref, highq_ref, q_ref, which):
    ch, sh = highq_ref[block, 0, 0:1], highq_ref[block, 1, 0:1]
    cl, sl = lowq_ref[0], lowq_ref[1]
    cosine = ch * cl - sh * sl
    sine = sh * cl + ch * sl
    lane = lax.broadcasted_iota(jnp.int32, (ROWS, 128), 1)
    sine_a = jnp.where(lane < ROPE // 2, -sine, 0.0)
    sine_b = jnp.where(lane < ROPE // 2, 0.0, sine)

    for h in range(LOCAL):
        q = dot(latq, wq_ref[h])
        scale = lax.rsqrt(jnp.sum(q * q, axis=1, keepdims=True) * (1.0 / QK) + EPS)
        n = q * scale * qgain
        t = n[:, NOPE:256]
        turned = (
            t * cosine
            + pltpu.roll(t, 128 - ROPE // 2, 1) * sine_a
            + pltpu.roll(t, ROPE // 2, 1) * sine_b
        )
        q_ref[which, h, :, 0:NOPE] = n[:, 0:NOPE].astype(BF)
        q_ref[which, h, :, NOPE:256] = turned.astype(BF)


def expand(unit, block, wkt_ref, wv_ref, gk_ref, gr_ref, lowk_ref, highk_ref, kt_ref, v_ref, slot):
    kv = unit[0:256, :]
    rope = unit[256:320, :].astype(F32)
    half = ROPE // 2
    ch = jnp.concatenate([highk_ref[block, 0:half]] * 2, axis=1)
    sh = jnp.concatenate([highk_ref[block, half:ROPE]] * 2, axis=1)
    cl, sl = lowk_ref[0:half], lowk_ref[half:ROPE]
    cosine = ch * cl - sh * sl
    sine = sh * cl + ch * sl
    rope_sq = jnp.sum(rope * rope, axis=0, keepdims=True)
    x = rope * gr_ref[...]
    a, b = x[0:half], x[half:ROPE]
    turned = jnp.concatenate([a * cosine - b * sine, b * cosine + a * sine], axis=0)
    kt = dot_nt(wkt_ref[...].reshape(LOCAL * NOPE, KR), kv)
    for h in range(LOCAL):
        k = kt[h * NOPE : (h + 1) * NOPE]
        scale = lax.rsqrt((jnp.sum(k * k, axis=0, keepdims=True) + rope_sq) * (1.0 / QK) + EPS)
        kt_ref[slot, h, 0:NOPE] = (k * scale * gk_ref[...]).astype(BF)
        kt_ref[slot, h, NOPE:QK] = (turned * scale).astype(BF)
    for h in range(0, LOCAL, 2):
        v = dot(kv, wv_ref[h // 2]).astype(BF)
        v_ref[slot, h, :, 0:VD] = v[:, 0:VD]
        v_ref[slot, h + 1, :, 0:VD] = v[:, VD : 2 * VD]


def attend(diagonal, q_ref, kt_ref, v_ref, m_ref, acc_ref, which, slot):
    for h in range(LOCAL):
        s = dot(q_ref[which, h], kt_ref[slot, h])
        if diagonal:
            row = lax.broadcasted_iota(jnp.int32, (ROWS, ROWS), 0)
            col = lax.broadcasted_iota(jnp.int32, (ROWS, ROWS), 1)
            s = jnp.where(col <= row, s, NEG_BIG)
        old = m_ref[which, h]
        new = jnp.maximum(old, jnp.max(s, axis=1, keepdims=True))
        fade = jnp.exp2((old - new) * SOFT)
        p = jnp.exp2((s - jnp.concatenate([new, new], 1)) * SOFT).astype(BF)
        m_ref[which, h] = new
        acc_ref[which, h] = acc_ref[which, h] * jnp.concatenate([fade, fade], 1) + dot(
            p, v_ref[slot, h]
        )


def attend_pair(q_ref, kt_ref, v_ref, m_ref, acc_ref, which):
    def score(h):
        q = q_ref[which, h]
        return dot(q, kt_ref[0, h]), dot(q, kt_ref[1, h])

    s0, s1 = score(0)
    for h in range(LOCAL):
        ahead = score(h + 1) if h + 1 < LOCAL else None
        old = m_ref[which, h]
        new = jnp.maximum(old, jnp.max(jnp.maximum(s0, s1), axis=1, keepdims=True))
        fade = jnp.exp2((old - new) * SOFT)
        wide = jnp.concatenate([new, new], 1)
        p0 = jnp.exp2((s0 - wide) * SOFT).astype(BF)
        p1 = jnp.exp2((s1 - wide) * SOFT).astype(BF)
        m_ref[which, h] = new
        acc_ref[which, h] = acc_ref[which, h] * jnp.concatenate([fade, fade], 1) + (
            dot(p0, v_ref[0, h]) + dot(p1, v_ref[1, h])
        )
        if ahead is not None:
            s0, s1 = ahead


def close_heads(acc_ref, which, att_ref, first):
    for h in range(LOCAL):
        att_ref[first + h] = (
            acc_ref[which, h, :, 0:VD] / acc_ref[which, h, :, VD : 2 * VD]
        ).astype(BF)


def finish(att_ref, mixed_ref, ogain_ref, wo_ref, out_ref):
    total = jnp.zeros((ROWS, VD), F32)
    for h in range(HEADS):
        at = att_ref[h].astype(F32)
        total = total + at * at
    scale = lax.rsqrt(jnp.sum(total, axis=1, keepdims=True) * (1.0 / (HEADS * VD)) + EPS)
    for h in range(HEADS):
        cols = slice(h * VD, (h + 1) * VD)
        mixed_ref[:, cols] = (att_ref[h].astype(F32) * scale * ogain_ref[:, cols]).astype(BF)

    def one(j, _):
        cols = pl.ds(pl.multiple_of(j * 512, 512), 512)
        w = wo_ref[:, :, :, :, :, cols].reshape(HEADS * VD, 512)
        out_ref[:, cols] = dot(mixed_ref[...], w).astype(BF)
        return 0

    lax.fori_loop(0, D // 512, one, 0)


def rms_rows(values, scaling):
    return values * lax.rsqrt(jnp.mean(values * values, axis=-1, keepdims=True) + EPS) * scaling


SLOTS = 128
KEPT = 2


def kernel(
    tok_in, ing_ref, wqd_in, wld_in, wrt_in, qlg_ref, klg_ref, wqu_in, wku_in, wvu_in,
    qg_ref, kg_ref, ogain_ref, wo_in, lowq_in, highq_in, lowk_in, highk_in,
    out_ref,
    wd, us, wo, kvb, lq, normed, sums, wq_ref, wkt_ref, wv_ref, q_ref, kt_ref, v_ref,
    m_ref, acc_ref, att_ref, mixed_ref, qgain_ref, gk_ref, gr_ref,
    tok_ref, wrt_ref, wqu_ref, lowq_ref, highq_ref, lowk_ref, highk_ref, lsem, ssem, rsem,
):
    sp, dp = lax.axis_index("sp"), lax.axis_index("dp")
    z, y = sp // 4, sp % 4
    x, c = dp // 2, dp % 2
    xl, xr, xo = (x + 3) % 4, (x + 1) % 4, (x + 2) % 4
    yl, yr, yo = (y + 3) % 4, (y + 1) % 4, (y + 2) % 4
    zl, zr, zo = (z + 3) % 4, (z + 1) % 4, (z + 2) % 4
    co = 1 - c
    zb = z % 2
    zpair = z + 1 - 2 * zb
    zmate = 3 - z

    def dev(xx=x, yy=y, zz=z, cc=c):
        return {"sp": zz * 4 + yy, "dp": xx * 2 + cc}

    X_R, X_L, Y_R, Y_L, Z_R, Z_L, CORE = (
        dev(xx=xr), dev(xx=xl), dev(yy=yr), dev(yy=yl), dev(zz=zr), dev(zz=zl), dev(cc=co)
    )
    zn, zm = zpair, (z + 3 + 2 * zb) % 4
    Z_N, Z_M = dev(zz=zn), dev(zz=zm)
    names, sent = {}, []

    def number(name):
        return names.setdefault(name, len(names))

    def push(name, view, to, dst=None):
        i = number(name)
        again = view if callable(view) else functools.partial(lambda v: v, view)
        view = again()
        pltpu.make_async_remote_copy(
            src_ref=view, dst_ref=view if dst is None else dst, send_sem=ssem.at[i],
            recv_sem=rsem.at[i], device_id=to, device_id_type=pl.DeviceIdType.MESH,
        ).start()
        sent.append((i, again))

    def got(name, view):
        pltpu.make_async_copy(view, view, rsem.at[number(name)]).wait()

    barrier = pltpu.get_barrier_semaphore()
    X_O, Y_O = dev(xx=xo), dev(yy=yo)
    for to in (X_R, X_L, X_O, Y_R, Y_L, Y_O, Z_R, Z_L, CORE):
        pl.semaphore_signal(barrier, 1, device_id=to, device_id_type=pl.DeviceIdType.MESH)

    hl = zb * 4 + y
    loads = [
        pltpu.make_async_copy(src, dst, lsem.at[i])
        for i, (src, dst) in enumerate((
            (wqu_in, wqu_ref), (wku_in, us.at[c, hl, x, 96:128]),
            (wvu_in, us.at[c, hl, x, 128:160]), (wo_in, wo.at[z, y, x, c]),
            (wqd_in, wd.at[dp, :, 0:QR]), (wld_in, wd.at[dp, :, QR : QR + KR]),
            (tok_in, tok_ref), (wrt_in, wrt_ref), (lowq_in, lowq_ref), (highq_in, highq_ref),
            (lowk_in, lowk_ref), (highk_in, highk_ref),
        ))
    ]
    for load in loads:
        load.start()
    loads[0].wait()
    us[c, hl, x, 0:64] = wqu_ref[:, 0:NOPE]
    us[c, hl, x, 64:96] = jnp.concatenate(
        [wqu_ref[0:32, NOPE:QK], wqu_ref[32:64, NOPE:QK]], axis=1
    )
    for load in loads[1:4]:
        load.wait()
    pl.semaphore_wait(barrier, 9)

    uown = us.at[c, hl, x]
    push("u_r", uown, X_R)
    push("u_l", uown, X_L)
    push("u_o", uown, X_O)
    wown = wo.at[z, y, x, c]
    push("w_yr", wown, Y_R)
    push("w_yl", wown, Y_L)
    push("w_yo", wown, Y_O)
    loads[4].wait()
    loads[5].wait()
    down = wd.at[dp]
    push("d_ra", wd.at[dp, 0:128], X_R)
    push("d_la", wd.at[dp, 128:256], X_L)
    push("d_rb", wd.at[dp, 128:256], X_R)
    push("d_lb", wd.at[dp, 0:128], X_L)
    push("d_c", down, CORE)

    for load in loads[6:]:
        load.wait()
    for r in range(0, ROWS, 64):
        rows = slice(r, r + 64)
        n = rms_rows(tok_ref[rows].astype(F32), ing_ref[...]).astype(BF)
        for k in range(8):
            normed[k, rows] = n[:, k * 256 : (k + 1) * 256]

    qgain_ref[:, 0:NOPE] = qg_ref[:, 0:NOPE]
    qgain_ref[:, NOPE:256] = jnp.concatenate(
        [qg_ref[:, NOPE:QK], jnp.zeros((1, 256 - QK), F32)], axis=1
    )
    kg = jnp.concatenate([kg_ref[...], jnp.zeros((1, 256 - QK), F32)], axis=1)
    column = jnp.broadcast_to(kg[:, 0:NOPE], (NOPE, NOPE)).T
    gk_ref[...] = jnp.concatenate([column, column], axis=1)
    column = jnp.broadcast_to(kg[:, NOPE:256], (NOPE, NOPE)).T[0:ROPE]
    gr_ref[...] = jnp.concatenate([column, column], axis=1)

    got("u_r", us.at[c, hl, xl])
    got("u_l", us.at[c, hl, xr])
    got("u_o", us.at[c, hl, xo])
    block0 = us.at[c, hl]
    push("u_z", block0, dev(zz=zpair))
    push("u_y0r", block0, Y_R)
    push("u_y0l", block0, Y_L)
    push("u_c0", block0, CORE)
    got("w_yr", wo.at[z, yl, x, c])
    got("w_yl", wo.at[z, yr, x, c])
    got("w_yo", wo.at[z, yo, x, c])
    push("w_zr", wo.at[z, :, x, c], Z_R)
    push("w_zl", wo.at[z, :, x, c], Z_L)

    def add(d, first=False):
        part = dot(normed[d], wd[d])
        if first:
            sums[...] = part
        else:
            sums[...] += part

    add(dp, True)
    got("d_c", wd.at[2 * x + co])
    add(2 * x + co)
    m_ref[...] = jnp.full(m_ref.shape, NEG_BIG, F32)
    acc_ref[...] = jnp.zeros(acc_ref.shape, F32)
    wq_ref[:, :, QK:256] = jnp.zeros((LOCAL, QR, 256 - QK), BF)
    kt_ref[:, :, QK:256, :] = jnp.zeros((KEPT, LOCAL, 256 - QK, 256), BF)
    v_ref[:, :, :, VD:256] = jnp.ones((KEPT, LOCAL, ROWS, 256 - VD), BF)
    rope_t = jnp.zeros((ROPE, ROWS), F32)
    for k in range(8):
        rope_t = rope_t + dot_nt(wrt_ref[:, k * 256 : (k + 1) * 256], normed[k])
    kvb[y, z, 256:320] = rope_t.astype(BF)
    base0, base1 = zb * 4, 4 - zb * 4
    block1 = us.at[c, base1 + y]

    def ring_y(j, base):
        got(f"u_y{j}r", us.at[c, base + yl])
        push(f"u_y{j}or", us.at[c, base + yl, 0:2], Y_R)
        push(f"u_c{j}l", us.at[c, base + yl], CORE)
        got(f"u_y{j}l", us.at[c, base + yr])
        push(f"u_y{j}ol", us.at[c, base + yr, 2:4], Y_L)
        push(f"u_c{j}r", us.at[c, base + yr], CORE)

    got("d_ra", wd.at[2 * xl + c, 0:128])
    push("d_or", wd.at[2 * xl + c, 0:128], X_R)
    got("d_la", wd.at[2 * xr + c, 128:256])
    push("d_ol", wd.at[2 * xr + c, 128:256], X_L)
    got("u_z", us.at[c, base1 + y])
    push("u_y1r", block1, Y_R)
    push("u_y1l", block1, Y_L)
    push("u_c1", block1, CORE)
    ring_y(0, base0)
    got("d_rb", wd.at[2 * xl + c, 128:256])
    push("d_cl", wd.at[2 * xl + c], CORE)
    got("d_lb", wd.at[2 * xr + c, 0:128])
    push("d_cr", wd.at[2 * xr + c], CORE)
    add(2 * xl + c)
    add(2 * xr + c)
    got("d_cl", wd.at[2 * xl + co])
    add(2 * xl + co)
    got("d_cr", wd.at[2 * xr + co])
    add(2 * xr + co)
    zrow = (z, zl, zr, zo)

    def row(k):
        push(f"w_xr{k}", wo.at[zrow[k], :, x, c], X_R)
        push(f"w_xl{k}", wo.at[zrow[k], :, x, c], X_L)

    row(0)
    got("w_zr", wo.at[zl, :, x, c])
    push("w_ozr", wo.at[zl, 0:2, x, c], Z_R)
    got("w_zl", wo.at[zr, :, x, c])
    push("w_ozl", wo.at[zr, 2:4, x, c], Z_L)
    row(1)
    row(2)
    got("u_c0", us.at[co, base0 + y])
    got("u_c1", us.at[co, base1 + y])
    got("u_c0l", us.at[co, base0 + yl])
    got("u_c0r", us.at[co, base0 + yr])
    for h in (base0 + y, base1 + y, base0 + yl, base0 + yr):
        prepare_head(us, h, wq_ref, wkt_ref, wv_ref)
    ring_y(1, base1)
    got("d_or", wd.at[2 * xo + c, 0:128])
    push("d_coa", wd.at[2 * xo + c, 0:128], CORE)
    got("d_ol", wd.at[2 * xo + c, 128:256])
    push("d_cob", wd.at[2 * xo + c, 128:256], CORE)
    add(2 * xo + c)
    got("d_coa", wd.at[2 * xo + co, 0:128])
    got("d_cob", wd.at[2 * xo + co, 128:256])
    add(2 * xo + co)

    lq[0] = rms_rows(sums[:, 0:QR], qlg_ref[...]).astype(BF)
    push("q", lq.at[0], dev(zz=zmate), lq.at[1])
    kvb[y, z, 0:256] = rms_rows(sums[:, QR : QR + KR], klg_ref[...]).astype(BF)
    own = kvb.at[y, z]
    push("k_yr", own, Y_R)
    push("k_yl", own, Y_L)
    push("k_zn", own, Z_N)
    push("k_zm", own, Z_M)

    for j, base in ((0, base0), (1, base1)):
        got(f"u_y{j}or", us.at[c, base + yo, 0:2])
        got(f"u_y{j}ol", us.at[c, base + yo, 2:4])
        push(f"u_c{j}o", us.at[c, base + yo], CORE)
    got("w_ozr", wo.at[zo, 0:2, x, c])
    got("w_ozl", wo.at[zo, 2:4, x, c])
    row(3)
    got("u_c1l", us.at[co, base1 + yl])
    got("u_c1r", us.at[co, base1 + yr])
    got("u_c0o", us.at[co, base0 + yo])
    got("u_c1o", us.at[co, base1 + yo])
    push("w_c", wo.at[:, :, x, c], CORE)
    for h in (base0 + yo, base1 + yl, base1 + yr, base1 + yo):
        prepare_head(us, h, wq_ref, wkt_ref, wv_ref)
    make_queries(lq[0], sp, wq_ref, qgain_ref[...], lowq_ref, highq_ref, q_ref, 0)
    def k_y():
        got("k_yr", kvb.at[yl, z])
        push("k_oyr", lambda: kvb.at[yl, z, 0:160], Y_R)
        got("k_yl", kvb.at[yr, z])
        push("k_oyl", lambda: kvb.at[yr, z, 160:320], Y_L)

    def k_zn():
        got("k_zn", kvb.at[y, zn])
        push("k_ozm", lambda: kvb.at[y, zn, 0:160], Z_M)
        push("k_ynr", lambda: kvb.at[y, zn], Y_R)
        push("k_ynl", lambda: kvb.at[y, zn], Y_L)

    def k_zm():
        got("k_zm", kvb.at[y, zm])
        push("k_ozn", lambda: kvb.at[y, zm, 160:320], Z_N)
        push("k_ymr", lambda: kvb.at[y, zm], Y_R)
        push("k_yml", lambda: kvb.at[y, zm], Y_L)

    def k_oy():
        got("k_oyr", kvb.at[yo, z, 0:160])
        got("k_oyl", kvb.at[yo, z, 160:320])
        push("k_pzn", lambda: kvb.at[yo, z], Z_N)
        push("k_pzm", lambda: kvb.at[yo, z], Z_M)

    def k_oz():
        got("k_ozm", kvb.at[y, zo, 0:160])
        got("k_ozn", kvb.at[y, zo, 160:320])
        push("k_yor", lambda: kvb.at[y, zo], Y_R)
        push("k_yol", lambda: kvb.at[y, zo], Y_L)

    def k_pz():
        got("k_pzn", kvb.at[yo, zn])
        push("k_pozm", lambda: kvb.at[yo, zn, 0:160], Z_M)
        got("k_pzm", kvb.at[yo, zm])
        push("k_pozn", lambda: kvb.at[yo, zm, 160:320], Z_N)

    def k_yn():
        got("k_ynr", kvb.at[yl, zn])
        got("k_ynl", kvb.at[yr, zn])

    def k_ym():
        got("k_ymr", kvb.at[yl, zm])
        got("k_yml", kvb.at[yr, zm])

    def k_yo():
        got("k_yor", kvb.at[yl, zo])
        got("k_yol", kvb.at[yr, zo])

    def k_poz():
        got("k_pozm", kvb.at[yo, zo, 0:160])
        got("k_pozn", kvb.at[yo, zo, 160:320])

    def queries_mate():
        got("q", lq.at[1])
        make_queries(
            lq[1], zmate * 4 + y, wq_ref, qgain_ref[...], lowq_ref, highq_ref, q_ref, 1
        )

    def wx(k):
        def go():
            r = zrow[k]
            got(f"w_xr{k}", wo.at[r, :, xl, c])
            push(f"w_oxr{k}", lambda: wo.at[r, 0:2, xl, c], X_R)
            push(f"w_cl{k}", lambda: wo.at[r, :, xl, c], CORE)
            got(f"w_xl{k}", wo.at[r, :, xr, c])
            push(f"w_oxl{k}", lambda: wo.at[r, 2:4, xr, c], X_L)
            push(f"w_cr{k}", lambda: wo.at[r, :, xr, c], CORE)

        return go

    def wxo(k):
        r = zrow[k]
        got(f"w_oxr{k}", wo.at[r, 0:2, xo, c])
        got(f"w_oxl{k}", wo.at[r, 2:4, xo, c])
        push(f"w_co{k}", wo.at[r, :, xo, c], CORE)

    hfirst = (z // 2) * LOCAL
    b_own, b_mate = sp, zmate * 4 + y

    def send_mate():
        close_heads(acc_ref, 1, att_ref, HEADS)
        push("att", lambda: att_ref.at[HEADS : HEADS + LOCAL], dev(zz=zmate), att_ref.at[pl.ds(hfirst, LOCAL)])

    def pick(test, yes, no):
        return no + test.astype(jnp.int32) * (yes - no)

    def source(step):
        dy = pick(step < 3, step, pick(step < 5, 0, pick(step < 7, step - 4, pick(
            step == 7, 0, pick(step == 8, 3, pick(step < 11, step - 8, pick(
                step < 13, 3, pick(step < 15, step - 12, 3))))))))
        dz = pick(step < 3, 0, pick(step < 5, step - 2, pick(step < 7, 1, pick(
            step == 7, 3, pick(step == 8, 0, pick(step < 11, 2, pick(
                step < 13, step - 10, 3)))))))
        yy = pick(dy == 0, y, pick(dy == 1, yl, pick(dy == 2, yr, yo)))
        zz = pick(dz == 0, z, pick(dz == 1, zn, pick(dz == 2, zm, zo)))
        return yy, zz, zz * 4 + yy

    b_last = jnp.maximum(b_own, b_mate)

    def expand_step(step, slot):
        yy, zz, b = source(step)
        expand(
            kvb[yy, zz], b, wkt_ref, wv_ref, gk_ref, gr_ref, lowk_ref, highk_ref, kt_ref,
            v_ref, slot,
        )

    def attend_to(which, slot, diagonal=False):
        attend(diagonal, q_ref, kt_ref, v_ref, m_ref, acc_ref, which, slot)

    def singles(b0, b1, own0, own1, skip_own, skip_mate):
        def single(j, _):
            which, slot = j // 2, j % 2
            b = pick(slot == 0, b0, b1)
            mine = pick(slot == 0, own0.astype(jnp.int32), own1.astype(jnp.int32)) * (1 - skip_own)
            mates = (b < b_mate).astype(jnp.int32) * (1 - skip_mate)

            @pl.when(pick(which == 0, mine, mates) == 1)
            def _():
                attend_to(which, slot)

            @pl.when((b == b_mate) & (which == 1))
            def _():
                attend_to(which, slot, True)

            return 0

        lax.fori_loop(0, 4, single, 0)

    zero = z - z
    expand_step(zero, 0)
    attend_to(0, 0, True)
    k_y()
    k_zn()
    expand_step(zero + 1, 0)
    expand_step(zero + 2, 1)
    queries_mate()
    mate_both = (source(zero + 1)[2] < b_mate) & (source(zero + 2)[2] < b_mate)

    @pl.when(mate_both)
    def _():
        attend_pair(q_ref, kt_ref, v_ref, m_ref, acc_ref, 1)

    at_pair = {1: (k_zm, k_oy, wx(0)), 2: (k_yn,), 3: (k_oz, k_pz, wx(1)), 4: (k_ym, wx(2)),
               5: (wx(3),), 6: (k_yo,), 7: (k_poz,)}

    def pair(i, _):
        for when, todo in at_pair.items():
            @pl.when(i == when)
            def _(todo=todo):
                for f in todo:
                    f()

        first = pick(i == 7, 0, 2 * i + 1)
        second = pick(i == 7, 15, 2 * i + 2)
        b0, b1 = source(first)[2], source(second)[2]
        own0 = (b0 < b_own) & (i > 0) & (first > 0)
        own1 = (b1 < b_own) & (i > 0) & (second != 8)
        own_both = own0 & own1
        mate_both = (b0 < b_mate) & (b1 < b_mate)
        either = (own_both | mate_both) & (i > 0)
        needed = ((b0 <= b_last) | (b1 <= b_last)) & (i > 0)
        lead = pick(own_both, 0, 1)

        @pl.when(either)
        def _():
            expand_step(first, 0)
            expand_step(second, 1)
            attend_pair(q_ref, kt_ref, v_ref, m_ref, acc_ref, lead)

        @pl.when(jnp.logical_not(either) & needed)
        def _():
            expand_step(first, 0)
            expand_step(second, 1)

        @pl.when(own_both & mate_both)
        def _():
            attend_pair(q_ref, kt_ref, v_ref, m_ref, acc_ref, 1)

        @pl.when(jnp.logical_not(own_both & mate_both))
        def _():
            singles(b0, b1, own0, own1, own_both.astype(jnp.int32), mate_both.astype(jnp.int32))

        return 0

    lax.fori_loop(0, 8, pair, 0)
    send_mate()

    def last(j, _):
        step = pick(j == 2, 8, j + 1)

        @pl.when(source(step)[2] < b_own)
        def _():
            expand_step(step, 0)
            attend_to(0, 0)

        return 0

    lax.fori_loop(0, 3, last, 0)
    close_heads(acc_ref, 0, att_ref, hfirst)
    for k in range(4):
        wxo(k)
    got("w_c", wo.at[:, :, x, co])
    for k in range(4):
        got(f"w_cl{k}", wo.at[zrow[k], :, xl, co])
        got(f"w_cr{k}", wo.at[zrow[k], :, xr, co])
        got(f"w_co{k}", wo.at[zrow[k], :, xo, co])
    got("att", att_ref.at[pl.ds(LOCAL - hfirst, LOCAL)])
    finish(att_ref, mixed_ref, ogain_ref, wo, out_ref)
    for i, again in sent:
        view = again()
        pltpu.make_async_copy(view, view, ssem.at[i]).wait()
    assert len(names) <= SLOTS


def per_device(
    tokens, in_gain, w_query_down, w_latent_down, w_rope_key, query_latent_gain, latent_gain,
    w_query_up, w_key_up, w_value_up, query_gain, key_gain, out_gain, w_out,
):
    blocks = lax.axis_size("sp")
    tables = [jnp.asarray(t) for t in rope_tables(blocks)]
    vm = pl.BlockSpec(memory_space=pltpu.VMEM)
    hbm = pl.BlockSpec(memory_space=pl.ANY)
    args = (
        tokens.reshape(ROWS, D), in_gain.reshape(1, D), w_query_down, w_latent_down, w_rope_key.T,
        query_latent_gain.reshape(1, QR), latent_gain.reshape(1, KR), w_query_up, w_key_up,
        w_value_up, query_gain.reshape(1, QK), key_gain.reshape(1, QK), out_gain.reshape(1, D), w_out, *tables,
    )
    out = pl.pallas_call(
        kernel,
        out_shape=pltpu.VMEM((ROWS, D), BF),
        in_specs=[hbm if i in (0, 2, 3, 4, 7, 8, 9) or i > 12 else vm for i in range(len(args))],
        out_specs=vm,
        scratch_shapes=[
            pltpu.VMEM((8, 256, QR + KR), BF),
            pltpu.VMEM((2, LOCAL, 4, 160, 128), BF),
            pltpu.VMEM((4, 4, 4, 2, 16, D), BF),
            pltpu.VMEM((4, 4, 320, 256), BF),
            pltpu.VMEM((2, ROWS, QR), BF),
            pltpu.VMEM((8, ROWS, 256), BF),
            pltpu.VMEM((ROWS, QR + KR), F32),
            pltpu.VMEM((LOCAL, QR, 256), BF),
            pltpu.VMEM((LOCAL, NOPE, KR), BF),
            pltpu.VMEM((LOCAL // 2, KR, 2 * VD), BF),
            pltpu.VMEM((2, LOCAL, ROWS, 256), BF),
            pltpu.VMEM((KEPT, LOCAL, 256, 256), BF),
            pltpu.VMEM((KEPT, LOCAL, 256, 256), BF),
            pltpu.VMEM((2, LOCAL, ROWS, 128), F32),
            pltpu.VMEM((2, LOCAL, ROWS, 256), F32),
            pltpu.VMEM((HEADS + LOCAL, ROWS, VD), BF),
            pltpu.VMEM((ROWS, D), BF),
            pltpu.VMEM((1, 256), F32),
            pltpu.VMEM((NOPE, 256), F32),
            pltpu.VMEM((ROPE, 256), F32),
            pltpu.VMEM((ROWS, D), BF),
            pltpu.VMEM((ROPE, D), BF),
            pltpu.VMEM((64, QK), BF),
        ]
        + [pltpu.VMEM(t.shape, F32) for t in tables]
        + [
            pltpu.SemaphoreType.DMA((12,)),
            pltpu.SemaphoreType.DMA((SLOTS,)),
            pltpu.SemaphoreType.DMA((SLOTS,)),
        ],
        compiler_params=pltpu.CompilerParams(
            vmem_limit_bytes=60 * 1024 * 1024, collective_id=0, has_side_effects=True
        ),
    )(*args)
    return out.reshape(1, ROWS, D)


def solution(mesh):
    in_specs = (
        P("dp", "sp", None), P(), P("dp", None), P("dp", None), P(), P(), P(),
        P("dp", "sp"), P("dp", "sp"), P("dp", "sp"), P(), P(), P(), P(("sp", "dp"), None),
    )
    return jax.shard_map(
        per_device, mesh=mesh, in_specs=in_specs, out_specs=P("dp", "sp", None), check_vma=False
    )
```

```python
import functools

import jax
import jax.numpy as jnp
import numpy as np
from jax import lax
from jax.experimental import pallas as pl
from jax.experimental.pallas import tpu as pltpu
from jax.sharding import PartitionSpec as P

HEADS, NOPE, ROPE, VD, QR, KR, QK = 16, 128, 64, 128, 512, 256, 192
D = 2048
ROWS = 256
EPS = 1e-06
THETA = 10000.0
NEG_BIG = -1e30
BF, F32 = jnp.bfloat16, jnp.float32
SOFT = float(QK**-0.5 * np.log2(np.e))
LOCAL = 8


def rope_tables(blocks):
    half = ROPE // 2
    freq = THETA ** (-np.arange(half) / half)
    low = np.arange(ROWS)[:, None] * freq[None, :]
    high = (np.arange(blocks) * ROWS)[:, None] * freq[None, :]
    pad = np.zeros((ROWS, 128 - ROPE))
    lowq = np.stack([np.concatenate([f(low), f(low), pad], 1) for f in (np.cos, np.sin)])
    hpad = np.zeros((blocks, 128 - ROPE))
    highq = np.stack([np.concatenate([f(high), f(high), hpad], 1) for f in (np.cos, np.sin)], 1)
    highq = np.broadcast_to(highq[:, :, None, :], (blocks, 2, 8, 128))
    lowk = np.concatenate([np.cos(low).T, np.sin(low).T], 0)
    highk = np.concatenate([np.cos(high), np.sin(high)], 1)
    highk = np.broadcast_to(highk[:, :, None], (blocks, ROPE, 128))
    return [np.ascontiguousarray(t, dtype=np.float32) for t in (lowq, highq, lowk, highk)]


def dot(a, b):
    return lax.dot_general(a, b, (((1,), (0,)), ((), ())), preferred_element_type=F32)


def dot_nt(a, b):
    return lax.dot_general(a, b, (((1,), (1,)), ((), ())), preferred_element_type=F32)


def prepare_head(us, h, wq_ref, wkt_ref, wv_ref):
    keys = []
    for x in range(4):
        for c in range(2):
            d = 2 * x + c
            unit = us[c, h, x]
            rows = slice(d * 64, d * 64 + 64)
            wq_ref[h, rows, 0:NOPE] = unit[0:64]
            wq_ref[h, d * 64 : d * 64 + 32, NOPE:QK] = unit[64:96, 0:ROPE]
            wq_ref[h, d * 64 + 32 : d * 64 + 64, NOPE:QK] = unit[64:96, ROPE:128]
            keys.append(unit[96:128])
            wv_ref[h // 2, d * 32 : d * 32 + 32, pl.ds(pl.multiple_of(h % 2 * VD, VD), VD)] = unit[128:160]
    wkt_ref[h] = jnp.concatenate(keys, axis=0).T


def make_queries(latq, block, wq_ref, qgain, lowq_ref, highq_ref, q_ref, which):
    ch, sh = highq_ref[block, 0, 0:1], highq_ref[block, 1, 0:1]
    cl, sl = lowq_ref[0], lowq_ref[1]
    cosine = ch * cl - sh * sl
    sine = sh * cl + ch * sl
    lane = lax.broadcasted_iota(jnp.int32, (ROWS, 128), 1)
    sine_a = jnp.where(lane < ROPE // 2, -sine, 0.0)
    sine_b = jnp.where(lane < ROPE // 2, 0.0, sine)

    for h in range(LOCAL):
        q = dot(latq, wq_ref[h])
        scale = lax.rsqrt(jnp.sum(q * q, axis=1, keepdims=True) * (1.0 / QK) + EPS)
        n = q * scale * qgain
        t = n[:, NOPE:256]
        turned = (
            t * cosine
            + pltpu.roll(t, 128 - ROPE // 2, 1) * sine_a
            + pltpu.roll(t, ROPE // 2, 1) * sine_b
        )
        q_ref[which, h, :, 0:NOPE] = n[:, 0:NOPE].astype(BF)
        q_ref[which, h, :, NOPE:256] = turned.astype(BF)


def expand(unit, block, wkt_ref, wv_ref, gk_ref, gr_ref, lowk_ref, highk_ref, place):
    kv = unit[0:256, :]
    rope = unit[256:320, :].astype(F32)
    half = ROPE // 2
    ch = jnp.concatenate([highk_ref[block, 0:half]] * 2, axis=1)
    sh = jnp.concatenate([highk_ref[block, half:ROPE]] * 2, axis=1)
    cl, sl = lowk_ref[0:half], lowk_ref[half:ROPE]
    cosine = ch * cl - sh * sl
    sine = sh * cl + ch * sl
    rope_sq = jnp.sum(rope * rope, axis=0, keepdims=True)
    x = rope * gr_ref[...]
    a, b = x[0:half], x[half:ROPE]
    turned = jnp.concatenate([a * cosine - b * sine, b * cosine + a * sine], axis=0)
    keys = dot_nt(wkt_ref[...].reshape(LOCAL * NOPE, KR), kv)
    for h in range(LOCAL):
        k = keys[h * NOPE : (h + 1) * NOPE]
        scale = lax.rsqrt((jnp.sum(k * k, axis=0, keepdims=True) + rope_sq) * (1.0 / QK) + EPS)
        kt, _ = place(h)
        kt[0:NOPE] = (k * scale * gk_ref[...]).astype(BF)
        kt[NOPE:QK] = (turned * scale).astype(BF)
    for h in range(0, LOCAL, 2):
        v = dot(kv, wv_ref[h // 2]).astype(BF)
        place(h)[1][:, 0:VD] = v[:, 0:VD]
        place(h + 1)[1][:, 0:VD] = v[:, VD : 2 * VD]


def attend(diagonal, q_ref, place, m_ref, acc_ref, which):
    for h in range(LOCAL):
        kt, v = place(h)
        s = dot(q_ref[which, h], kt[...])
        if diagonal:
            row = lax.broadcasted_iota(jnp.int32, (ROWS, ROWS), 0)
            col = lax.broadcasted_iota(jnp.int32, (ROWS, ROWS), 1)
            s = jnp.where(col <= row, s, NEG_BIG)
        old = m_ref[which, h]
        new = jnp.maximum(old, jnp.max(s, axis=1, keepdims=True))
        fade = jnp.exp2((old - new) * SOFT)
        p = jnp.exp2((s - jnp.concatenate([new, new], 1)) * SOFT).astype(BF)
        m_ref[which, h] = new
        acc_ref[which, h] = acc_ref[which, h] * jnp.concatenate([fade, fade], 1) + dot(
            p, v[...]
        )


def attend_pair(q_ref, place0, place1, m_ref, acc_ref, which, heads):
    def score(h):
        q = q_ref[which, h]
        return dot(q, place0(h)[0][...]), dot(q, place1(h)[0][...])

    s0, s1 = score(heads[0])
    for h in heads:
        ahead = score(h + 1) if h + 1 in heads else None
        old = m_ref[which, h]
        new = jnp.maximum(old, jnp.max(jnp.maximum(s0, s1), axis=1, keepdims=True))
        fade = jnp.exp2((old - new) * SOFT)
        wide = jnp.concatenate([new, new], 1)
        p0 = jnp.exp2((s0 - wide) * SOFT).astype(BF)
        p1 = jnp.exp2((s1 - wide) * SOFT).astype(BF)
        m_ref[which, h] = new
        acc_ref[which, h] = acc_ref[which, h] * jnp.concatenate([fade, fade], 1) + (
            dot(p0, place0(h)[1][...]) + dot(p1, place1(h)[1][...])
        )
        if ahead is not None:
            s0, s1 = ahead


def close_heads(acc_ref, which, att_ref, first, heads=range(LOCAL)):
    for h in heads:
        att_ref[first + h] = (
            acc_ref[which, h, :, 0:VD] / acc_ref[which, h, :, VD : 2 * VD]
        ).astype(BF)


def finish(att_ref, mixed_ref, ogain_ref, wo_ref, out_ref):
    total = jnp.zeros((ROWS, VD), F32)
    for h in range(HEADS):
        at = att_ref[h].astype(F32)
        total = total + at * at
    scale = lax.rsqrt(jnp.sum(total, axis=1, keepdims=True) * (1.0 / (HEADS * VD)) + EPS)
    for h in range(HEADS):
        cols = slice(h * VD, (h + 1) * VD)
        mixed_ref[:, cols] = (att_ref[h].astype(F32) * scale * ogain_ref[:, cols]).astype(BF)

    def one(j, _):
        cols = pl.ds(pl.multiple_of(j * 512, 512), 512)
        w = wo_ref[:, :, :, :, :, cols].reshape(HEADS * VD, 512)
        out_ref[:, cols] = dot(mixed_ref[...], w).astype(BF)
        return 0

    lax.fori_loop(0, D // 512, one, 0)


def rms_rows(values, scaling):
    return values * lax.rsqrt(jnp.mean(values * values, axis=-1, keepdims=True) + EPS) * scaling


SLOTS = 128
SPLIT = 4


def kernel(
    tok_in, ing_ref, wqd_in, wld_in, wrt_in, qlg_ref, klg_ref, wqu_in, wku_in, wvu_in,
    qg_ref, kg_ref, ogain_ref, wo_in, lowq_in, highq_in, lowk_in, highk_in,
    out_ref,
    wd, us, wo, kvb, lq, normed, sums, wq_ref, wkt_ref, wv_ref, q_ref, kt_ref, v_ref, kt_keep, v_keep,
    m_ref, acc_ref, att_ref, mixed_ref, qgain_ref, gk_ref, gr_ref,
    tok_ref, wrt_ref, wqu_ref, lowq_ref, highq_ref, lowk_ref, highk_ref, lsem, ssem, rsem,
):
    sp, dp = lax.axis_index("sp"), lax.axis_index("dp")
    z, y = sp // 4, sp % 4
    x, c = dp // 2, dp % 2
    xl, xr, xo = (x + 3) % 4, (x + 1) % 4, (x + 2) % 4
    yl, yr, yo = (y + 3) % 4, (y + 1) % 4, (y + 2) % 4
    zl, zr, zo = (z + 3) % 4, (z + 1) % 4, (z + 2) % 4
    co = 1 - c
    zb = z % 2
    zpair = z + 1 - 2 * zb
    zmate = 3 - z

    def dev(xx=x, yy=y, zz=z, cc=c):
        return {"sp": zz * 4 + yy, "dp": xx * 2 + cc}

    X_R, X_L, Y_R, Y_L, Z_R, Z_L, CORE = (
        dev(xx=xr), dev(xx=xl), dev(yy=yr), dev(yy=yl), dev(zz=zr), dev(zz=zl), dev(cc=co)
    )
    zn, zm = zpair, (z + 3 + 2 * zb) % 4
    Z_N, Z_M = dev(zz=zn), dev(zz=zm)
    names, sent = {}, []

    def number(name):
        return names.setdefault(name, len(names))

    def push(name, view, to, dst=None):
        i = number(name)
        again = view if callable(view) else functools.partial(lambda v: v, view)
        view = again()
        pltpu.make_async_remote_copy(
            src_ref=view, dst_ref=view if dst is None else dst, send_sem=ssem.at[i],
            recv_sem=rsem.at[i], device_id=to, device_id_type=pl.DeviceIdType.MESH,
        ).start()
        sent.append((i, again))

    def got(name, view):
        pltpu.make_async_copy(view, view, rsem.at[number(name)]).wait()

    barrier = pltpu.get_barrier_semaphore()
    X_O, Y_O = dev(xx=xo), dev(yy=yo)
    for to in (X_R, X_L, X_O, Y_R, Y_L, Y_O, Z_R, Z_L, CORE):
        pl.semaphore_signal(barrier, 1, device_id=to, device_id_type=pl.DeviceIdType.MESH)

    hl = zb * 4 + y
    loads = [
        pltpu.make_async_copy(src, dst, lsem.at[i])
        for i, (src, dst) in enumerate((
            (wqu_in, wqu_ref), (wku_in, us.at[c, hl, x, 96:128]),
            (wvu_in, us.at[c, hl, x, 128:160]), (wo_in, wo.at[z, y, x, c]),
            (wqd_in, wd.at[dp, :, 0:QR]), (wld_in, wd.at[dp, :, QR : QR + KR]),
            (tok_in, tok_ref), (wrt_in, wrt_ref), (lowq_in, lowq_ref), (highq_in, highq_ref),
            (lowk_in, lowk_ref), (highk_in, highk_ref),
        ))
    ]
    for load in loads:
        load.start()
    loads[0].wait()
    us[c, hl, x, 0:64] = wqu_ref[:, 0:NOPE]
    us[c, hl, x, 64:96] = jnp.concatenate(
        [wqu_ref[0:32, NOPE:QK], wqu_ref[32:64, NOPE:QK]], axis=1
    )
    for load in loads[1:4]:
        load.wait()
    pl.semaphore_wait(barrier, 9)

    uown = us.at[c, hl, x]
    push("u_r", uown, X_R)
    push("u_l", uown, X_L)
    push("u_o", uown, X_O)
    wown = wo.at[z, y, x, c]
    push("w_yr", wown, Y_R)
    push("w_yl", wown, Y_L)
    push("w_yo", wown, Y_O)
    loads[4].wait()
    loads[5].wait()
    down = wd.at[dp]
    push("d_ra", wd.at[dp, 0:128], X_R)
    push("d_la", wd.at[dp, 128:256], X_L)
    push("d_rb", wd.at[dp, 128:256], X_R)
    push("d_lb", wd.at[dp, 0:128], X_L)
    push("d_c", down, CORE)

    for load in loads[6:]:
        load.wait()
    for r in range(0, ROWS, 64):
        rows = slice(r, r + 64)
        n = rms_rows(tok_ref[rows].astype(F32), ing_ref[...]).astype(BF)
        for k in range(8):
            normed[k, rows] = n[:, k * 256 : (k + 1) * 256]

    qgain_ref[:, 0:NOPE] = qg_ref[:, 0:NOPE]
    qgain_ref[:, NOPE:256] = jnp.concatenate(
        [qg_ref[:, NOPE:QK], jnp.zeros((1, 256 - QK), F32)], axis=1
    )
    kg = jnp.concatenate([kg_ref[...], jnp.zeros((1, 256 - QK), F32)], axis=1)
    column = jnp.broadcast_to(kg[:, 0:NOPE], (NOPE, NOPE)).T
    gk_ref[...] = jnp.concatenate([column, column], axis=1)
    column = jnp.broadcast_to(kg[:, NOPE:256], (NOPE, NOPE)).T[0:ROPE]
    gr_ref[...] = jnp.concatenate([column, column], axis=1)

    got("u_r", us.at[c, hl, xl])
    got("u_l", us.at[c, hl, xr])
    got("u_o", us.at[c, hl, xo])
    block0 = us.at[c, hl]
    push("u_z", block0, dev(zz=zpair))
    push("u_y0r", block0, Y_R)
    push("u_y0l", block0, Y_L)
    push("u_c0", block0, CORE)
    got("w_yr", wo.at[z, yl, x, c])
    got("w_yl", wo.at[z, yr, x, c])
    got("w_yo", wo.at[z, yo, x, c])
    push("w_zr", wo.at[z, :, x, c], Z_R)
    push("w_zl", wo.at[z, :, x, c], Z_L)

    def add(d, first=False):
        part = dot(normed[d], wd[d])
        if first:
            sums[...] = part
        else:
            sums[...] += part

    add(dp, True)
    got("d_c", wd.at[2 * x + co])
    add(2 * x + co)
    m_ref[...] = jnp.full(m_ref.shape, NEG_BIG, F32)
    acc_ref[...] = jnp.zeros(acc_ref.shape, F32)
    wq_ref[:, :, QK:256] = jnp.zeros((LOCAL, QR, 256 - QK), BF)
    kt_ref[:, :, QK:256, :] = jnp.zeros((2, SPLIT, 256 - QK, 256), BF)
    v_ref[:, :, :, VD:256] = jnp.ones((2, SPLIT, ROWS, 256 - VD), BF)

    def blank(i, _):
        kt_keep[i, :, QK:256, :] = jnp.zeros((LOCAL - SPLIT, 256 - QK, 256), BF)
        v_keep[i, :, :, VD:256] = jnp.ones((LOCAL - SPLIT, ROWS, 256 - VD), BF)
        return 0

    lax.fori_loop(0, 16, blank, 0)
    rope_t = jnp.zeros((ROPE, ROWS), F32)
    for k in range(8):
        rope_t = rope_t + dot_nt(wrt_ref[:, k * 256 : (k + 1) * 256], normed[k])
    kvb[y, z, 256:320] = rope_t.astype(BF)
    base0, base1 = zb * 4, 4 - zb * 4
    block1 = us.at[c, base1 + y]

    def ring_y(j, base):
        got(f"u_y{j}r", us.at[c, base + yl])
        push(f"u_y{j}or", us.at[c, base + yl, 0:2], Y_R)
        push(f"u_c{j}l", us.at[c, base + yl], CORE)
        got(f"u_y{j}l", us.at[c, base + yr])
        push(f"u_y{j}ol", us.at[c, base + yr, 2:4], Y_L)
        push(f"u_c{j}r", us.at[c, base + yr], CORE)

    got("d_ra", wd.at[2 * xl + c, 0:128])
    push("d_or", wd.at[2 * xl + c, 0:128], X_R)
    got("d_la", wd.at[2 * xr + c, 128:256])
    push("d_ol", wd.at[2 * xr + c, 128:256], X_L)
    got("u_z", us.at[c, base1 + y])
    push("u_y1r", block1, Y_R)
    push("u_y1l", block1, Y_L)
    push("u_c1", block1, CORE)
    ring_y(0, base0)
    got("d_rb", wd.at[2 * xl + c, 128:256])
    push("d_cl", wd.at[2 * xl + c], CORE)
    got("d_lb", wd.at[2 * xr + c, 0:128])
    push("d_cr", wd.at[2 * xr + c], CORE)
    add(2 * xl + c)
    add(2 * xr + c)
    got("d_cl", wd.at[2 * xl + co])
    add(2 * xl + co)
    got("d_cr", wd.at[2 * xr + co])
    add(2 * xr + co)
    zrow = (z, zl, zr, zo)

    def row(k):
        push(f"w_xr{k}", wo.at[zrow[k], :, x, c], X_R)
        push(f"w_xl{k}", wo.at[zrow[k], :, x, c], X_L)

    row(0)
    got("w_zr", wo.at[zl, :, x, c])
    push("w_ozr", wo.at[zl, 0:2, x, c], Z_R)
    got("w_zl", wo.at[zr, :, x, c])
    push("w_ozl", wo.at[zr, 2:4, x, c], Z_L)
    row(1)
    row(2)
    got("u_c0", us.at[co, base0 + y])
    got("u_c1", us.at[co, base1 + y])
    got("u_c0l", us.at[co, base0 + yl])
    got("u_c0r", us.at[co, base0 + yr])
    for h in (base0 + y, base1 + y, base0 + yl, base0 + yr):
        prepare_head(us, h, wq_ref, wkt_ref, wv_ref)
    ring_y(1, base1)
    got("d_or", wd.at[2 * xo + c, 0:128])
    push("d_coa", wd.at[2 * xo + c, 0:128], CORE)
    got("d_ol", wd.at[2 * xo + c, 128:256])
    push("d_cob", wd.at[2 * xo + c, 128:256], CORE)
    add(2 * xo + c)
    got("d_coa", wd.at[2 * xo + co, 0:128])
    got("d_cob", wd.at[2 * xo + co, 128:256])
    add(2 * xo + co)

    lq[0] = rms_rows(sums[:, 0:QR], qlg_ref[...]).astype(BF)
    push("q", lq.at[0], dev(zz=zmate), lq.at[1])
    kvb[y, z, 0:256] = rms_rows(sums[:, QR : QR + KR], klg_ref[...]).astype(BF)
    own = kvb.at[y, z]
    push("k_yr", own, Y_R)
    push("k_yl", own, Y_L)
    push("k_zn", own, Z_N)
    push("k_zm", own, Z_M)

    for j, base in ((0, base0), (1, base1)):
        got(f"u_y{j}or", us.at[c, base + yo, 0:2])
        got(f"u_y{j}ol", us.at[c, base + yo, 2:4])
        push(f"u_c{j}o", us.at[c, base + yo], CORE)
    got("w_ozr", wo.at[zo, 0:2, x, c])
    got("w_ozl", wo.at[zo, 2:4, x, c])
    row(3)
    got("u_c1l", us.at[co, base1 + yl])
    got("u_c1r", us.at[co, base1 + yr])
    got("u_c0o", us.at[co, base0 + yo])
    got("u_c1o", us.at[co, base1 + yo])
    push("w_c", wo.at[:, :, x, c], CORE)
    for h in (base0 + yo, base1 + yl, base1 + yr, base1 + yo):
        prepare_head(us, h, wq_ref, wkt_ref, wv_ref)
    make_queries(lq[0], sp, wq_ref, qgain_ref[...], lowq_ref, highq_ref, q_ref, 0)
    def k_y():
        got("k_yr", kvb.at[yl, z])
        push("k_oyr", lambda: kvb.at[yl, z, 0:160], Y_R)
        got("k_yl", kvb.at[yr, z])
        push("k_oyl", lambda: kvb.at[yr, z, 160:320], Y_L)

    def k_zn():
        got("k_zn", kvb.at[y, zn])
        push("k_ozm", lambda: kvb.at[y, zn, 0:160], Z_M)
        push("k_ynr", lambda: kvb.at[y, zn], Y_R)
        push("k_ynl", lambda: kvb.at[y, zn], Y_L)

    def k_zm():
        got("k_zm", kvb.at[y, zm])
        push("k_ozn", lambda: kvb.at[y, zm, 160:320], Z_N)
        push("k_ymr", lambda: kvb.at[y, zm], Y_R)
        push("k_yml", lambda: kvb.at[y, zm], Y_L)

    def k_oy():
        got("k_oyr", kvb.at[yo, z, 0:160])
        got("k_oyl", kvb.at[yo, z, 160:320])
        push("k_pzn", lambda: kvb.at[yo, z], Z_N)
        push("k_pzm", lambda: kvb.at[yo, z], Z_M)

    def k_oz():
        got("k_ozm", kvb.at[y, zo, 0:160])
        got("k_ozn", kvb.at[y, zo, 160:320])
        push("k_yor", lambda: kvb.at[y, zo], Y_R)
        push("k_yol", lambda: kvb.at[y, zo], Y_L)

    def k_pz():
        got("k_pzn", kvb.at[yo, zn])
        push("k_pozm", lambda: kvb.at[yo, zn, 0:160], Z_M)
        got("k_pzm", kvb.at[yo, zm])
        push("k_pozn", lambda: kvb.at[yo, zm, 160:320], Z_N)

    def k_yn():
        got("k_ynr", kvb.at[yl, zn])
        got("k_ynl", kvb.at[yr, zn])

    def k_ym():
        got("k_ymr", kvb.at[yl, zm])
        got("k_yml", kvb.at[yr, zm])

    def k_yo():
        got("k_yor", kvb.at[yl, zo])
        got("k_yol", kvb.at[yr, zo])

    def k_poz():
        got("k_pozm", kvb.at[yo, zo, 0:160])
        got("k_pozn", kvb.at[yo, zo, 160:320])

    def queries_mate():
        got("q", lq.at[1])
        make_queries(
            lq[1], zmate * 4 + y, wq_ref, qgain_ref[...], lowq_ref, highq_ref, q_ref, 1
        )

    def wx(k):
        def go():
            r = zrow[k]
            got(f"w_xr{k}", wo.at[r, :, xl, c])
            push(f"w_oxr{k}", lambda: wo.at[r, 0:2, xl, c], X_R)
            push(f"w_cl{k}", lambda: wo.at[r, :, xl, c], CORE)
            got(f"w_xl{k}", wo.at[r, :, xr, c])
            push(f"w_oxl{k}", lambda: wo.at[r, 2:4, xr, c], X_L)
            push(f"w_cr{k}", lambda: wo.at[r, :, xr, c], CORE)

        return go

    def wxo(k):
        r = zrow[k]
        got(f"w_oxr{k}", wo.at[r, 0:2, xo, c])
        got(f"w_oxl{k}", wo.at[r, 2:4, xo, c])
        push(f"w_co{k}", wo.at[r, :, xo, c], CORE)

    hfirst = (z // 2) * LOCAL
    b_own, b_mate = sp, zmate * 4 + y

    low, high = range(SPLIT), range(SPLIT, LOCAL)

    def send_mate(heads):
        close_heads(acc_ref, 1, att_ref, HEADS, heads)
        push(
            f"att{heads[0]}", lambda: att_ref.at[HEADS + heads[0] : HEADS + heads[-1] + 1],
            dev(zz=zmate), att_ref.at[pl.ds(hfirst + heads[0], SPLIT)],
        )

    def place(slot, step):
        def of(h):
            if h < SPLIT:
                return kt_ref.at[slot, h], v_ref.at[slot, h]
            return kt_keep.at[step, h - SPLIT], v_keep.at[step, h - SPLIT]

        return of

    def pick(test, yes, no):
        return no + test.astype(jnp.int32) * (yes - no)

    def source(step):
        dy = pick(step < 3, step, pick(step < 5, 0, pick(step < 7, step - 4, pick(
            step == 7, 0, pick(step == 8, 3, pick(step < 11, step - 8, pick(
                step < 13, 3, pick(step < 15, step - 12, 3))))))))
        dz = pick(step < 3, 0, pick(step < 5, step - 2, pick(step < 7, 1, pick(
            step == 7, 3, pick(step == 8, 0, pick(step < 11, 2, pick(
                step < 13, step - 10, 3)))))))
        yy = pick(dy == 0, y, pick(dy == 1, yl, pick(dy == 2, yr, yo)))
        zz = pick(dz == 0, z, pick(dz == 1, zn, pick(dz == 2, zm, zo)))
        return yy, zz, zz * 4 + yy

    b_last = jnp.maximum(b_own, b_mate)

    def expand_step(step, slot):
        yy, zz, b = source(step)
        expand(
            kvb[yy, zz], b, wkt_ref, wv_ref, gk_ref, gr_ref, lowk_ref, highk_ref,
            place(slot, step),
        )

    def attend_to(which, slot, step, diagonal=False):
        attend(diagonal, q_ref, place(slot, step), m_ref, acc_ref, which)

    def attend_both(which, first, second, heads):
        attend_pair(
            q_ref, place(0, first), place(1, second), m_ref, acc_ref, which, heads
        )

    def singles(first, second, b0, b1, own0, own1, skip_own, skip_mate):
        def single(j, _):
            which, slot = j // 2, j % 2
            step = pick(slot == 0, first, second)
            b = pick(slot == 0, b0, b1)
            mine = pick(slot == 0, own0.astype(jnp.int32), own1.astype(jnp.int32)) * (1 - skip_own)
            mates = (b < b_mate).astype(jnp.int32) * (1 - skip_mate)

            @pl.when(pick(which == 0, mine, mates) == 1)
            def _():
                attend_to(which, slot, step)

            @pl.when((b == b_mate) & (which == 1))
            def _():
                attend_to(which, slot, step, True)

            return 0

        lax.fori_loop(0, 4, single, 0)

    zero = z - z
    expand_step(zero, 0)
    attend_to(0, 0, zero, True)
    k_y()
    k_zn()
    expand_step(zero + 1, 0)
    expand_step(zero + 2, 1)
    queries_mate()
    mate_both = (source(zero + 1)[2] < b_mate) & (source(zero + 2)[2] < b_mate)

    @pl.when(mate_both)
    def _():
        attend_both(1, zero + 1, zero + 2, low)

    def units(i):
        first = pick(i == 7, 0, 2 * i + 1)
        second = pick(i == 7, 15, 2 * i + 2)
        return first, second, source(first)[2], source(second)[2]

    at_pair = {1: (k_zm, k_oy, wx(0)), 2: (k_yn,), 3: (k_oz, k_pz, wx(1)), 4: (k_ym, wx(2)),
               5: (wx(3),), 6: (k_yo,), 7: (k_poz,)}

    def pair(i, _):
        for when, todo in at_pair.items():
            @pl.when(i == when)
            def _(todo=todo):
                for f in todo:
                    f()

        first, second, b0, b1 = units(i)
        own0 = (b0 < b_own) & (i > 0) & (first > 0)
        own1 = (b1 < b_own) & (i > 0) & (second != 8)
        own_both = own0 & own1
        mate_both = (b0 < b_mate) & (b1 < b_mate)
        needed = ((b0 <= b_last) | (b1 <= b_last)) & (i > 0)
        mate_first = mate_both & jnp.logical_not(own_both)

        @pl.when(own_both)
        def _():
            expand_step(first, 0)
            expand_step(second, 1)
            attend_both(0, first, second, range(LOCAL))

        @pl.when(mate_first & (i > 0))
        def _():
            expand_step(first, 0)
            expand_step(second, 1)
            attend_both(1, first, second, low)

        @pl.when(jnp.logical_not(own_both | mate_both) & needed)
        def _():
            expand_step(first, 0)
            expand_step(second, 1)

        @pl.when(own_both & mate_both)
        def _():
            attend_both(1, first, second, low)

        @pl.when(jnp.logical_not(own_both & mate_both))
        def _():
            singles(
                first, second, b0, b1, own0, own1, own_both.astype(jnp.int32), mate_both.astype(jnp.int32),
            )

        return 0

    lax.fori_loop(0, 8, pair, 0)
    send_mate(low)

    def rest(i, _):
        first, second, b0, b1 = units(i)

        @pl.when((b0 < b_mate) & (b1 < b_mate))
        def _():
            attend_both(1, first, second, high)

        return 0

    lax.fori_loop(0, 8, rest, 0)
    send_mate(high)

    def last(j, _):
        step = pick(j == 2, 8, j + 1)

        @pl.when(source(step)[2] < b_own)
        def _():
            expand_step(step, 0)
            attend_to(0, 0, step)

        return 0

    lax.fori_loop(0, 3, last, 0)
    close_heads(acc_ref, 0, att_ref, hfirst)
    for k in range(4):
        wxo(k)
    got("w_c", wo.at[:, :, x, co])
    for k in range(4):
        got(f"w_cl{k}", wo.at[zrow[k], :, xl, co])
        got(f"w_cr{k}", wo.at[zrow[k], :, xr, co])
        got(f"w_co{k}", wo.at[zrow[k], :, xo, co])
    for heads in (low, high):
        got(f"att{heads[0]}", att_ref.at[pl.ds(LOCAL - hfirst + heads[0], SPLIT)])
    finish(att_ref, mixed_ref, ogain_ref, wo, out_ref)
    for i, again in sent:
        view = again()
        pltpu.make_async_copy(view, view, ssem.at[i]).wait()
    assert len(names) <= SLOTS


def per_device(
    tokens, in_gain, w_query_down, w_latent_down, w_rope_key, query_latent_gain, latent_gain,
    w_query_up, w_key_up, w_value_up, query_gain, key_gain, out_gain, w_out,
):
    blocks = lax.axis_size("sp")
    tables = [jnp.asarray(t) for t in rope_tables(blocks)]
    vm = pl.BlockSpec(memory_space=pltpu.VMEM)
    hbm = pl.BlockSpec(memory_space=pl.ANY)
    args = (
        tokens.reshape(ROWS, D), in_gain.reshape(1, D), w_query_down, w_latent_down, w_rope_key.T,
        query_latent_gain.reshape(1, QR), latent_gain.reshape(1, KR), w_query_up, w_key_up,
        w_value_up, query_gain.reshape(1, QK), key_gain.reshape(1, QK), out_gain.reshape(1, D), w_out, *tables,
    )
    out = pl.pallas_call(
        kernel,
        out_shape=pltpu.VMEM((ROWS, D), BF),
        in_specs=[hbm if i in (0, 2, 3, 4, 7, 8, 9) or i > 12 else vm for i in range(len(args))],
        out_specs=vm,
        scratch_shapes=[
            pltpu.VMEM((8, 256, QR + KR), BF),
            pltpu.VMEM((2, LOCAL, 4, 160, 128), BF),
            pltpu.VMEM((4, 4, 4, 2, 16, D), BF),
            pltpu.VMEM((4, 4, 320, 256), BF),
            pltpu.VMEM((2, ROWS, QR), BF),
            pltpu.VMEM((8, ROWS, 256), BF),
            pltpu.VMEM((ROWS, QR + KR), F32),
            pltpu.VMEM((LOCAL, QR, 256), BF),
            pltpu.VMEM((LOCAL, NOPE, KR), BF),
            pltpu.VMEM((LOCAL // 2, KR, 2 * VD), BF),
            pltpu.VMEM((2, LOCAL, ROWS, 256), BF),
            pltpu.VMEM((2, SPLIT, 256, 256), BF),
            pltpu.VMEM((2, SPLIT, 256, 256), BF),
            pltpu.VMEM((16, LOCAL - SPLIT, 256, 256), BF),
            pltpu.VMEM((16, LOCAL - SPLIT, 256, 256), BF),
            pltpu.VMEM((2, LOCAL, ROWS, 128), F32),
            pltpu.VMEM((2, LOCAL, ROWS, 256), F32),
            pltpu.VMEM((HEADS + LOCAL, ROWS, VD), BF),
            pltpu.VMEM((ROWS, D), BF),
            pltpu.VMEM((1, 256), F32),
            pltpu.VMEM((NOPE, 256), F32),
            pltpu.VMEM((ROPE, 256), F32),
            pltpu.VMEM((ROWS, D), BF),
            pltpu.VMEM((ROPE, D), BF),
            pltpu.VMEM((64, QK), BF),
        ]
        + [pltpu.VMEM(t.shape, F32) for t in tables]
        + [
            pltpu.SemaphoreType.DMA((12,)),
            pltpu.SemaphoreType.DMA((SLOTS,)),
            pltpu.SemaphoreType.DMA((SLOTS,)),
        ],
        compiler_params=pltpu.CompilerParams(
            vmem_limit_bytes=60 * 1024 * 1024, collective_id=0, has_side_effects=True
        ),
    )(*args)
    return out.reshape(1, ROWS, D)


def solution(mesh):
    in_specs = (
        P("dp", "sp", None), P(), P("dp", None), P("dp", None), P(), P(), P(),
        P("dp", "sp"), P("dp", "sp"), P("dp", "sp"), P(), P(), P(), P(("sp", "dp"), None),
    )
    return jax.shard_map(
        per_device, mesh=mesh, in_specs=in_specs, out_specs=P("dp", "sp", None), check_vma=False
    )
```

```python
import functools

import jax
import jax.numpy as jnp
import numpy as np
from jax import lax
from jax.experimental import pallas as pl
from jax.experimental.pallas import tpu as pltpu
from jax.sharding import PartitionSpec as P

HEADS, NOPE, ROPE, VD, QR, KR, QK = 16, 128, 64, 128, 512, 256, 192
D = 2048
ROWS = 256
EPS = 1e-06
THETA = 10000.0
NEG_BIG = -1e30
BF, F32 = jnp.bfloat16, jnp.float32
SOFT = float(QK**-0.5 * np.log2(np.e))
LOCAL = 8


def rope_tables(blocks):
    half = ROPE // 2
    freq = THETA ** (-np.arange(half) / half)
    low = np.arange(ROWS)[:, None] * freq[None, :]
    high = (np.arange(blocks) * ROWS)[:, None] * freq[None, :]
    pad = np.zeros((ROWS, 128 - ROPE))
    lowq = np.stack([np.concatenate([f(low), f(low), pad], 1) for f in (np.cos, np.sin)])
    hpad = np.zeros((blocks, 128 - ROPE))
    highq = np.stack([np.concatenate([f(high), f(high), hpad], 1) for f in (np.cos, np.sin)], 1)
    highq = np.broadcast_to(highq[:, :, None, :], (blocks, 2, 8, 128))
    lowk = np.concatenate([np.cos(low).T, np.sin(low).T], 0)
    highk = np.concatenate([np.cos(high), np.sin(high)], 1)
    highk = np.broadcast_to(highk[:, :, None], (blocks, ROPE, 128))
    return [np.ascontiguousarray(t, dtype=np.float32) for t in (lowq, highq, lowk, highk)]


def dot(a, b):
    return lax.dot_general(a, b, (((1,), (0,)), ((), ())), preferred_element_type=F32)


def dot_nt(a, b):
    return lax.dot_general(a, b, (((1,), (1,)), ((), ())), preferred_element_type=F32)


def prepare_head(us, h, wq_ref, wkt_ref, wv_ref):
    keys = []
    for x in range(4):
        for c in range(2):
            d = 2 * x + c
            unit = us[c, h, x]
            rows = slice(d * 64, d * 64 + 64)
            wq_ref[h, rows, 0:NOPE] = unit[0:64]
            wq_ref[h, d * 64 : d * 64 + 32, NOPE:QK] = unit[64:96, 0:ROPE]
            wq_ref[h, d * 64 + 32 : d * 64 + 64, NOPE:QK] = unit[64:96, ROPE:128]
            keys.append(unit[96:128])
            wv_ref[h // 2, d * 32 : d * 32 + 32, pl.ds(pl.multiple_of(h % 2 * VD, VD), VD)] = unit[128:160]
    wkt_ref[h] = jnp.concatenate(keys, axis=0).T


def make_queries(latq, block, wq_ref, qgain, lowq_ref, highq_ref, q_ref, which):
    ch, sh = highq_ref[block, 0, 0:1], highq_ref[block, 1, 0:1]
    cl, sl = lowq_ref[0], lowq_ref[1]
    cosine = ch * cl - sh * sl
    sine = sh * cl + ch * sl
    lane = lax.broadcasted_iota(jnp.int32, (ROWS, 128), 1)
    sine_a = jnp.where(lane < ROPE // 2, -sine, 0.0)
    sine_b = jnp.where(lane < ROPE // 2, 0.0, sine)

    for h in range(LOCAL):
        q = dot(latq, wq_ref[h])
        scale = lax.rsqrt(jnp.sum(q * q, axis=1, keepdims=True) * (1.0 / QK) + EPS)
        n = q * scale * qgain
        t = n[:, NOPE:256]
        turned = (
            t * cosine
            + pltpu.roll(t, 128 - ROPE // 2, 1) * sine_a
            + pltpu.roll(t, ROPE // 2, 1) * sine_b
        )
        q_ref[which, h, :, 0:NOPE] = n[:, 0:NOPE].astype(BF)
        q_ref[which, h, :, NOPE:256] = turned.astype(BF)


def expand(unit, block, wkt_ref, wv_ref, gk_ref, gr_ref, lowk_ref, highk_ref, place):
    kv = unit[0:256, :]
    rope = unit[256:320, :].astype(F32)
    half = ROPE // 2
    ch = jnp.concatenate([highk_ref[block, 0:half]] * 2, axis=1)
    sh = jnp.concatenate([highk_ref[block, half:ROPE]] * 2, axis=1)
    cl, sl = lowk_ref[0:half], lowk_ref[half:ROPE]
    cosine = ch * cl - sh * sl
    sine = sh * cl + ch * sl
    rope_sq = jnp.sum(rope * rope, axis=0, keepdims=True)
    x = rope * gr_ref[...]
    a, b = x[0:half], x[half:ROPE]
    turned = jnp.concatenate([a * cosine - b * sine, b * cosine + a * sine], axis=0)
    keys = dot_nt(wkt_ref[...].reshape(LOCAL * NOPE, KR), kv)
    for h in range(LOCAL):
        k = keys[h * NOPE : (h + 1) * NOPE]
        scale = lax.rsqrt((jnp.sum(k * k, axis=0, keepdims=True) + rope_sq) * (1.0 / QK) + EPS)
        kt, _ = place(h)
        kt[0:NOPE] = (k * scale * gk_ref[...]).astype(BF)
        kt[NOPE:QK] = (turned * scale).astype(BF)
    for h in range(0, LOCAL, 2):
        v = dot(kv, wv_ref[h // 2]).astype(BF)
        place(h)[1][:, 0:VD] = v[:, 0:VD]
        place(h + 1)[1][:, 0:VD] = v[:, VD : 2 * VD]


def attend(diagonal, q_ref, place, m_ref, acc_ref, which):
    for h in range(LOCAL):
        kt, v = place(h)
        s = dot(q_ref[which, h], kt[...])
        if diagonal:
            row = lax.broadcasted_iota(jnp.int32, (ROWS, ROWS), 0)
            col = lax.broadcasted_iota(jnp.int32, (ROWS, ROWS), 1)
            s = jnp.where(col <= row, s, NEG_BIG)
        old = m_ref[which, h]
        new = jnp.maximum(old, jnp.max(s, axis=1, keepdims=True))
        fade = jnp.exp2((old - new) * SOFT)
        p = jnp.exp2((s - jnp.concatenate([new, new], 1)) * SOFT).astype(BF)
        m_ref[which, h] = new
        acc_ref[which, h] = acc_ref[which, h] * jnp.concatenate([fade, fade], 1) + dot(
            p, v[...]
        )


def attend_pair(q_ref, place0, place1, m_ref, acc_ref, which, heads):
    def score(h):
        q = q_ref[which, h]
        return dot(q, place0(h)[0][...]), dot(q, place1(h)[0][...])

    s0, s1 = score(heads[0])
    for h in heads:
        ahead = score(h + 1) if h + 1 in heads else None
        old = m_ref[which, h]
        new = jnp.maximum(old, jnp.max(jnp.maximum(s0, s1), axis=1, keepdims=True))
        fade = jnp.exp2((old - new) * SOFT)
        wide = jnp.concatenate([new, new], 1)
        p0 = jnp.exp2((s0 - wide) * SOFT).astype(BF)
        p1 = jnp.exp2((s1 - wide) * SOFT).astype(BF)
        m_ref[which, h] = new
        acc_ref[which, h] = acc_ref[which, h] * jnp.concatenate([fade, fade], 1) + (
            dot(p0, place0(h)[1][...]) + dot(p1, place1(h)[1][...])
        )
        if ahead is not None:
            s0, s1 = ahead


def close_heads(acc_ref, which, att_ref, first, heads=range(LOCAL)):
    for h in heads:
        att_ref[first + h] = (
            acc_ref[which, h, :, 0:VD] / acc_ref[which, h, :, VD : 2 * VD]
        ).astype(BF)


def finish(att_ref, mixed_ref, ogain_ref, wo_ref, out_ref):
    total = jnp.zeros((ROWS, VD), F32)
    for h in range(HEADS):
        at = att_ref[h].astype(F32)
        total = total + at * at
    scale = lax.rsqrt(jnp.sum(total, axis=1, keepdims=True) * (1.0 / (HEADS * VD)) + EPS)
    for h in range(HEADS):
        cols = slice(h * VD, (h + 1) * VD)
        mixed_ref[:, cols] = (att_ref[h].astype(F32) * scale * ogain_ref[:, cols]).astype(BF)

    def one(j, _):
        cols = pl.ds(pl.multiple_of(j * 512, 512), 512)
        w = wo_ref[:, :, :, :, :, cols].reshape(HEADS * VD, 512)
        out_ref[:, cols] = dot(mixed_ref[...], w).astype(BF)
        return 0

    lax.fori_loop(0, D // 512, one, 0)


def rms_rows(values, scaling):
    return values * lax.rsqrt(jnp.mean(values * values, axis=-1, keepdims=True) + EPS) * scaling


SLOTS = 128
SPLIT = 4


def kernel(
    tok_in, ing_ref, wqd_in, wld_in, wrt_in, qlg_ref, klg_ref, wqu_in, wku_in, wvu_in,
    qg_ref, kg_ref, ogain_ref, wo_in, lowq_in, highq_in, lowk_in, highk_in,
    out_ref,
    wd, us, wo, kvb, lq, normed, sums, wq_ref, wkt_ref, wv_ref, q_ref, kt_ref, v_ref, kt_keep, v_keep,
    m_ref, acc_ref, att_ref, mixed_ref, qgain_ref, gk_ref, gr_ref,
    tok_ref, wrt_ref, wqu_ref, lowq_ref, highq_ref, lowk_ref, highk_ref, lsem, ssem, rsem,
):
    sp, dp = lax.axis_index("sp"), lax.axis_index("dp")
    z, y = sp // 4, sp % 4
    x, c = dp // 2, dp % 2
    xl, xr, xo = (x + 3) % 4, (x + 1) % 4, (x + 2) % 4
    yl, yr, yo = (y + 3) % 4, (y + 1) % 4, (y + 2) % 4
    zl, zr, zo = (z + 3) % 4, (z + 1) % 4, (z + 2) % 4
    co = 1 - c
    zb = z % 2
    zpair = z + 1 - 2 * zb
    zmate = 3 - z

    def dev(xx=x, yy=y, zz=z, cc=c):
        return {"sp": zz * 4 + yy, "dp": xx * 2 + cc}

    X_R, X_L, Y_R, Y_L, Z_R, Z_L, CORE = (
        dev(xx=xr), dev(xx=xl), dev(yy=yr), dev(yy=yl), dev(zz=zr), dev(zz=zl), dev(cc=co)
    )
    zn, zm = zpair, (z + 3 + 2 * zb) % 4
    Z_N, Z_M = dev(zz=zn), dev(zz=zm)
    names, sent = {}, []

    def number(name):
        return names.setdefault(name, len(names))

    def push(name, view, to, dst=None):
        i = number(name)
        again = view if callable(view) else functools.partial(lambda v: v, view)
        view = again()
        pltpu.make_async_remote_copy(
            src_ref=view, dst_ref=view if dst is None else dst, send_sem=ssem.at[i],
            recv_sem=rsem.at[i], device_id=to, device_id_type=pl.DeviceIdType.MESH,
        ).start()
        sent.append((i, again))

    def got(name, view):
        pltpu.make_async_copy(view, view, rsem.at[number(name)]).wait()

    barrier = pltpu.get_barrier_semaphore()
    X_O, Y_O = dev(xx=xo), dev(yy=yo)
    for to in (X_R, X_L, X_O, Y_R, Y_L, Y_O, Z_R, Z_L, CORE):
        pl.semaphore_signal(barrier, 1, device_id=to, device_id_type=pl.DeviceIdType.MESH)

    hl = zb * 4 + y
    loads = [
        pltpu.make_async_copy(src, dst, lsem.at[i])
        for i, (src, dst) in enumerate((
            (wqu_in, wqu_ref), (wku_in, us.at[c, hl, x, 96:128]),
            (wvu_in, us.at[c, hl, x, 128:160]), (wo_in, wo.at[z, y, x, c]),
            (wqd_in, wd.at[dp, :, 0:QR]), (wld_in, wd.at[dp, :, QR : QR + KR]),
            (tok_in, tok_ref), (wrt_in, wrt_ref), (lowq_in, lowq_ref), (highq_in, highq_ref),
            (lowk_in, lowk_ref), (highk_in, highk_ref),
        ))
    ]
    for load in loads:
        load.start()
    loads[0].wait()
    us[c, hl, x, 0:64] = wqu_ref[:, 0:NOPE]
    us[c, hl, x, 64:96] = jnp.concatenate(
        [wqu_ref[0:32, NOPE:QK], wqu_ref[32:64, NOPE:QK]], axis=1
    )
    for load in loads[1:4]:
        load.wait()
    pl.semaphore_wait(barrier, 9)

    uown = us.at[c, hl, x]
    push("u_r", uown, X_R)
    push("u_l", uown, X_L)
    push("u_o", uown, X_O)
    wown = wo.at[z, y, x, c]
    push("w_yr", wown, Y_R)
    push("w_yl", wown, Y_L)
    push("w_yo", wown, Y_O)
    loads[4].wait()
    loads[5].wait()
    down = wd.at[dp]
    push("d_ra", wd.at[dp, 0:128], X_R)
    push("d_la", wd.at[dp, 128:256], X_L)
    push("d_rb", wd.at[dp, 128:256], X_R)
    push("d_lb", wd.at[dp, 0:128], X_L)
    push("d_c", down, CORE)

    for load in loads[6:]:
        load.wait()
    for r in range(0, ROWS, 64):
        rows = slice(r, r + 64)
        n = rms_rows(tok_ref[rows].astype(F32), ing_ref[...]).astype(BF)
        for k in range(8):
            normed[k, rows] = n[:, k * 256 : (k + 1) * 256]

    qgain_ref[:, 0:NOPE] = qg_ref[:, 0:NOPE]
    qgain_ref[:, NOPE:256] = jnp.concatenate(
        [qg_ref[:, NOPE:QK], jnp.zeros((1, 256 - QK), F32)], axis=1
    )
    kg = jnp.concatenate([kg_ref[...], jnp.zeros((1, 256 - QK), F32)], axis=1)
    column = jnp.broadcast_to(kg[:, 0:NOPE], (NOPE, NOPE)).T
    gk_ref[...] = jnp.concatenate([column, column], axis=1)
    column = jnp.broadcast_to(kg[:, NOPE:256], (NOPE, NOPE)).T[0:ROPE]
    gr_ref[...] = jnp.concatenate([column, column], axis=1)

    got("u_r", us.at[c, hl, xl])
    got("u_l", us.at[c, hl, xr])
    got("u_o", us.at[c, hl, xo])
    block0 = us.at[c, hl]
    push("u_z", block0, dev(zz=zpair))
    push("u_y0r", block0, Y_R)
    push("u_y0l", block0, Y_L)
    push("u_c0", block0, CORE)
    got("w_yr", wo.at[z, yl, x, c])
    got("w_yl", wo.at[z, yr, x, c])
    got("w_yo", wo.at[z, yo, x, c])
    push("w_zr", wo.at[z, :, x, c], Z_R)
    push("w_zl", wo.at[z, :, x, c], Z_L)

    def add(d, first=False):
        part = dot(normed[d], wd[d])
        if first:
            sums[...] = part
        else:
            sums[...] += part

    add(dp, True)
    got("d_c", wd.at[2 * x + co])
    add(2 * x + co)
    m_ref[...] = jnp.full(m_ref.shape, NEG_BIG, F32)
    acc_ref[...] = jnp.zeros(acc_ref.shape, F32)
    wq_ref[:, :, QK:256] = jnp.zeros((LOCAL, QR, 256 - QK), BF)
    kt_ref[:, :, QK:256, :] = jnp.zeros((2, SPLIT, 256 - QK, 256), BF)
    v_ref[:, :, :, VD:256] = jnp.ones((2, SPLIT, ROWS, 256 - VD), BF)

    def blank(i, _):
        kt_keep[i, :, QK:256, :] = jnp.zeros((LOCAL - SPLIT, 256 - QK, 256), BF)
        v_keep[i, :, :, VD:256] = jnp.ones((LOCAL - SPLIT, ROWS, 256 - VD), BF)
        return 0

    lax.fori_loop(0, 16, blank, 0)
    rope_t = jnp.zeros((ROPE, ROWS), F32)
    for k in range(8):
        rope_t = rope_t + dot_nt(wrt_ref[:, k * 256 : (k + 1) * 256], normed[k])
    kvb[y, z, 256:320] = rope_t.astype(BF)
    base0, base1 = zb * 4, 4 - zb * 4
    block1 = us.at[c, base1 + y]

    def ring_y(j, base):
        got(f"u_y{j}r", us.at[c, base + yl])
        push(f"u_y{j}or", us.at[c, base + yl, 0:2], Y_R)
        push(f"u_c{j}l", us.at[c, base + yl], CORE)
        got(f"u_y{j}l", us.at[c, base + yr])
        push(f"u_y{j}ol", us.at[c, base + yr, 2:4], Y_L)
        push(f"u_c{j}r", us.at[c, base + yr], CORE)

    got("d_ra", wd.at[2 * xl + c, 0:128])
    push("d_or", wd.at[2 * xl + c, 0:128], X_R)
    got("d_la", wd.at[2 * xr + c, 128:256])
    push("d_ol", wd.at[2 * xr + c, 128:256], X_L)
    got("u_z", us.at[c, base1 + y])
    push("u_y1r", block1, Y_R)
    push("u_y1l", block1, Y_L)
    push("u_c1", block1, CORE)
    ring_y(0, base0)
    got("d_rb", wd.at[2 * xl + c, 128:256])
    push("d_cl", wd.at[2 * xl + c], CORE)
    got("d_lb", wd.at[2 * xr + c, 0:128])
    push("d_cr", wd.at[2 * xr + c], CORE)
    add(2 * xl + c)
    add(2 * xr + c)
    got("d_cl", wd.at[2 * xl + co])
    add(2 * xl + co)
    got("d_cr", wd.at[2 * xr + co])
    add(2 * xr + co)
    zrow = (z, zl, zr, zo)

    def row(k):
        push(f"w_xr{k}", wo.at[zrow[k], :, x, c], X_R)
        push(f"w_xl{k}", wo.at[zrow[k], :, x, c], X_L)

    row(0)
    got("w_zr", wo.at[zl, :, x, c])
    push("w_ozr", wo.at[zl, 0:2, x, c], Z_R)
    got("w_zl", wo.at[zr, :, x, c])
    push("w_ozl", wo.at[zr, 2:4, x, c], Z_L)
    row(1)
    row(2)
    got("u_c0", us.at[co, base0 + y])
    got("u_c1", us.at[co, base1 + y])
    got("u_c0l", us.at[co, base0 + yl])
    got("u_c0r", us.at[co, base0 + yr])
    for h in (base0 + y, base1 + y, base0 + yl, base0 + yr):
        prepare_head(us, h, wq_ref, wkt_ref, wv_ref)
    ring_y(1, base1)
    got("d_or", wd.at[2 * xo + c, 0:128])
    push("d_coa", wd.at[2 * xo + c, 0:128], CORE)
    got("d_ol", wd.at[2 * xo + c, 128:256])
    push("d_cob", wd.at[2 * xo + c, 128:256], CORE)
    add(2 * xo + c)
    got("d_coa", wd.at[2 * xo + co, 0:128])
    got("d_cob", wd.at[2 * xo + co, 128:256])
    add(2 * xo + co)

    lq[0] = rms_rows(sums[:, 0:QR], qlg_ref[...]).astype(BF)
    push("q", lq.at[0], dev(zz=zmate), lq.at[1])
    kvb[y, z, 0:256] = rms_rows(sums[:, QR : QR + KR], klg_ref[...]).astype(BF)
    own = kvb.at[y, z]
    push("k_yr", own, Y_R)
    push("k_yl", own, Y_L)
    push("k_zn", own, Z_N)
    push("k_zm", own, Z_M)

    for j, base in ((0, base0), (1, base1)):
        got(f"u_y{j}or", us.at[c, base + yo, 0:2])
        got(f"u_y{j}ol", us.at[c, base + yo, 2:4])
        push(f"u_c{j}o", us.at[c, base + yo], CORE)
    got("w_ozr", wo.at[zo, 0:2, x, c])
    got("w_ozl", wo.at[zo, 2:4, x, c])
    row(3)
    got("u_c1l", us.at[co, base1 + yl])
    got("u_c1r", us.at[co, base1 + yr])
    got("u_c0o", us.at[co, base0 + yo])
    got("u_c1o", us.at[co, base1 + yo])
    push("w_c", wo.at[:, :, x, c], CORE)
    for h in (base0 + yo, base1 + yl, base1 + yr, base1 + yo):
        prepare_head(us, h, wq_ref, wkt_ref, wv_ref)
    make_queries(lq[0], sp, wq_ref, qgain_ref[...], lowq_ref, highq_ref, q_ref, 0)
    def k_y():
        got("k_yr", kvb.at[yl, z])
        push("k_oyr", lambda: kvb.at[yl, z, 0:160], Y_R)
        got("k_yl", kvb.at[yr, z])
        push("k_oyl", lambda: kvb.at[yr, z, 160:320], Y_L)

    def k_zn():
        got("k_zn", kvb.at[y, zn])
        push("k_ozm", lambda: kvb.at[y, zn, 0:160], Z_M)
        push("k_ynr", lambda: kvb.at[y, zn], Y_R)
        push("k_ynl", lambda: kvb.at[y, zn], Y_L)

    def k_zm():
        got("k_zm", kvb.at[y, zm])
        push("k_ozn", lambda: kvb.at[y, zm, 160:320], Z_N)
        push("k_ymr", lambda: kvb.at[y, zm], Y_R)
        push("k_yml", lambda: kvb.at[y, zm], Y_L)

    def k_oy():
        got("k_oyr", kvb.at[yo, z, 0:160])
        got("k_oyl", kvb.at[yo, z, 160:320])
        push("k_pzn", lambda: kvb.at[yo, z], Z_N)
        push("k_pzm", lambda: kvb.at[yo, z], Z_M)

    def k_oz():
        got("k_ozm", kvb.at[y, zo, 0:160])
        got("k_ozn", kvb.at[y, zo, 160:320])
        push("k_yor", lambda: kvb.at[y, zo], Y_R)
        push("k_yol", lambda: kvb.at[y, zo], Y_L)

    def k_pz():
        got("k_pzn", kvb.at[yo, zn])
        push("k_pozm", lambda: kvb.at[yo, zn, 0:160], Z_M)
        got("k_pzm", kvb.at[yo, zm])
        push("k_pozn", lambda: kvb.at[yo, zm, 160:320], Z_N)

    def k_yn():
        got("k_ynr", kvb.at[yl, zn])
        got("k_ynl", kvb.at[yr, zn])

    def k_ym():
        got("k_ymr", kvb.at[yl, zm])
        got("k_yml", kvb.at[yr, zm])

    def k_yo():
        got("k_yor", kvb.at[yl, zo])
        got("k_yol", kvb.at[yr, zo])

    def k_poz():
        got("k_pozm", kvb.at[yo, zo, 0:160])
        got("k_pozn", kvb.at[yo, zo, 160:320])

    def queries_mate():
        got("q", lq.at[1])
        make_queries(
            lq[1], zmate * 4 + y, wq_ref, qgain_ref[...], lowq_ref, highq_ref, q_ref, 1
        )

    def wx(k):
        def go():
            r = zrow[k]
            got(f"w_xr{k}", wo.at[r, :, xl, c])
            push(f"w_oxr{k}", lambda: wo.at[r, 0:2, xl, c], X_R)
            push(f"w_cl{k}", lambda: wo.at[r, :, xl, c], CORE)
            got(f"w_xl{k}", wo.at[r, :, xr, c])
            push(f"w_oxl{k}", lambda: wo.at[r, 2:4, xr, c], X_L)
            push(f"w_cr{k}", lambda: wo.at[r, :, xr, c], CORE)

        return go

    def wxo(k):
        r = zrow[k]
        got(f"w_oxr{k}", wo.at[r, 0:2, xo, c])
        got(f"w_oxl{k}", wo.at[r, 2:4, xo, c])
        push(f"w_co{k}", lambda: wo.at[r, :, xo, c], CORE)

    hfirst = (z // 2) * LOCAL
    b_own, b_mate = sp, zmate * 4 + y

    low, high = range(SPLIT), range(SPLIT, LOCAL)

    def send_mate(heads):
        close_heads(acc_ref, 1, att_ref, HEADS, heads)
        push(
            f"att{heads[0]}", lambda: att_ref.at[HEADS + heads[0] : HEADS + heads[-1] + 1],
            dev(zz=zmate), att_ref.at[pl.ds(hfirst + heads[0], SPLIT)],
        )

    def place(slot, step):
        def of(h):
            if h < SPLIT:
                return kt_ref.at[slot, h], v_ref.at[slot, h]
            return kt_keep.at[step, h - SPLIT], v_keep.at[step, h - SPLIT]

        return of

    def pick(test, yes, no):
        return no + test.astype(jnp.int32) * (yes - no)

    def source(step):
        dy = pick(step < 3, step, pick(step < 5, 0, pick(step < 7, step - 4, pick(
            step == 7, 0, pick(step == 8, 3, pick(step < 11, step - 8, pick(
                step < 13, 3, pick(step < 15, step - 12, 3))))))))
        dz = pick(step < 3, 0, pick(step < 5, step - 2, pick(step < 7, 1, pick(
            step == 7, 3, pick(step == 8, 0, pick(step < 11, 2, pick(
                step < 13, step - 10, 3)))))))
        yy = pick(dy == 0, y, pick(dy == 1, yl, pick(dy == 2, yr, yo)))
        zz = pick(dz == 0, z, pick(dz == 1, zn, pick(dz == 2, zm, zo)))
        return yy, zz, zz * 4 + yy

    b_last = jnp.maximum(b_own, b_mate)

    def expand_step(step, slot):
        yy, zz, b = source(step)
        expand(
            kvb[yy, zz], b, wkt_ref, wv_ref, gk_ref, gr_ref, lowk_ref, highk_ref,
            place(slot, step),
        )

    def attend_to(which, slot, step, diagonal=False):
        attend(diagonal, q_ref, place(slot, step), m_ref, acc_ref, which)

    def attend_both(which, first, second, heads):
        attend_pair(
            q_ref, place(0, first), place(1, second), m_ref, acc_ref, which, heads
        )

    def singles(first, second, b0, b1, own0, own1, skip_own, skip_mate):
        def single(j, _):
            which, slot = j // 2, j % 2
            step = pick(slot == 0, first, second)
            b = pick(slot == 0, b0, b1)
            mine = pick(slot == 0, own0.astype(jnp.int32), own1.astype(jnp.int32)) * (1 - skip_own)
            mates = (b < b_mate).astype(jnp.int32) * (1 - skip_mate)

            @pl.when(pick(which == 0, mine, mates) == 1)
            def _():
                attend_to(which, slot, step)

            @pl.when((b == b_mate) & (which == 1))
            def _():
                attend_to(which, slot, step, True)

            return 0

        lax.fori_loop(0, 4, single, 0)

    zero = z - z
    expand_step(zero, 0)
    attend_to(0, 0, zero, True)
    k_y()
    k_zn()
    expand_step(zero + 1, 0)
    expand_step(zero + 2, 1)
    queries_mate()
    mate_both = (source(zero + 1)[2] < b_mate) & (source(zero + 2)[2] < b_mate)

    @pl.when(mate_both)
    def _():
        attend_both(1, zero + 1, zero + 2, low)

    def units(i):
        first = pick(i == 7, 0, 2 * i + 1)
        second = pick(i == 7, 15, 2 * i + 2)
        return first, second, source(first)[2], source(second)[2]

    at_pair = {1: (k_zm, k_oy, wx(0)), 2: (k_yn,), 3: (k_oz, k_pz, wx(1)), 4: (k_ym, wx(2)),
               5: (wx(3),), 6: (k_yo,), 7: (k_poz, lambda: wxo(0), lambda: wxo(1))}
    i_send = pick(z == 3, 6, 8)

    def rest(i, _):
        first, second, b0, b1 = units(i)

        @pl.when((b0 < b_mate) & (b1 < b_mate))
        def _():
            attend_both(1, first, second, high)

        return 0


    def pair(i, _):
        for when, todo in at_pair.items():
            @pl.when(i == when)
            def _(todo=todo):
                for f in todo:
                    f()

        @pl.when(i == i_send)
        def _():
            send_mate(low)
            lax.fori_loop(0, 8, rest, 0)
            send_mate(high)

        @pl.when(i < 8)
        def _():
            pair_work(i)

        return 0

    def pair_work(i):
        first, second, b0, b1 = units(i)
        own0 = (b0 < b_own) & (i > 0) & (first > 0)
        own1 = (b1 < b_own) & (i > 0) & (second != 8)
        own_both = own0 & own1
        mate_both = (b0 < b_mate) & (b1 < b_mate)
        needed = ((b0 <= b_last) | (b1 <= b_last)) & (i > 0)
        mate_first = mate_both & jnp.logical_not(own_both)

        @pl.when(own_both)
        def _():
            expand_step(first, 0)
            expand_step(second, 1)
            attend_both(0, first, second, range(LOCAL))

        @pl.when(mate_first & (i > 0))
        def _():
            expand_step(first, 0)
            expand_step(second, 1)
            attend_both(1, first, second, low)

        @pl.when(jnp.logical_not(own_both | mate_both) & needed)
        def _():
            expand_step(first, 0)
            expand_step(second, 1)

        @pl.when(own_both & mate_both)
        def _():
            attend_both(1, first, second, low)

        @pl.when(jnp.logical_not(own_both & mate_both))
        def _():
            singles(
                first, second, b0, b1, own0, own1, own_both.astype(jnp.int32), mate_both.astype(jnp.int32),
            )

    lax.fori_loop(0, 9, pair, 0)
    for k in (2, 3):
        wxo(k)

    def last(j, _):
        step = pick(j == 2, 8, j + 1)

        @pl.when(source(step)[2] < b_own)
        def _():
            expand_step(step, 0)
            attend_to(0, 0, step)

        return 0

    lax.fori_loop(0, 3, last, 0)
    close_heads(acc_ref, 0, att_ref, hfirst)
    got("w_c", wo.at[:, :, x, co])
    for k in range(4):
        got(f"w_cl{k}", wo.at[zrow[k], :, xl, co])
        got(f"w_cr{k}", wo.at[zrow[k], :, xr, co])
        got(f"w_co{k}", wo.at[zrow[k], :, xo, co])
    for heads in (low, high):
        got(f"att{heads[0]}", att_ref.at[pl.ds(LOCAL - hfirst + heads[0], SPLIT)])
    finish(att_ref, mixed_ref, ogain_ref, wo, out_ref)
    for i, again in sent:
        view = again()
        pltpu.make_async_copy(view, view, ssem.at[i]).wait()
    assert len(names) <= SLOTS


def per_device(
    tokens, in_gain, w_query_down, w_latent_down, w_rope_key, query_latent_gain, latent_gain,
    w_query_up, w_key_up, w_value_up, query_gain, key_gain, out_gain, w_out,
):
    blocks = lax.axis_size("sp")
    tables = [jnp.asarray(t) for t in rope_tables(blocks)]
    vm = pl.BlockSpec(memory_space=pltpu.VMEM)
    hbm = pl.BlockSpec(memory_space=pl.ANY)
    args = (
        tokens.reshape(ROWS, D), in_gain.reshape(1, D), w_query_down, w_latent_down, w_rope_key.T,
        query_latent_gain.reshape(1, QR), latent_gain.reshape(1, KR), w_query_up, w_key_up,
        w_value_up, query_gain.reshape(1, QK), key_gain.reshape(1, QK), out_gain.reshape(1, D), w_out, *tables,
    )
    out = pl.pallas_call(
        kernel,
        out_shape=pltpu.VMEM((ROWS, D), BF),
        in_specs=[hbm if i in (0, 2, 3, 4, 7, 8, 9) or i > 12 else vm for i in range(len(args))],
        out_specs=vm,
        scratch_shapes=[
            pltpu.VMEM((8, 256, QR + KR), BF),
            pltpu.VMEM((2, LOCAL, 4, 160, 128), BF),
            pltpu.VMEM((4, 4, 4, 2, 16, D), BF),
            pltpu.VMEM((4, 4, 320, 256), BF),
            pltpu.VMEM((2, ROWS, QR), BF),
            pltpu.VMEM((8, ROWS, 256), BF),
            pltpu.VMEM((ROWS, QR + KR), F32),
            pltpu.VMEM((LOCAL, QR, 256), BF),
            pltpu.VMEM((LOCAL, NOPE, KR), BF),
            pltpu.VMEM((LOCAL // 2, KR, 2 * VD), BF),
            pltpu.VMEM((2, LOCAL, ROWS, 256), BF),
            pltpu.VMEM((2, SPLIT, 256, 256), BF),
            pltpu.VMEM((2, SPLIT, 256, 256), BF),
            pltpu.VMEM((16, LOCAL - SPLIT, 256, 256), BF),
            pltpu.VMEM((16, LOCAL - SPLIT, 256, 256), BF),
            pltpu.VMEM((2, LOCAL, ROWS, 128), F32),
            pltpu.VMEM((2, LOCAL, ROWS, 256), F32),
            pltpu.VMEM((HEADS + LOCAL, ROWS, VD), BF),
            pltpu.VMEM((ROWS, D), BF),
            pltpu.VMEM((1, 256), F32),
            pltpu.VMEM((NOPE, 256), F32),
            pltpu.VMEM((ROPE, 256), F32),
            pltpu.VMEM((ROWS, D), BF),
            pltpu.VMEM((ROPE, D), BF),
            pltpu.VMEM((64, QK), BF),
        ]
        + [pltpu.VMEM(t.shape, F32) for t in tables]
        + [
            pltpu.SemaphoreType.DMA((12,)),
            pltpu.SemaphoreType.DMA((SLOTS,)),
            pltpu.SemaphoreType.DMA((SLOTS,)),
        ],
        compiler_params=pltpu.CompilerParams(
            vmem_limit_bytes=60 * 1024 * 1024, collective_id=0, has_side_effects=True
        ),
    )(*args)
    return out.reshape(1, ROWS, D)


def solution(mesh):
    in_specs = (
        P("dp", "sp", None), P(), P("dp", None), P("dp", None), P(), P(), P(),
        P("dp", "sp"), P("dp", "sp"), P("dp", "sp"), P(), P(), P(), P(("sp", "dp"), None),
    )
    return jax.shard_map(
        per_device, mesh=mesh, in_specs=in_specs, out_specs=P("dp", "sp", None), check_vma=False
    )
```

```python
import functools

import jax
import jax.numpy as jnp
import numpy as np
from jax import lax
from jax.experimental import pallas as pl
from jax.experimental.pallas import tpu as pltpu
from jax.sharding import PartitionSpec as P

HEADS, NOPE, ROPE, VD, QR, KR, QK = 16, 128, 64, 128, 512, 256, 192
D = 2048
ROWS = 256
EPS = 1e-06
THETA = 10000.0
NEG_BIG = -1e30
BF, F32 = jnp.bfloat16, jnp.float32
SOFT = float(QK**-0.5 * np.log2(np.e))
LOCAL = 8


def rope_tables(blocks):
    half = ROPE // 2
    freq = THETA ** (-np.arange(half) / half)
    low = np.arange(ROWS)[:, None] * freq[None, :]
    high = (np.arange(blocks) * ROWS)[:, None] * freq[None, :]
    pad = np.zeros((ROWS, 128 - ROPE))
    lowq = np.stack([np.concatenate([f(low), f(low), pad], 1) for f in (np.cos, np.sin)])
    hpad = np.zeros((blocks, 128 - ROPE))
    highq = np.stack([np.concatenate([f(high), f(high), hpad], 1) for f in (np.cos, np.sin)], 1)
    highq = np.broadcast_to(highq[:, :, None, :], (blocks, 2, 8, 128))
    lowk = np.concatenate([np.cos(low).T, np.sin(low).T], 0)
    highk = np.concatenate([np.cos(high), np.sin(high)], 1)
    highk = np.broadcast_to(highk[:, :, None], (blocks, ROPE, 128))
    return [np.ascontiguousarray(t, dtype=np.float32) for t in (lowq, highq, lowk, highk)]


def dot(a, b):
    return lax.dot_general(a, b, (((1,), (0,)), ((), ())), preferred_element_type=F32)


def dot_nt(a, b):
    return lax.dot_general(a, b, (((1,), (1,)), ((), ())), preferred_element_type=F32)


def prepare_head(us, h, wq_ref, wkt_ref, wv_ref):
    keys = []
    for x in range(4):
        for c in range(2):
            d = 2 * x + c
            unit = us[c, h, x]
            rows = slice(d * 64, d * 64 + 64)
            wq_ref[h, rows, 0:NOPE] = unit[0:64]
            wq_ref[h, d * 64 : d * 64 + 32, NOPE:QK] = unit[64:96, 0:ROPE]
            wq_ref[h, d * 64 + 32 : d * 64 + 64, NOPE:QK] = unit[64:96, ROPE:128]
            keys.append(unit[96:128])
            wv_ref[h // 2, d * 32 : d * 32 + 32, pl.ds(pl.multiple_of(h % 2 * VD, VD), VD)] = unit[128:160]
    wkt_ref[h] = jnp.concatenate(keys, axis=0).T


def make_queries(latq, block, wq_ref, qgain, lowq_ref, highq_ref, q_ref, which):
    ch, sh = highq_ref[block, 0, 0:1], highq_ref[block, 1, 0:1]
    cl, sl = lowq_ref[0], lowq_ref[1]
    cosine = ch * cl - sh * sl
    sine = sh * cl + ch * sl
    lane = lax.broadcasted_iota(jnp.int32, (ROWS, 128), 1)
    sine_a = jnp.where(lane < ROPE // 2, -sine, 0.0)
    sine_b = jnp.where(lane < ROPE // 2, 0.0, sine)

    for h in range(LOCAL):
        q = dot(latq, wq_ref[h])
        scale = lax.rsqrt(jnp.sum(q * q, axis=1, keepdims=True) * (1.0 / QK) + EPS)
        n = q * scale * qgain
        t = n[:, NOPE:256]
        turned = (
            t * cosine
            + pltpu.roll(t, 128 - ROPE // 2, 1) * sine_a
            + pltpu.roll(t, ROPE // 2, 1) * sine_b
        )
        q_ref[which, h, :, 0:NOPE] = n[:, 0:NOPE].astype(BF)
        q_ref[which, h, :, NOPE:256] = turned.astype(BF)


def expand(unit, block, wkt_ref, wv_ref, gk_ref, gr_ref, lowk_ref, highk_ref, place):
    kv = unit[0:256, :]
    rope = unit[256:320, :].astype(F32)
    half = ROPE // 2
    ch = jnp.concatenate([highk_ref[block, 0:half]] * 2, axis=1)
    sh = jnp.concatenate([highk_ref[block, half:ROPE]] * 2, axis=1)
    cl, sl = lowk_ref[0:half], lowk_ref[half:ROPE]
    cosine = ch * cl - sh * sl
    sine = sh * cl + ch * sl
    rope_sq = jnp.sum(rope * rope, axis=0, keepdims=True)
    x = rope * gr_ref[...]
    a, b = x[0:half], x[half:ROPE]
    turned = jnp.concatenate([a * cosine - b * sine, b * cosine + a * sine], axis=0)
    keys = dot_nt(wkt_ref[...].reshape(LOCAL * NOPE, KR), kv)
    for h in range(LOCAL):
        k = keys[h * NOPE : (h + 1) * NOPE]
        scale = lax.rsqrt((jnp.sum(k * k, axis=0, keepdims=True) + rope_sq) * (1.0 / QK) + EPS)
        kt, _ = place(h)
        kt[0:NOPE] = (k * scale * gk_ref[...]).astype(BF)
        kt[NOPE:QK] = (turned * scale).astype(BF)
    for h in range(0, LOCAL, 2):
        v = dot(kv, wv_ref[h // 2]).astype(BF)
        place(h)[1][:, 0:VD] = v[:, 0:VD]
        place(h + 1)[1][:, 0:VD] = v[:, VD : 2 * VD]


def attend(diagonal, q_ref, place, m_ref, acc_ref, which):
    for h in range(LOCAL):
        kt, v = place(h)
        s = dot(q_ref[which, h], kt[...])
        if diagonal:
            row = lax.broadcasted_iota(jnp.int32, (ROWS, ROWS), 0)
            col = lax.broadcasted_iota(jnp.int32, (ROWS, ROWS), 1)
            s = jnp.where(col <= row, s, NEG_BIG)
        old = m_ref[which, h]
        new = jnp.maximum(old, jnp.max(s, axis=1, keepdims=True))
        fade = jnp.exp2((old - new) * SOFT)
        p = jnp.exp2((s - jnp.concatenate([new, new], 1)) * SOFT).astype(BF)
        m_ref[which, h] = new
        acc_ref[which, h] = acc_ref[which, h] * jnp.concatenate([fade, fade], 1) + dot(
            p, v[...]
        )


def attend_pair(q_ref, place0, place1, m_ref, acc_ref, which, heads):
    def score(h):
        q = q_ref[which, h]
        return dot(q, place0(h)[0][...]), dot(q, place1(h)[0][...])

    s0, s1 = score(heads[0])
    for h in heads:
        ahead = score(h + 1) if h + 1 in heads else None
        old = m_ref[which, h]
        new = jnp.maximum(old, jnp.max(jnp.maximum(s0, s1), axis=1, keepdims=True))
        fade = jnp.exp2((old - new) * SOFT)
        wide = jnp.concatenate([new, new], 1)
        p0 = jnp.exp2((s0 - wide) * SOFT).astype(BF)
        p1 = jnp.exp2((s1 - wide) * SOFT).astype(BF)
        m_ref[which, h] = new
        acc_ref[which, h] = acc_ref[which, h] * jnp.concatenate([fade, fade], 1) + (
            dot(p0, place0(h)[1][...]) + dot(p1, place1(h)[1][...])
        )
        if ahead is not None:
            s0, s1 = ahead


def close_heads(acc_ref, which, att_ref, first, heads=range(LOCAL)):
    for h in heads:
        att_ref[first + h] = (
            acc_ref[which, h, :, 0:VD] / acc_ref[which, h, :, VD : 2 * VD]
        ).astype(BF)


def finish(att_ref, mixed_ref, ogain_ref, wo_ref, out_ref):
    total = jnp.zeros((ROWS, VD), F32)
    for h in range(HEADS):
        at = att_ref[h].astype(F32)
        total = total + at * at
    scale = lax.rsqrt(jnp.sum(total, axis=1, keepdims=True) * (1.0 / (HEADS * VD)) + EPS)
    for h in range(HEADS):
        cols = slice(h * VD, (h + 1) * VD)
        mixed_ref[:, cols] = (att_ref[h].astype(F32) * scale * ogain_ref[:, cols]).astype(BF)

    def one(j, _):
        cols = pl.ds(pl.multiple_of(j * 512, 512), 512)
        w = wo_ref[:, :, :, :, :, cols].reshape(HEADS * VD, 512)
        out_ref[:, cols] = dot(mixed_ref[...], w).astype(BF)
        return 0

    lax.fori_loop(0, D // 512, one, 0)


def rms_rows(values, scaling):
    return values * lax.rsqrt(jnp.mean(values * values, axis=-1, keepdims=True) + EPS) * scaling


SLOTS = 128
SPLIT = 4


def kernel(
    tok_in, ing_ref, wqd_in, wld_in, wrt_in, qlg_ref, klg_ref, wqu_in, wku_in, wvu_in,
    qg_ref, kg_ref, ogain_ref, wo_in, lowq_in, highq_in, lowk_in, highk_in,
    out_ref,
    wd, us, wo, kvb, lq, normed, sums, wq_ref, wkt_ref, wv_ref, q_ref, kt_ref, v_ref, kt_keep, v_keep,
    m_ref, acc_ref, att_ref, mixed_ref, qgain_ref, gk_ref, gr_ref,
    tok_ref, wrt_ref, wqu_ref, lowq_ref, highq_ref, lowk_ref, highk_ref, lsem, ssem, rsem,
):
    sp, dp = lax.axis_index("sp"), lax.axis_index("dp")
    z, y = sp // 4, sp % 4
    x, c = dp // 2, dp % 2
    xl, xr, xo = (x + 3) % 4, (x + 1) % 4, (x + 2) % 4
    yl, yr, yo = (y + 3) % 4, (y + 1) % 4, (y + 2) % 4
    zl, zr, zo = (z + 3) % 4, (z + 1) % 4, (z + 2) % 4
    co = 1 - c
    zb = z % 2
    zpair = z + 1 - 2 * zb
    zmate = 3 - z

    def dev(xx=x, yy=y, zz=z, cc=c):
        return {"sp": zz * 4 + yy, "dp": xx * 2 + cc}

    X_R, X_L, Y_R, Y_L, Z_R, Z_L, CORE = (
        dev(xx=xr), dev(xx=xl), dev(yy=yr), dev(yy=yl), dev(zz=zr), dev(zz=zl), dev(cc=co)
    )
    zn, zm = zpair, (z + 3 + 2 * zb) % 4
    Z_N, Z_M = dev(zz=zn), dev(zz=zm)
    names, sent = {}, []

    def number(name):
        return names.setdefault(name, len(names))

    def push(name, view, to, dst=None):
        i = number(name)
        again = view if callable(view) else functools.partial(lambda v: v, view)
        view = again()
        pltpu.make_async_remote_copy(
            src_ref=view, dst_ref=view if dst is None else dst, send_sem=ssem.at[i],
            recv_sem=rsem.at[i], device_id=to, device_id_type=pl.DeviceIdType.MESH,
        ).start()
        sent.append((i, again))

    def got(name, view):
        pltpu.make_async_copy(view, view, rsem.at[number(name)]).wait()

    barrier = pltpu.get_barrier_semaphore()
    X_O, Y_O = dev(xx=xo), dev(yy=yo)
    for to in (X_R, X_L, X_O, Y_R, Y_L, Y_O, Z_R, Z_L, CORE):
        pl.semaphore_signal(barrier, 1, device_id=to, device_id_type=pl.DeviceIdType.MESH)

    hl = zb * 4 + y
    loads = [
        pltpu.make_async_copy(src, dst, lsem.at[i])
        for i, (src, dst) in enumerate((
            (wqu_in, wqu_ref), (wku_in, us.at[c, hl, x, 96:128]),
            (wvu_in, us.at[c, hl, x, 128:160]), (wo_in, wo.at[z, y, x, c]),
            (wqd_in, wd.at[dp, :, 0:QR]), (wld_in, wd.at[dp, :, QR : QR + KR]),
            (tok_in, tok_ref), (wrt_in, wrt_ref), (lowq_in, lowq_ref), (highq_in, highq_ref),
            (lowk_in, lowk_ref), (highk_in, highk_ref),
        ))
    ]
    for load in loads:
        load.start()
    loads[0].wait()
    us[c, hl, x, 0:64] = wqu_ref[:, 0:NOPE]
    us[c, hl, x, 64:96] = jnp.concatenate(
        [wqu_ref[0:32, NOPE:QK], wqu_ref[32:64, NOPE:QK]], axis=1
    )
    for load in loads[1:4]:
        load.wait()
    pl.semaphore_wait(barrier, 9)

    uown = us.at[c, hl, x]
    push("u_r", uown, X_R)
    push("u_l", uown, X_L)
    push("u_o", uown, X_O)
    wown = wo.at[z, y, x, c]
    push("w_yr", wown, Y_R)
    push("w_yl", wown, Y_L)
    push("w_yo", wown, Y_O)
    loads[4].wait()
    loads[5].wait()
    down = wd.at[dp]
    push("d_ra", wd.at[dp, 0:128], X_R)
    push("d_la", wd.at[dp, 128:256], X_L)
    push("d_rb", wd.at[dp, 128:256], X_R)
    push("d_lb", wd.at[dp, 0:128], X_L)
    push("d_c", down, CORE)

    for load in loads[6:]:
        load.wait()
    for r in range(0, ROWS, 64):
        rows = slice(r, r + 64)
        n = rms_rows(tok_ref[rows].astype(F32), ing_ref[...]).astype(BF)
        for k in range(8):
            normed[k, rows] = n[:, k * 256 : (k + 1) * 256]

    qgain_ref[:, 0:NOPE] = qg_ref[:, 0:NOPE]
    qgain_ref[:, NOPE:256] = jnp.concatenate(
        [qg_ref[:, NOPE:QK], jnp.zeros((1, 256 - QK), F32)], axis=1
    )
    kg = jnp.concatenate([kg_ref[...], jnp.zeros((1, 256 - QK), F32)], axis=1)
    column = jnp.broadcast_to(kg[:, 0:NOPE], (NOPE, NOPE)).T
    gk_ref[...] = jnp.concatenate([column, column], axis=1)
    column = jnp.broadcast_to(kg[:, NOPE:256], (NOPE, NOPE)).T[0:ROPE]
    gr_ref[...] = jnp.concatenate([column, column], axis=1)

    got("u_r", us.at[c, hl, xl])
    got("u_l", us.at[c, hl, xr])
    got("u_o", us.at[c, hl, xo])
    block0 = us.at[c, hl]
    push("u_z", block0, dev(zz=zpair))
    push("u_y0r", block0, Y_R)
    push("u_y0l", block0, Y_L)
    push("u_c0", block0, CORE)
    got("w_yr", wo.at[z, yl, x, c])
    got("w_yl", wo.at[z, yr, x, c])
    got("w_yo", wo.at[z, yo, x, c])
    push("w_zr", wo.at[z, :, x, c], Z_R)
    push("w_zl", wo.at[z, :, x, c], Z_L)

    def add(d, first=False):
        part = dot(normed[d], wd[d])
        if first:
            sums[...] = part
        else:
            sums[...] += part

    add(dp, True)
    got("d_c", wd.at[2 * x + co])
    add(2 * x + co)
    m_ref[...] = jnp.full(m_ref.shape, NEG_BIG, F32)
    acc_ref[...] = jnp.zeros(acc_ref.shape, F32)
    wq_ref[:, :, QK:256] = jnp.zeros((LOCAL, QR, 256 - QK), BF)
    kt_ref[:, :, QK:256, :] = jnp.zeros((2, SPLIT, 256 - QK, 256), BF)
    v_ref[:, :, :, VD:256] = jnp.ones((2, SPLIT, ROWS, 256 - VD), BF)

    def blank(i, _):
        kt_keep[i, :, QK:256, :] = jnp.zeros((LOCAL - SPLIT, 256 - QK, 256), BF)
        v_keep[i, :, :, VD:256] = jnp.ones((LOCAL - SPLIT, ROWS, 256 - VD), BF)
        return 0

    lax.fori_loop(0, 16, blank, 0)
    rope_t = jnp.zeros((ROPE, ROWS), F32)
    for k in range(8):
        rope_t = rope_t + dot_nt(wrt_ref[:, k * 256 : (k + 1) * 256], normed[k])
    kvb[y, z, 256:320] = rope_t.astype(BF)
    base0, base1 = zb * 4, 4 - zb * 4
    block1 = us.at[c, base1 + y]

    def ring_y(j, base):
        got(f"u_y{j}r", us.at[c, base + yl])
        push(f"u_y{j}or", us.at[c, base + yl, 0:2], Y_R)
        push(f"u_c{j}l", us.at[c, base + yl], CORE)
        got(f"u_y{j}l", us.at[c, base + yr])
        push(f"u_y{j}ol", us.at[c, base + yr, 2:4], Y_L)
        push(f"u_c{j}r", us.at[c, base + yr], CORE)

    got("d_ra", wd.at[2 * xl + c, 0:128])
    push("d_or", wd.at[2 * xl + c, 0:128], X_R)
    got("d_la", wd.at[2 * xr + c, 128:256])
    push("d_ol", wd.at[2 * xr + c, 128:256], X_L)
    got("u_z", us.at[c, base1 + y])
    push("u_y1r", block1, Y_R)
    push("u_y1l", block1, Y_L)
    push("u_c1", block1, CORE)
    ring_y(0, base0)
    got("d_rb", wd.at[2 * xl + c, 128:256])
    push("d_cl", wd.at[2 * xl + c], CORE)
    got("d_lb", wd.at[2 * xr + c, 0:128])
    push("d_cr", wd.at[2 * xr + c], CORE)
    add(2 * xl + c)
    add(2 * xr + c)
    got("d_cl", wd.at[2 * xl + co])
    add(2 * xl + co)
    got("d_cr", wd.at[2 * xr + co])
    add(2 * xr + co)
    zrow = (z, zl, zr, zo)

    def row(k):
        push(f"w_xr{k}", wo.at[zrow[k], :, x, c], X_R)
        push(f"w_xl{k}", wo.at[zrow[k], :, x, c], X_L)

    row(0)
    got("w_zr", wo.at[zl, :, x, c])
    push("w_ozr", wo.at[zl, 0:2, x, c], Z_R)
    got("w_zl", wo.at[zr, :, x, c])
    push("w_ozl", wo.at[zr, 2:4, x, c], Z_L)
    row(1)
    row(2)
    got("u_c0", us.at[co, base0 + y])
    got("u_c1", us.at[co, base1 + y])
    got("u_c0l", us.at[co, base0 + yl])
    got("u_c0r", us.at[co, base0 + yr])
    for h in (base0 + y, base1 + y, base0 + yl, base0 + yr):
        prepare_head(us, h, wq_ref, wkt_ref, wv_ref)
    ring_y(1, base1)
    got("d_or", wd.at[2 * xo + c, 0:128])
    push("d_coa", wd.at[2 * xo + c, 0:128], CORE)
    got("d_ol", wd.at[2 * xo + c, 128:256])
    push("d_cob", wd.at[2 * xo + c, 128:256], CORE)
    add(2 * xo + c)
    got("d_coa", wd.at[2 * xo + co, 0:128])
    got("d_cob", wd.at[2 * xo + co, 128:256])
    add(2 * xo + co)

    lq[0] = rms_rows(sums[:, 0:QR], qlg_ref[...]).astype(BF)
    push("q", lq.at[0], dev(zz=zmate), lq.at[1])
    kvb[y, z, 0:256] = rms_rows(sums[:, QR : QR + KR], klg_ref[...]).astype(BF)
    own = kvb.at[y, z]
    push("k_yr", own, Y_R)
    push("k_yl", own, Y_L)
    push("k_zn", own, Z_N)
    push("k_zm", own, Z_M)

    for j, base in ((0, base0), (1, base1)):
        got(f"u_y{j}or", us.at[c, base + yo, 0:2])
        got(f"u_y{j}ol", us.at[c, base + yo, 2:4])
        push(f"u_c{j}o", us.at[c, base + yo], CORE)
    got("w_ozr", wo.at[zo, 0:2, x, c])
    got("w_ozl", wo.at[zo, 2:4, x, c])
    row(3)
    got("u_c1l", us.at[co, base1 + yl])
    got("u_c1r", us.at[co, base1 + yr])
    got("u_c0o", us.at[co, base0 + yo])
    got("u_c1o", us.at[co, base1 + yo])
    push("w_c", wo.at[:, :, x, c], CORE)
    for h in (base0 + yo, base1 + yl, base1 + yr, base1 + yo):
        prepare_head(us, h, wq_ref, wkt_ref, wv_ref)
    make_queries(lq[0], sp, wq_ref, qgain_ref[...], lowq_ref, highq_ref, q_ref, 0)
    def k_y():
        got("k_yr", kvb.at[yl, z])
        push("k_oyr", lambda: kvb.at[yl, z, 0:160], Y_R)
        got("k_yl", kvb.at[yr, z])
        push("k_oyl", lambda: kvb.at[yr, z, 160:320], Y_L)

    def k_zn():
        got("k_zn", kvb.at[y, zn])
        push("k_ozm", lambda: kvb.at[y, zn, 0:160], Z_M)
        push("k_ynr", lambda: kvb.at[y, zn], Y_R)
        push("k_ynl", lambda: kvb.at[y, zn], Y_L)

    def k_zm():
        got("k_zm", kvb.at[y, zm])
        push("k_ozn", lambda: kvb.at[y, zm, 160:320], Z_N)
        push("k_ymr", lambda: kvb.at[y, zm], Y_R)
        push("k_yml", lambda: kvb.at[y, zm], Y_L)

    def k_oy():
        got("k_oyr", kvb.at[yo, z, 0:160])
        got("k_oyl", kvb.at[yo, z, 160:320])
        push("k_pzn", lambda: kvb.at[yo, z], Z_N)
        push("k_pzm", lambda: kvb.at[yo, z], Z_M)

    def k_oz():
        got("k_ozm", kvb.at[y, zo, 0:160])
        got("k_ozn", kvb.at[y, zo, 160:320])
        push("k_yor", lambda: kvb.at[y, zo], Y_R)
        push("k_yol", lambda: kvb.at[y, zo], Y_L)

    def k_pz():
        got("k_pzn", kvb.at[yo, zn])
        push("k_pozm", lambda: kvb.at[yo, zn, 0:160], Z_M)
        got("k_pzm", kvb.at[yo, zm])
        push("k_pozn", lambda: kvb.at[yo, zm, 160:320], Z_N)

    def k_yn():
        got("k_ynr", kvb.at[yl, zn])
        got("k_ynl", kvb.at[yr, zn])

    def k_ym():
        got("k_ymr", kvb.at[yl, zm])
        got("k_yml", kvb.at[yr, zm])

    def k_yo():
        got("k_yor", kvb.at[yl, zo])
        got("k_yol", kvb.at[yr, zo])

    def k_poz():
        got("k_pozm", kvb.at[yo, zo, 0:160])
        got("k_pozn", kvb.at[yo, zo, 160:320])

    def queries_mate():
        got("q", lq.at[1])
        make_queries(
            lq[1], zmate * 4 + y, wq_ref, qgain_ref[...], lowq_ref, highq_ref, q_ref, 1
        )

    def wx(k):
        def go():
            r = zrow[k]
            got(f"w_xr{k}", wo.at[r, :, xl, c])
            push(f"w_oxr{k}", lambda: wo.at[r, 0:2, xl, c], X_R)
            push(f"w_cl{k}", lambda: wo.at[r, :, xl, c], CORE)
            got(f"w_xl{k}", wo.at[r, :, xr, c])
            push(f"w_oxl{k}", lambda: wo.at[r, 2:4, xr, c], X_L)
            push(f"w_cr{k}", lambda: wo.at[r, :, xr, c], CORE)

        return go

    def wxo(k):
        r = zrow[k]
        got(f"w_oxr{k}", wo.at[r, 0:2, xo, c])
        got(f"w_oxl{k}", wo.at[r, 2:4, xo, c])
        push(f"w_co{k}", lambda: wo.at[r, :, xo, c], CORE)

    hfirst = (z // 2) * LOCAL
    b_own, b_mate = sp, zmate * 4 + y

    low, high = range(SPLIT), range(SPLIT, LOCAL)

    def send_mate(heads):
        close_heads(acc_ref, 1, att_ref, HEADS, heads)
        push(
            f"att{heads[0]}", lambda: att_ref.at[HEADS + heads[0] : HEADS + heads[-1] + 1],
            dev(zz=zmate), att_ref.at[pl.ds(hfirst + heads[0], SPLIT)],
        )

    def place(slot, step):
        def of(h):
            if h < SPLIT:
                return kt_ref.at[slot, h], v_ref.at[slot, h]
            return kt_keep.at[step, h - SPLIT], v_keep.at[step, h - SPLIT]

        return of

    def pick(test, yes, no):
        return no + test.astype(jnp.int32) * (yes - no)

    def source(step):
        dy = pick(step < 3, step, pick(step < 5, 0, pick(step < 7, step - 4, pick(
            step == 7, 0, pick(step == 8, 3, pick(step < 11, step - 8, pick(
                step < 13, 3, pick(step < 15, step - 12, 3))))))))
        dz = pick(step < 3, 0, pick(step < 5, step - 2, pick(step < 7, 1, pick(
            step == 7, 3, pick(step == 8, 0, pick(step < 11, 2, pick(
                step < 13, step - 10, 3)))))))
        yy = pick(dy == 0, y, pick(dy == 1, yl, pick(dy == 2, yr, yo)))
        zz = pick(dz == 0, z, pick(dz == 1, zn, pick(dz == 2, zm, zo)))
        return yy, zz, zz * 4 + yy

    b_last = jnp.maximum(b_own, b_mate)

    def expand_step(step, slot):
        yy, zz, b = source(step)
        expand(
            kvb[yy, zz], b, wkt_ref, wv_ref, gk_ref, gr_ref, lowk_ref, highk_ref,
            place(slot, step),
        )

    def attend_to(which, slot, step, diagonal=False):
        attend(diagonal, q_ref, place(slot, step), m_ref, acc_ref, which)

    def attend_both(which, first, second, heads):
        attend_pair(
            q_ref, place(0, first), place(1, second), m_ref, acc_ref, which, heads
        )

    def singles(first, second, b0, b1, own0, own1, skip_own, skip_mate):
        def single(j, _):
            which, slot = j // 2, j % 2
            step = pick(slot == 0, first, second)
            b = pick(slot == 0, b0, b1)
            mine = pick(slot == 0, own0.astype(jnp.int32), own1.astype(jnp.int32)) * (1 - skip_own)
            mates = (b < b_mate).astype(jnp.int32) * (1 - skip_mate)

            @pl.when(pick(which == 0, mine, mates) == 1)
            def _():
                attend_to(which, slot, step)

            @pl.when((b == b_mate) & (which == 1))
            def _():
                attend_to(which, slot, step, True)

            return 0

        lax.fori_loop(0, 4, single, 0)

    zero = z - z
    expand_step(zero, 0)
    attend_to(0, 0, zero, True)
    k_y()
    k_zn()
    expand_step(zero + 1, 0)
    expand_step(zero + 2, 1)
    queries_mate()
    mate_both = (source(zero + 1)[2] < b_mate) & (source(zero + 2)[2] < b_mate)

    @pl.when(mate_both)
    def _():
        attend_both(1, zero + 1, zero + 2, low)

    def units(i):
        first = pick(i == 7, 0, 2 * i + 1)
        second = pick(i == 7, 15, 2 * i + 2)
        return first, second, source(first)[2], source(second)[2]

    at_pair = {1: (k_zm, k_oy, wx(0)), 2: (k_yn,), 3: (k_oz, wx(1)), 4: (k_ym, k_pz, wx(2)),
               5: (wx(3),), 6: (k_yo,), 7: (k_poz, lambda: wxo(0), lambda: wxo(1))}
    i_send = pick(z == 3, 6, 8)

    def rest(i, _):
        first, second, b0, b1 = units(i)

        @pl.when((b0 < b_mate) & (b1 < b_mate))
        def _():
            attend_both(1, first, second, high)

        return 0


    def pair(i, _):
        for when, todo in at_pair.items():
            @pl.when(i == when)
            def _(todo=todo):
                for f in todo:
                    f()

        @pl.when(i == i_send)
        def _():
            send_mate(low)
            lax.fori_loop(0, 8, rest, 0)
            send_mate(high)

        @pl.when(i < 8)
        def _():
            pair_work(i)

        return 0

    def pair_work(i):
        first, second, b0, b1 = units(i)
        now = (i > 0) & jnp.logical_not((z == 2) & (i > 5))
        own0 = (b0 < b_own) & now & (first > 0)
        own1 = (b1 < b_own) & now & (second != 8)
        own_both = own0 & own1
        mate_both = (b0 < b_mate) & (b1 < b_mate)
        needed = ((b0 <= b_last) | (b1 <= b_last)) & (i > 0)
        mate_first = mate_both & jnp.logical_not(own_both)

        @pl.when(own_both)
        def _():
            expand_step(first, 0)
            expand_step(second, 1)
            attend_both(0, first, second, range(LOCAL))

        @pl.when(mate_first & (i > 0))
        def _():
            expand_step(first, 0)
            expand_step(second, 1)
            attend_both(1, first, second, low)

        @pl.when(jnp.logical_not(own_both | mate_both) & needed)
        def _():
            expand_step(first, 0)
            expand_step(second, 1)

        @pl.when(own_both & mate_both)
        def _():
            attend_both(1, first, second, low)

        @pl.when(jnp.logical_not(own_both & mate_both))
        def _():
            singles(
                first, second, b0, b1, own0, own1, own_both.astype(jnp.int32), mate_both.astype(jnp.int32),
            )

    lax.fori_loop(0, 9, pair, 0)
    for k in (2, 3):
        wxo(k)

    def last(j, _):
        step = pick(j == 2, 8, pick(j < 2, j + 1, j + 10))

        @pl.when((source(step)[2] < b_own) & ((j < 3) | (z == 2)))
        def _():
            expand_step(step, 0)
            attend_to(0, 0, step)

        return 0

    lax.fori_loop(0, 6, last, 0)
    close_heads(acc_ref, 0, att_ref, hfirst)
    got("w_c", wo.at[:, :, x, co])
    for k in range(4):
        got(f"w_cl{k}", wo.at[zrow[k], :, xl, co])
        got(f"w_cr{k}", wo.at[zrow[k], :, xr, co])
        got(f"w_co{k}", wo.at[zrow[k], :, xo, co])
    for heads in (low, high):
        got(f"att{heads[0]}", att_ref.at[pl.ds(LOCAL - hfirst + heads[0], SPLIT)])
    finish(att_ref, mixed_ref, ogain_ref, wo, out_ref)
    for i, again in sent:
        view = again()
        pltpu.make_async_copy(view, view, ssem.at[i]).wait()
    assert len(names) <= SLOTS


def per_device(
    tokens, in_gain, w_query_down, w_latent_down, w_rope_key, query_latent_gain, latent_gain,
    w_query_up, w_key_up, w_value_up, query_gain, key_gain, out_gain, w_out,
):
    blocks = lax.axis_size("sp")
    tables = [jnp.asarray(t) for t in rope_tables(blocks)]
    vm = pl.BlockSpec(memory_space=pltpu.VMEM)
    hbm = pl.BlockSpec(memory_space=pl.ANY)
    args = (
        tokens.reshape(ROWS, D), in_gain.reshape(1, D), w_query_down, w_latent_down, w_rope_key.T,
        query_latent_gain.reshape(1, QR), latent_gain.reshape(1, KR), w_query_up, w_key_up,
        w_value_up, query_gain.reshape(1, QK), key_gain.reshape(1, QK), out_gain.reshape(1, D), w_out, *tables,
    )
    out = pl.pallas_call(
        kernel,
        out_shape=pltpu.VMEM((ROWS, D), BF),
        in_specs=[hbm if i in (0, 2, 3, 4, 7, 8, 9) or i > 12 else vm for i in range(len(args))],
        out_specs=vm,
        scratch_shapes=[
            pltpu.VMEM((8, 256, QR + KR), BF),
            pltpu.VMEM((2, LOCAL, 4, 160, 128), BF),
            pltpu.VMEM((4, 4, 4, 2, 16, D), BF),
            pltpu.VMEM((4, 4, 320, 256), BF),
            pltpu.VMEM((2, ROWS, QR), BF),
            pltpu.VMEM((8, ROWS, 256), BF),
            pltpu.VMEM((ROWS, QR + KR), F32),
            pltpu.VMEM((LOCAL, QR, 256), BF),
            pltpu.VMEM((LOCAL, NOPE, KR), BF),
            pltpu.VMEM((LOCAL // 2, KR, 2 * VD), BF),
            pltpu.VMEM((2, LOCAL, ROWS, 256), BF),
            pltpu.VMEM((2, SPLIT, 256, 256), BF),
            pltpu.VMEM((2, SPLIT, 256, 256), BF),
            pltpu.VMEM((16, LOCAL - SPLIT, 256, 256), BF),
            pltpu.VMEM((16, LOCAL - SPLIT, 256, 256), BF),
            pltpu.VMEM((2, LOCAL, ROWS, 128), F32),
            pltpu.VMEM((2, LOCAL, ROWS, 256), F32),
            pltpu.VMEM((HEADS + LOCAL, ROWS, VD), BF),
            pltpu.VMEM((ROWS, D), BF),
            pltpu.VMEM((1, 256), F32),
            pltpu.VMEM((NOPE, 256), F32),
            pltpu.VMEM((ROPE, 256), F32),
            pltpu.VMEM((ROWS, D), BF),
            pltpu.VMEM((ROPE, D), BF),
            pltpu.VMEM((64, QK), BF),
        ]
        + [pltpu.VMEM(t.shape, F32) for t in tables]
        + [
            pltpu.SemaphoreType.DMA((12,)),
            pltpu.SemaphoreType.DMA((SLOTS,)),
            pltpu.SemaphoreType.DMA((SLOTS,)),
        ],
        compiler_params=pltpu.CompilerParams(
            vmem_limit_bytes=60 * 1024 * 1024, collective_id=0, has_side_effects=True
        ),
    )(*args)
    return out.reshape(1, ROWS, D)


def solution(mesh):
    in_specs = (
        P("dp", "sp", None), P(), P("dp", None), P("dp", None), P(), P(), P(),
        P("dp", "sp"), P("dp", "sp"), P("dp", "sp"), P(), P(), P(), P(("sp", "dp"), None),
    )
    return jax.shard_map(
        per_device, mesh=mesh, in_specs=in_specs, out_specs=P("dp", "sp", None), check_vma=False
    )
```

```python
import functools

import jax
import jax.numpy as jnp
import numpy as np
from jax import lax
from jax.experimental import pallas as pl
from jax.experimental.pallas import tpu as pltpu
from jax.sharding import PartitionSpec as P

HEADS, NOPE, ROPE, VD, QR, KR, QK = 16, 128, 64, 128, 512, 256, 192
D = 2048
ROWS = 256
EPS = 1e-06
THETA = 10000.0
NEG_BIG = -1e30
BF, F32 = jnp.bfloat16, jnp.float32
SOFT = float(QK**-0.5 * np.log2(np.e))
LOCAL = 8


def rope_tables(blocks):
    half = ROPE // 2
    freq = THETA ** (-np.arange(half) / half)
    low = np.arange(ROWS)[:, None] * freq[None, :]
    high = (np.arange(blocks) * ROWS)[:, None] * freq[None, :]
    pad = np.zeros((ROWS, 128 - ROPE))
    lowq = np.stack([np.concatenate([f(low), f(low), pad], 1) for f in (np.cos, np.sin)])
    hpad = np.zeros((blocks, 128 - ROPE))
    highq = np.stack([np.concatenate([f(high), f(high), hpad], 1) for f in (np.cos, np.sin)], 1)
    highq = np.broadcast_to(highq[:, :, None, :], (blocks, 2, 8, 128))
    lowk = np.concatenate([np.cos(low).T, np.sin(low).T], 0)
    highk = np.concatenate([np.cos(high), np.sin(high)], 1)
    highk = np.broadcast_to(highk[:, :, None], (blocks, ROPE, 128))
    return [np.ascontiguousarray(t, dtype=np.float32) for t in (lowq, highq, lowk, highk)]


def dot(a, b):
    return lax.dot_general(a, b, (((1,), (0,)), ((), ())), preferred_element_type=F32)


def dot_nt(a, b):
    return lax.dot_general(a, b, (((1,), (1,)), ((), ())), preferred_element_type=F32)


def prepare_head(us, h, wq_ref, wkt_ref, wv_ref):
    keys = []
    for x in range(4):
        for c in range(2):
            d = 2 * x + c
            unit = us[c, h, x]
            rows = slice(d * 64, d * 64 + 64)
            wq_ref[h, rows, 0:NOPE] = unit[0:64]
            wq_ref[h, d * 64 : d * 64 + 32, NOPE:QK] = unit[64:96, 0:ROPE]
            wq_ref[h, d * 64 + 32 : d * 64 + 64, NOPE:QK] = unit[64:96, ROPE:128]
            keys.append(unit[96:128])
            wv_ref[h // 2, d * 32 : d * 32 + 32, pl.ds(pl.multiple_of(h % 2 * VD, VD), VD)] = unit[128:160]
    wkt_ref[h] = jnp.concatenate(keys, axis=0).T


def make_queries(latq, block, wq_ref, qgain, lowq_ref, highq_ref, q_ref, which, heads):
    ch, sh = highq_ref[block, 0, 0:1], highq_ref[block, 1, 0:1]
    cl, sl = lowq_ref[0], lowq_ref[1]
    cosine = ch * cl - sh * sl
    sine = sh * cl + ch * sl
    lane = lax.broadcasted_iota(jnp.int32, (ROWS, 128), 1)
    sine_a = jnp.where(lane < ROPE // 2, -sine, 0.0)
    sine_b = jnp.where(lane < ROPE // 2, 0.0, sine)

    for h in heads:
        q = dot(latq, wq_ref[h])
        scale = lax.rsqrt(jnp.sum(q * q, axis=1, keepdims=True) * (1.0 / QK) + EPS)
        n = q * scale * qgain
        t = n[:, NOPE:256]
        turned = (
            t * cosine
            + pltpu.roll(t, 128 - ROPE // 2, 1) * sine_a
            + pltpu.roll(t, ROPE // 2, 1) * sine_b
        )
        q_ref[which, h, :, 0:NOPE] = n[:, 0:NOPE].astype(BF)
        q_ref[which, h, :, NOPE:256] = turned.astype(BF)


def expand(unit, block, wkt_ref, wv_ref, gk_ref, gr_ref, lowk_ref, highk_ref, place):
    kv = unit[0:256, :]
    rope = unit[256:320, :].astype(F32)
    half = ROPE // 2
    ch = jnp.concatenate([highk_ref[block, 0:half]] * 2, axis=1)
    sh = jnp.concatenate([highk_ref[block, half:ROPE]] * 2, axis=1)
    cl, sl = lowk_ref[0:half], lowk_ref[half:ROPE]
    cosine = ch * cl - sh * sl
    sine = sh * cl + ch * sl
    rope_sq = jnp.sum(rope * rope, axis=0, keepdims=True)
    x = rope * gr_ref[...]
    a, b = x[0:half], x[half:ROPE]
    turned = jnp.concatenate([a * cosine - b * sine, b * cosine + a * sine], axis=0)
    keys = dot_nt(wkt_ref[...].reshape(LOCAL * NOPE, KR), kv)
    for h in range(LOCAL):
        k = keys[h * NOPE : (h + 1) * NOPE]
        scale = lax.rsqrt((jnp.sum(k * k, axis=0, keepdims=True) + rope_sq) * (1.0 / QK) + EPS)
        kt, _ = place(h)
        kt[0:NOPE] = (k * scale * gk_ref[...]).astype(BF)
        kt[NOPE:QK] = (turned * scale).astype(BF)
    for h in range(0, LOCAL, 2):
        v = dot(kv, wv_ref[h // 2]).astype(BF)
        place(h)[1][:, 0:VD] = v[:, 0:VD]
        place(h + 1)[1][:, 0:VD] = v[:, VD : 2 * VD]


def attend(diagonal, q_ref, place, m_ref, acc_ref, which):
    for h in range(LOCAL):
        kt, v = place(h)
        s = dot(q_ref[which, h], kt[...])
        if diagonal:
            row = lax.broadcasted_iota(jnp.int32, (ROWS, ROWS), 0)
            col = lax.broadcasted_iota(jnp.int32, (ROWS, ROWS), 1)
            s = jnp.where(col <= row, s, NEG_BIG)
        old = m_ref[which, h]
        new = jnp.maximum(old, jnp.max(s, axis=1, keepdims=True))
        fade = jnp.exp2((old - new) * SOFT)
        p = jnp.exp2((s - jnp.concatenate([new, new], 1)) * SOFT).astype(BF)
        m_ref[which, h] = new
        acc_ref[which, h] = acc_ref[which, h] * jnp.concatenate([fade, fade], 1) + dot(
            p, v[...]
        )


def attend_pair(q_ref, place0, place1, m_ref, acc_ref, which, heads):
    def score(h):
        q = q_ref[which, h]
        return dot(q, place0(h)[0][...]), dot(q, place1(h)[0][...])

    s0, s1 = score(heads[0])
    for h in heads:
        ahead = score(h + 1) if h + 1 in heads else None
        old = m_ref[which, h]
        new = jnp.maximum(old, jnp.max(jnp.maximum(s0, s1), axis=1, keepdims=True))
        fade = jnp.exp2((old - new) * SOFT)
        wide = jnp.concatenate([new, new], 1)
        p0 = jnp.exp2((s0 - wide) * SOFT).astype(BF)
        p1 = jnp.exp2((s1 - wide) * SOFT).astype(BF)
        m_ref[which, h] = new
        acc_ref[which, h] = acc_ref[which, h] * jnp.concatenate([fade, fade], 1) + (
            dot(p0, place0(h)[1][...]) + dot(p1, place1(h)[1][...])
        )
        if ahead is not None:
            s0, s1 = ahead


def close_heads(acc_ref, which, att_ref, first, heads=range(LOCAL)):
    for h in heads:
        att_ref[first + h] = (
            acc_ref[which, h, :, 0:VD] / acc_ref[which, h, :, VD : 2 * VD]
        ).astype(BF)


def squares(att_ref, first, count):
    total = jnp.zeros((ROWS, VD), F32)
    for h in range(count):
        at = att_ref[first + h].astype(F32)
        total = total + at * at
    return total


def finish(att_ref, total, mixed_ref, ogain_ref, wo_ref, out_ref):
    scale = lax.rsqrt(jnp.sum(total, axis=1, keepdims=True) * (1.0 / (HEADS * VD)) + EPS)
    for h in range(HEADS):
        cols = slice(h * VD, (h + 1) * VD)
        mixed_ref[:, cols] = (att_ref[h].astype(F32) * scale * ogain_ref[:, cols]).astype(BF)

    def one(j, _):
        cols = pl.ds(pl.multiple_of(j * 512, 512), 512)
        w = wo_ref[:, :, :, :, :, cols].reshape(HEADS * VD, 512)
        out_ref[:, cols] = dot(mixed_ref[...], w).astype(BF)
        return 0

    lax.fori_loop(0, D // 512, one, 0)


def rms_rows(values, scaling):
    return values * lax.rsqrt(jnp.mean(values * values, axis=-1, keepdims=True) + EPS) * scaling


SLOTS = 128
SPLIT = 4


def kernel(
    tok_in, ing_ref, wqd_in, wld_in, wrt_in, qlg_ref, klg_ref, wqu_in, wku_in, wvu_in,
    qg_ref, kg_ref, ogain_ref, wo_in, lowq_in, highq_in, lowk_in, highk_in,
    out_ref,
    wd, us, wo, kvb, lq, normed, sums, wq_ref, wkt_ref, wv_ref, q_ref, kt_ref, v_ref, kt_keep, v_keep,
    m_ref, acc_ref, att_ref, mixed_ref, qgain_ref, gk_ref, gr_ref,
    tok_ref, wrt_ref, wqu_ref, lowq_ref, highq_ref, lowk_ref, highk_ref, lsem, ssem, rsem,
):
    sp, dp = lax.axis_index("sp"), lax.axis_index("dp")
    z, y = sp // 4, sp % 4
    x, c = dp // 2, dp % 2
    xl, xr, xo = (x + 3) % 4, (x + 1) % 4, (x + 2) % 4
    yl, yr, yo = (y + 3) % 4, (y + 1) % 4, (y + 2) % 4
    zl, zr, zo = (z + 3) % 4, (z + 1) % 4, (z + 2) % 4
    co = 1 - c
    zb = z % 2
    zpair = z + 1 - 2 * zb
    zmate = 3 - z

    def dev(xx=x, yy=y, zz=z, cc=c):
        return {"sp": zz * 4 + yy, "dp": xx * 2 + cc}

    X_R, X_L, Y_R, Y_L, Z_R, Z_L, CORE = (
        dev(xx=xr), dev(xx=xl), dev(yy=yr), dev(yy=yl), dev(zz=zr), dev(zz=zl), dev(cc=co)
    )
    zn, zm = zpair, (z + 3 + 2 * zb) % 4
    Z_N, Z_M = dev(zz=zn), dev(zz=zm)
    names, sent = {}, []

    def number(name):
        return names.setdefault(name, len(names))

    def push(name, view, to, dst=None):
        i = number(name)
        again = view if callable(view) else functools.partial(lambda v: v, view)
        view = again()
        pltpu.make_async_remote_copy(
            src_ref=view, dst_ref=view if dst is None else dst, send_sem=ssem.at[i],
            recv_sem=rsem.at[i], device_id=to, device_id_type=pl.DeviceIdType.MESH,
        ).start()
        sent.append((i, again))

    def got(name, view):
        pltpu.make_async_copy(view, view, rsem.at[number(name)]).wait()

    barrier = pltpu.get_barrier_semaphore()
    X_O, Y_O = dev(xx=xo), dev(yy=yo)
    for to in (X_R, X_L, X_O, Y_R, Y_L, Y_O, Z_R, Z_L, CORE):
        pl.semaphore_signal(barrier, 1, device_id=to, device_id_type=pl.DeviceIdType.MESH)

    hl = zb * 4 + y
    loads = [
        pltpu.make_async_copy(src, dst, lsem.at[i])
        for i, (src, dst) in enumerate((
            (wqu_in, wqu_ref), (wku_in, us.at[c, hl, x, 96:128]),
            (wvu_in, us.at[c, hl, x, 128:160]), (wo_in, wo.at[z, y, x, c]),
            (wqd_in, wd.at[dp, :, 0:QR]), (wld_in, wd.at[dp, :, QR : QR + KR]),
            (tok_in, tok_ref), (wrt_in, wrt_ref), (lowq_in, lowq_ref), (highq_in, highq_ref),
            (lowk_in, lowk_ref), (highk_in, highk_ref),
        ))
    ]
    for load in loads:
        load.start()
    loads[0].wait()
    us[c, hl, x, 0:64] = wqu_ref[:, 0:NOPE]
    us[c, hl, x, 64:96] = jnp.concatenate(
        [wqu_ref[0:32, NOPE:QK], wqu_ref[32:64, NOPE:QK]], axis=1
    )
    for load in loads[1:4]:
        load.wait()
    pl.semaphore_wait(barrier, 9)

    uown = us.at[c, hl, x]
    push("u_r", uown, X_R)
    push("u_l", uown, X_L)
    push("u_o", uown, X_O)
    wown = wo.at[z, y, x, c]
    push("w_yr", wown, Y_R)
    push("w_yl", wown, Y_L)
    push("w_yo", wown, Y_O)
    loads[4].wait()
    loads[5].wait()
    down = wd.at[dp]
    push("d_ra", wd.at[dp, 0:128], X_R)
    push("d_la", wd.at[dp, 128:256], X_L)
    push("d_rb", wd.at[dp, 128:256], X_R)
    push("d_lb", wd.at[dp, 0:128], X_L)
    push("d_c", down, CORE)

    for load in loads[6:]:
        load.wait()
    for r in range(0, ROWS, 64):
        rows = slice(r, r + 64)
        n = rms_rows(tok_ref[rows].astype(F32), ing_ref[...]).astype(BF)
        for k in range(8):
            normed[k, rows] = n[:, k * 256 : (k + 1) * 256]

    qgain_ref[:, 0:NOPE] = qg_ref[:, 0:NOPE]
    qgain_ref[:, NOPE:256] = jnp.concatenate(
        [qg_ref[:, NOPE:QK], jnp.zeros((1, 256 - QK), F32)], axis=1
    )
    kg = jnp.concatenate([kg_ref[...], jnp.zeros((1, 256 - QK), F32)], axis=1)
    column = jnp.broadcast_to(kg[:, 0:NOPE], (NOPE, NOPE)).T
    gk_ref[...] = jnp.concatenate([column, column], axis=1)
    column = jnp.broadcast_to(kg[:, NOPE:256], (NOPE, NOPE)).T[0:ROPE]
    gr_ref[...] = jnp.concatenate([column, column], axis=1)

    got("u_r", us.at[c, hl, xl])
    got("u_l", us.at[c, hl, xr])
    got("u_o", us.at[c, hl, xo])
    block0 = us.at[c, hl]
    push("u_z", block0, dev(zz=zpair))
    push("u_y0r", block0, Y_R)
    push("u_y0l", block0, Y_L)
    push("u_c0", block0, CORE)
    got("w_yr", wo.at[z, yl, x, c])
    got("w_yl", wo.at[z, yr, x, c])
    got("w_yo", wo.at[z, yo, x, c])
    push("w_zr", wo.at[z, :, x, c], Z_R)
    push("w_zl", wo.at[z, :, x, c], Z_L)

    def add(d, first=False):
        part = dot(normed[d], wd[d])
        if first:
            sums[...] = part
        else:
            sums[...] += part

    add(dp, True)
    got("d_c", wd.at[2 * x + co])
    add(2 * x + co)
    m_ref[...] = jnp.full(m_ref.shape, NEG_BIG, F32)
    acc_ref[...] = jnp.zeros(acc_ref.shape, F32)
    wq_ref[:, :, QK:256] = jnp.zeros((LOCAL, QR, 256 - QK), BF)
    kt_ref[:, :, QK:256, :] = jnp.zeros((2, SPLIT, 256 - QK, 256), BF)
    v_ref[:, :, :, VD:256] = jnp.ones((2, SPLIT, ROWS, 256 - VD), BF)

    def blank(i, _):
        kt_keep[i, :, QK:256, :] = jnp.zeros((LOCAL - SPLIT, 256 - QK, 256), BF)
        v_keep[i, :, :, VD:256] = jnp.ones((LOCAL - SPLIT, ROWS, 256 - VD), BF)
        return 0

    lax.fori_loop(0, 16, blank, 0)
    rope_t = jnp.zeros((ROPE, ROWS), F32)
    for k in range(8):
        rope_t = rope_t + dot_nt(wrt_ref[:, k * 256 : (k + 1) * 256], normed[k])
    kvb[y, z, 256:320] = rope_t.astype(BF)
    base0, base1 = zb * 4, 4 - zb * 4
    block1 = us.at[c, base1 + y]

    def ring_y(j, base):
        got(f"u_y{j}r", us.at[c, base + yl])
        push(f"u_y{j}or", us.at[c, base + yl, 0:2], Y_R)
        push(f"u_c{j}l", us.at[c, base + yl], CORE)
        got(f"u_y{j}l", us.at[c, base + yr])
        push(f"u_y{j}ol", us.at[c, base + yr, 2:4], Y_L)
        push(f"u_c{j}r", us.at[c, base + yr], CORE)

    got("d_ra", wd.at[2 * xl + c, 0:128])
    push("d_or", wd.at[2 * xl + c, 0:128], X_R)
    got("d_la", wd.at[2 * xr + c, 128:256])
    push("d_ol", wd.at[2 * xr + c, 128:256], X_L)
    got("u_z", us.at[c, base1 + y])
    push("u_y1r", block1, Y_R)
    push("u_y1l", block1, Y_L)
    push("u_c1", block1, CORE)
    ring_y(0, base0)
    got("d_rb", wd.at[2 * xl + c, 128:256])
    push("d_cl", wd.at[2 * xl + c], CORE)
    got("d_lb", wd.at[2 * xr + c, 0:128])
    push("d_cr", wd.at[2 * xr + c], CORE)
    add(2 * xl + c)
    add(2 * xr + c)
    got("d_cl", wd.at[2 * xl + co])
    add(2 * xl + co)
    got("d_cr", wd.at[2 * xr + co])
    add(2 * xr + co)
    zrow = (z, zl, zr, zo)

    def row(k):
        push(f"w_xr{k}", wo.at[zrow[k], :, x, c], X_R)
        push(f"w_xl{k}", wo.at[zrow[k], :, x, c], X_L)

    row(0)
    got("w_zr", wo.at[zl, :, x, c])
    push("w_ozr", wo.at[zl, 0:2, x, c], Z_R)
    got("w_zl", wo.at[zr, :, x, c])
    push("w_ozl", wo.at[zr, 2:4, x, c], Z_L)
    row(1)
    row(2)
    got("u_c0", us.at[co, base0 + y])
    got("u_c1", us.at[co, base1 + y])
    got("u_c0l", us.at[co, base0 + yl])
    got("u_c0r", us.at[co, base0 + yr])
    for h in (base0 + y, base1 + y, base0 + yl, base0 + yr):
        prepare_head(us, h, wq_ref, wkt_ref, wv_ref)
    ring_y(1, base1)
    got("d_or", wd.at[2 * xo + c, 0:128])
    push("d_coa", wd.at[2 * xo + c, 0:128], CORE)
    got("d_ol", wd.at[2 * xo + c, 128:256])
    push("d_cob", wd.at[2 * xo + c, 128:256], CORE)
    add(2 * xo + c)
    got("d_coa", wd.at[2 * xo + co, 0:128])
    got("d_cob", wd.at[2 * xo + co, 128:256])
    add(2 * xo + co)

    lq[0] = rms_rows(sums[:, 0:QR], qlg_ref[...]).astype(BF)
    push("q", lq.at[0], dev(zz=zmate), lq.at[1])
    kvb[y, z, 0:256] = rms_rows(sums[:, QR : QR + KR], klg_ref[...]).astype(BF)
    own = kvb.at[y, z]
    push("k_yr", own, Y_R)
    push("k_yl", own, Y_L)
    push("k_zn", own, Z_N)
    push("k_zm", own, Z_M)

    def queries_own(heads):
        make_queries(lq[0], sp, wq_ref, qgain_ref[...], lowq_ref, highq_ref, q_ref, 0, heads)

    queries_own((base0 + y, base1 + y, base0 + yl, base0 + yr))

    for j, base in ((0, base0), (1, base1)):
        got(f"u_y{j}or", us.at[c, base + yo, 0:2])
        got(f"u_y{j}ol", us.at[c, base + yo, 2:4])
        push(f"u_c{j}o", us.at[c, base + yo], CORE)
    got("w_ozr", wo.at[zo, 0:2, x, c])
    got("w_ozl", wo.at[zo, 2:4, x, c])
    row(3)
    got("u_c1l", us.at[co, base1 + yl])
    got("u_c1r", us.at[co, base1 + yr])
    got("u_c0o", us.at[co, base0 + yo])
    got("u_c1o", us.at[co, base1 + yo])
    push("w_c", wo.at[:, :, x, c], CORE)
    for h in (base0 + yo, base1 + yl, base1 + yr, base1 + yo):
        prepare_head(us, h, wq_ref, wkt_ref, wv_ref)
    queries_own((base0 + yo, base1 + yl, base1 + yr, base1 + yo))
    def k_y():
        got("k_yr", kvb.at[yl, z])
        push("k_oyr", lambda: kvb.at[yl, z, 0:160], Y_R)
        got("k_yl", kvb.at[yr, z])
        push("k_oyl", lambda: kvb.at[yr, z, 160:320], Y_L)

    def k_zn():
        got("k_zn", kvb.at[y, zn])
        push("k_ozm", lambda: kvb.at[y, zn, 0:160], Z_M)
        push("k_ynr", lambda: kvb.at[y, zn], Y_R)
        push("k_ynl", lambda: kvb.at[y, zn], Y_L)

    def k_zm():
        got("k_zm", kvb.at[y, zm])
        push("k_ozn", lambda: kvb.at[y, zm, 160:320], Z_N)
        push("k_ymr", lambda: kvb.at[y, zm], Y_R)
        push("k_yml", lambda: kvb.at[y, zm], Y_L)

    def k_oy():
        got("k_oyr", kvb.at[yo, z, 0:160])
        got("k_oyl", kvb.at[yo, z, 160:320])
        push("k_pzn", lambda: kvb.at[yo, z], Z_N)
        push("k_pzm", lambda: kvb.at[yo, z], Z_M)

    def k_oz():
        got("k_ozm", kvb.at[y, zo, 0:160])
        got("k_ozn", kvb.at[y, zo, 160:320])
        push("k_yor", lambda: kvb.at[y, zo], Y_R)
        push("k_yol", lambda: kvb.at[y, zo], Y_L)

    def k_pz():
        got("k_pzn", kvb.at[yo, zn])
        push("k_pozm", lambda: kvb.at[yo, zn, 0:160], Z_M)
        got("k_pzm", kvb.at[yo, zm])
        push("k_pozn", lambda: kvb.at[yo, zm, 160:320], Z_N)

    def k_yn():
        got("k_ynr", kvb.at[yl, zn])
        got("k_ynl", kvb.at[yr, zn])

    def k_ym():
        got("k_ymr", kvb.at[yl, zm])
        got("k_yml", kvb.at[yr, zm])

    def k_yo():
        got("k_yor", kvb.at[yl, zo])
        got("k_yol", kvb.at[yr, zo])

    def k_poz():
        got("k_pozm", kvb.at[yo, zo, 0:160])
        got("k_pozn", kvb.at[yo, zo, 160:320])

    def queries_mate():
        got("q", lq.at[1])
        make_queries(
            lq[1], zmate * 4 + y, wq_ref, qgain_ref[...], lowq_ref, highq_ref, q_ref, 1,
            range(LOCAL),
        )

    def wx(k):
        def go():
            r = zrow[k]
            got(f"w_xr{k}", wo.at[r, :, xl, c])
            push(f"w_oxr{k}", lambda: wo.at[r, 0:2, xl, c], X_R)
            push(f"w_cl{k}", lambda: wo.at[r, :, xl, c], CORE)
            got(f"w_xl{k}", wo.at[r, :, xr, c])
            push(f"w_oxl{k}", lambda: wo.at[r, 2:4, xr, c], X_L)
            push(f"w_cr{k}", lambda: wo.at[r, :, xr, c], CORE)

        return go

    def wxo(k):
        r = zrow[k]
        got(f"w_oxr{k}", wo.at[r, 0:2, xo, c])
        got(f"w_oxl{k}", wo.at[r, 2:4, xo, c])
        push(f"w_co{k}", lambda: wo.at[r, :, xo, c], CORE)

    hfirst = (z // 2) * LOCAL
    b_own, b_mate = sp, zmate * 4 + y

    low, high = range(SPLIT), range(SPLIT, LOCAL)

    def send_mate(heads):
        close_heads(acc_ref, 1, att_ref, HEADS, heads)
        push(
            f"att{heads[0]}", lambda: att_ref.at[HEADS + heads[0] : HEADS + heads[-1] + 1],
            dev(zz=zmate), att_ref.at[pl.ds(hfirst + heads[0], SPLIT)],
        )

    def place(slot, step):
        def of(h):
            if h < SPLIT:
                return kt_ref.at[slot, h], v_ref.at[slot, h]
            return kt_keep.at[step, h - SPLIT], v_keep.at[step, h - SPLIT]

        return of

    def pick(test, yes, no):
        return no + test.astype(jnp.int32) * (yes - no)

    def source(step):
        dy = pick(step < 3, step, pick(step < 5, 0, pick(step < 7, step - 4, pick(
            step == 7, 0, pick(step == 8, 3, pick(step < 11, step - 8, pick(
                step < 13, 3, pick(step < 15, step - 12, 3))))))))
        dz = pick(step < 3, 0, pick(step < 5, step - 2, pick(step < 7, 1, pick(
            step == 7, 3, pick(step == 8, 0, pick(step < 11, 2, pick(
                step < 13, step - 10, 3)))))))
        yy = pick(dy == 0, y, pick(dy == 1, yl, pick(dy == 2, yr, yo)))
        zz = pick(dz == 0, z, pick(dz == 1, zn, pick(dz == 2, zm, zo)))
        return yy, zz, zz * 4 + yy

    b_last = jnp.maximum(b_own, b_mate)

    def expand_step(step, slot):
        yy, zz, b = source(step)
        expand(
            kvb[yy, zz], b, wkt_ref, wv_ref, gk_ref, gr_ref, lowk_ref, highk_ref,
            place(slot, step),
        )

    def attend_to(which, slot, step, diagonal=False):
        attend(diagonal, q_ref, place(slot, step), m_ref, acc_ref, which)

    def attend_both(which, first, second, heads):
        attend_pair(
            q_ref, place(0, first), place(1, second), m_ref, acc_ref, which, heads
        )

    def singles(first, second, b0, b1, own0, own1, skip_own, skip_mate):
        def single(j, _):
            which, slot = j // 2, j % 2
            step = pick(slot == 0, first, second)
            b = pick(slot == 0, b0, b1)
            mine = pick(slot == 0, own0.astype(jnp.int32), own1.astype(jnp.int32)) * (1 - skip_own)
            mates = (b < b_mate).astype(jnp.int32) * (1 - skip_mate)

            @pl.when(pick(which == 0, mine, mates) == 1)
            def _():
                attend_to(which, slot, step)

            @pl.when((b == b_mate) & (which == 1))
            def _():
                attend_to(which, slot, step, True)

            return 0

        lax.fori_loop(0, 4, single, 0)

    zero = z - z
    expand_step(zero, 0)
    attend_to(0, 0, zero, True)
    k_y()
    k_zn()
    expand_step(zero + 1, 0)
    expand_step(zero + 2, 1)
    queries_mate()
    mate_both = (source(zero + 1)[2] < b_mate) & (source(zero + 2)[2] < b_mate)

    @pl.when(mate_both)
    def _():
        attend_both(1, zero + 1, zero + 2, low)

    def units(i):
        first = pick(i == 7, 0, 2 * i + 1)
        second = pick(i == 7, 15, 2 * i + 2)
        return first, second, source(first)[2], source(second)[2]

    at_pair = {1: (k_zm, k_oy, wx(0)), 2: (k_yn,), 3: (k_oz, wx(1)), 4: (k_ym, k_pz, wx(2)),
               5: (wx(3),), 6: (k_yo,), 7: (k_poz, lambda: wxo(0), lambda: wxo(1))}
    i_send = pick(z == 3, 6, 8)

    def rest(i, _):
        first, second, b0, b1 = units(i)

        @pl.when((b0 < b_mate) & (b1 < b_mate))
        def _():
            attend_both(1, first, second, high)

        return 0


    def pair(i, _):
        for when, todo in at_pair.items():
            @pl.when(i == when)
            def _(todo=todo):
                for f in todo:
                    f()

        @pl.when(i == i_send)
        def _():
            send_mate(low)
            lax.fori_loop(0, 8, rest, 0)
            send_mate(high)

        @pl.when(i < 8)
        def _():
            pair_work(i)

        return 0

    def pair_work(i):
        first, second, b0, b1 = units(i)
        now = (i > 0) & jnp.logical_not((z == 2) & (i > 5))
        own0 = (b0 < b_own) & now & (first > 0)
        own1 = (b1 < b_own) & now & (second != 8)
        own_both = own0 & own1
        mate_both = (b0 < b_mate) & (b1 < b_mate)
        needed = ((b0 <= b_last) | (b1 <= b_last)) & (i > 0)
        mate_first = mate_both & jnp.logical_not(own_both)

        @pl.when(own_both)
        def _():
            expand_step(first, 0)
            expand_step(second, 1)
            attend_both(0, first, second, range(LOCAL))

        @pl.when(mate_first & (i > 0))
        def _():
            expand_step(first, 0)
            expand_step(second, 1)
            attend_both(1, first, second, low)

        @pl.when(jnp.logical_not(own_both | mate_both) & needed)
        def _():
            expand_step(first, 0)
            expand_step(second, 1)

        @pl.when(own_both & mate_both)
        def _():
            attend_both(1, first, second, low)

        @pl.when(jnp.logical_not(own_both & mate_both))
        def _():
            singles(
                first, second, b0, b1, own0, own1, own_both.astype(jnp.int32), mate_both.astype(jnp.int32),
            )

    lax.fori_loop(0, 9, pair, 0)
    for k in (2, 3):
        wxo(k)

    def last(j, _):
        step = pick(j == 2, 8, pick(j < 2, j + 1, j + 10))

        @pl.when((source(step)[2] < b_own) & ((j < 3) | (z == 2)))
        def _():
            expand_step(step, 0)
            attend_to(0, 0, step)

        return 0

    lax.fori_loop(0, 6, last, 0)
    close_heads(acc_ref, 0, att_ref, hfirst)
    got("w_c", wo.at[:, :, x, co])
    for k in range(4):
        got(f"w_cl{k}", wo.at[zrow[k], :, xl, co])
        got(f"w_cr{k}", wo.at[zrow[k], :, xr, co])
        got(f"w_co{k}", wo.at[zrow[k], :, xo, co])
    total = squares(att_ref, hfirst, LOCAL)
    for heads in (low, high):
        first = LOCAL - hfirst + heads[0]
        got(f"att{heads[0]}", att_ref.at[pl.ds(first, SPLIT)])
        total = total + squares(att_ref, first, SPLIT)
    finish(att_ref, total, mixed_ref, ogain_ref, wo, out_ref)
    for i, again in sent:
        view = again()
        pltpu.make_async_copy(view, view, ssem.at[i]).wait()
    assert len(names) <= SLOTS


def per_device(
    tokens, in_gain, w_query_down, w_latent_down, w_rope_key, query_latent_gain, latent_gain,
    w_query_up, w_key_up, w_value_up, query_gain, key_gain, out_gain, w_out,
):
    blocks = lax.axis_size("sp")
    tables = [jnp.asarray(t) for t in rope_tables(blocks)]
    vm = pl.BlockSpec(memory_space=pltpu.VMEM)
    hbm = pl.BlockSpec(memory_space=pl.ANY)
    args = (
        tokens.reshape(ROWS, D), in_gain.reshape(1, D), w_query_down, w_latent_down, w_rope_key.T,
        query_latent_gain.reshape(1, QR), latent_gain.reshape(1, KR), w_query_up, w_key_up,
        w_value_up, query_gain.reshape(1, QK), key_gain.reshape(1, QK), out_gain.reshape(1, D), w_out, *tables,
    )
    out = pl.pallas_call(
        kernel,
        out_shape=pltpu.VMEM((ROWS, D), BF),
        in_specs=[hbm if i in (0, 2, 3, 4, 7, 8, 9) or i > 12 else vm for i in range(len(args))],
        out_specs=vm,
        scratch_shapes=[
            pltpu.VMEM((8, 256, QR + KR), BF),
            pltpu.VMEM((2, LOCAL, 4, 160, 128), BF),
            pltpu.VMEM((4, 4, 4, 2, 16, D), BF),
            pltpu.VMEM((4, 4, 320, 256), BF),
            pltpu.VMEM((2, ROWS, QR), BF),
            pltpu.VMEM((8, ROWS, 256), BF),
            pltpu.VMEM((ROWS, QR + KR), F32),
            pltpu.VMEM((LOCAL, QR, 256), BF),
            pltpu.VMEM((LOCAL, NOPE, KR), BF),
            pltpu.VMEM((LOCAL // 2, KR, 2 * VD), BF),
            pltpu.VMEM((2, LOCAL, ROWS, 256), BF),
            pltpu.VMEM((2, SPLIT, 256, 256), BF),
            pltpu.VMEM((2, SPLIT, 256, 256), BF),
            pltpu.VMEM((16, LOCAL - SPLIT, 256, 256), BF),
            pltpu.VMEM((16, LOCAL - SPLIT, 256, 256), BF),
            pltpu.VMEM((2, LOCAL, ROWS, 128), F32),
            pltpu.VMEM((2, LOCAL, ROWS, 256), F32),
            pltpu.VMEM((HEADS + LOCAL, ROWS, VD), BF),
            pltpu.VMEM((ROWS, D), BF),
            pltpu.VMEM((1, 256), F32),
            pltpu.VMEM((NOPE, 256), F32),
            pltpu.VMEM((ROPE, 256), F32),
            pltpu.VMEM((ROWS, D), BF),
            pltpu.VMEM((ROPE, D), BF),
            pltpu.VMEM((64, QK), BF),
        ]
        + [pltpu.VMEM(t.shape, F32) for t in tables]
        + [
            pltpu.SemaphoreType.DMA((12,)),
            pltpu.SemaphoreType.DMA((SLOTS,)),
            pltpu.SemaphoreType.DMA((SLOTS,)),
        ],
        compiler_params=pltpu.CompilerParams(
            vmem_limit_bytes=60 * 1024 * 1024, collective_id=0, has_side_effects=True
        ),
    )(*args)
    return out.reshape(1, ROWS, D)


def solution(mesh):
    in_specs = (
        P("dp", "sp", None), P(), P("dp", None), P("dp", None), P(), P(), P(),
        P("dp", "sp"), P("dp", "sp"), P("dp", "sp"), P(), P(), P(), P(("sp", "dp"), None),
    )
    return jax.shard_map(
        per_device, mesh=mesh, in_specs=in_specs, out_specs=P("dp", "sp", None), check_vma=False
    )
```

```python
import functools

import jax
import jax.numpy as jnp
import numpy as np
from jax import lax
from jax.experimental import pallas as pl
from jax.experimental.pallas import tpu as pltpu
from jax.sharding import PartitionSpec as P

HEADS, NOPE, ROPE, VD, QR, KR, QK = 16, 128, 64, 128, 512, 256, 192
D = 2048
ROWS = 256
EPS = 1e-06
THETA = 10000.0
NEG_BIG = -1e30
BF, F32 = jnp.bfloat16, jnp.float32
SOFT = float(QK**-0.5 * np.log2(np.e))
LOCAL = 8


def rope_tables(blocks):
    half = ROPE // 2
    freq = THETA ** (-np.arange(half) / half)
    low = np.arange(ROWS)[:, None] * freq[None, :]
    high = (np.arange(blocks) * ROWS)[:, None] * freq[None, :]
    pad = np.zeros((ROWS, 128 - ROPE))
    lowq = np.stack([np.concatenate([f(low), f(low), pad], 1) for f in (np.cos, np.sin)])
    hpad = np.zeros((blocks, 128 - ROPE))
    highq = np.stack([np.concatenate([f(high), f(high), hpad], 1) for f in (np.cos, np.sin)], 1)
    highq = np.broadcast_to(highq[:, :, None, :], (blocks, 2, 8, 128))
    lowk = np.concatenate([np.cos(low).T, np.sin(low).T], 0)
    highk = np.concatenate([np.cos(high), np.sin(high)], 1)
    highk = np.broadcast_to(highk[:, :, None], (blocks, ROPE, 128))
    return [np.ascontiguousarray(t, dtype=np.float32) for t in (lowq, highq, lowk, highk)]


def dot(a, b):
    return lax.dot_general(a, b, (((1,), (0,)), ((), ())), preferred_element_type=F32)


def dot_nt(a, b):
    return lax.dot_general(a, b, (((1,), (1,)), ((), ())), preferred_element_type=F32)


def prepare_head(us, h, wq_ref, wkt_ref, wv_ref):
    keys = []
    for x in range(4):
        for c in range(2):
            d = 2 * x + c
            unit = us[c, h, x]
            rows = slice(d * 64, d * 64 + 64)
            wq_ref[h, rows, 0:NOPE] = unit[0:64]
            wq_ref[h, d * 64 : d * 64 + 32, NOPE:QK] = unit[64:96, 0:ROPE]
            wq_ref[h, d * 64 + 32 : d * 64 + 64, NOPE:QK] = unit[64:96, ROPE:128]
            keys.append(unit[96:128])
            wv_ref[h // 2, d * 32 : d * 32 + 32, pl.ds(pl.multiple_of(h % 2 * VD, VD), VD)] = unit[128:160]
    wkt_ref[h] = jnp.concatenate(keys, axis=0).T


def make_queries(latq, block, wq_ref, qgain, lowq_ref, highq_ref, q_ref, which, heads):
    ch, sh = highq_ref[block, 0, 0:1], highq_ref[block, 1, 0:1]
    cl, sl = lowq_ref[0], lowq_ref[1]
    cosine = ch * cl - sh * sl
    sine = sh * cl + ch * sl
    lane = lax.broadcasted_iota(jnp.int32, (ROWS, 128), 1)
    sine_a = jnp.where(lane < ROPE // 2, -sine, 0.0)
    sine_b = jnp.where(lane < ROPE // 2, 0.0, sine)

    for h in heads:
        q = dot(latq, wq_ref[h])
        scale = lax.rsqrt(jnp.sum(q * q, axis=1, keepdims=True) * (1.0 / QK) + EPS)
        n = q * scale * qgain
        t = n[:, NOPE:256]
        turned = (
            t * cosine
            + pltpu.roll(t, 128 - ROPE // 2, 1) * sine_a
            + pltpu.roll(t, ROPE // 2, 1) * sine_b
        )
        q_ref[which, h, :, 0:NOPE] = n[:, 0:NOPE].astype(BF)
        q_ref[which, h, :, NOPE:256] = turned.astype(BF)


def expand(unit, block, wkt_ref, wv_ref, gk_ref, gr_ref, lowk_ref, highk_ref, place, count):
    kv = unit[0:256, :]
    rope = unit[256:320, :].astype(F32)
    half = ROPE // 2
    ch = jnp.concatenate([highk_ref[block, 0:half]] * 2, axis=1)
    sh = jnp.concatenate([highk_ref[block, half:ROPE]] * 2, axis=1)
    cl, sl = lowk_ref[0:half], lowk_ref[half:ROPE]
    cosine = ch * cl - sh * sl
    sine = sh * cl + ch * sl
    rope_sq = jnp.sum(rope * rope, axis=0, keepdims=True)
    x = rope * gr_ref[...]
    a, b = x[0:half], x[half:ROPE]
    turned = jnp.concatenate([a * cosine - b * sine, b * cosine + a * sine], axis=0)
    keys = dot_nt(wkt_ref[0:count].reshape(count * NOPE, KR), kv)
    for h in range(count):
        k = keys[h * NOPE : (h + 1) * NOPE]
        scale = lax.rsqrt((jnp.sum(k * k, axis=0, keepdims=True) + rope_sq) * (1.0 / QK) + EPS)
        kt, _ = place(h)
        kt[0:NOPE] = (k * scale * gk_ref[...]).astype(BF)
        kt[NOPE:QK] = (turned * scale).astype(BF)
    for h in range(0, count, 2):
        v = dot(kv, wv_ref[h // 2]).astype(BF)
        place(h)[1][:, 0:VD] = v[:, 0:VD]
        place(h + 1)[1][:, 0:VD] = v[:, VD : 2 * VD]


def attend(diagonal, q_ref, place, m_ref, acc_ref, which):
    for h in range(LOCAL):
        kt, v = place(h)
        s = dot(q_ref[which, h], kt[...])
        if diagonal:
            row = lax.broadcasted_iota(jnp.int32, (ROWS, ROWS), 0)
            col = lax.broadcasted_iota(jnp.int32, (ROWS, ROWS), 1)
            s = jnp.where(col <= row, s, NEG_BIG)
        old = m_ref[which, h]
        new = jnp.maximum(old, jnp.max(s, axis=1, keepdims=True))
        fade = jnp.exp2((old - new) * SOFT)
        p = jnp.exp2((s - jnp.concatenate([new, new], 1)) * SOFT).astype(BF)
        m_ref[which, h] = new
        acc_ref[which, h] = acc_ref[which, h] * jnp.concatenate([fade, fade], 1) + dot(
            p, v[...]
        )


def attend_pair(q_ref, place0, place1, m_ref, acc_ref, which, heads):
    def score(h):
        q = q_ref[which, h]
        return dot(q, place0(h)[0][...]), dot(q, place1(h)[0][...])

    s0, s1 = score(heads[0])
    for h in heads:
        ahead = score(h + 1) if h + 1 in heads else None
        old = m_ref[which, h]
        new = jnp.maximum(old, jnp.max(jnp.maximum(s0, s1), axis=1, keepdims=True))
        fade = jnp.exp2((old - new) * SOFT)
        wide = jnp.concatenate([new, new], 1)
        p0 = jnp.exp2((s0 - wide) * SOFT).astype(BF)
        p1 = jnp.exp2((s1 - wide) * SOFT).astype(BF)
        m_ref[which, h] = new
        acc_ref[which, h] = acc_ref[which, h] * jnp.concatenate([fade, fade], 1) + (
            dot(p0, place0(h)[1][...]) + dot(p1, place1(h)[1][...])
        )
        if ahead is not None:
            s0, s1 = ahead


def close_heads(acc_ref, which, att_ref, first, heads=range(LOCAL)):
    for h in heads:
        att_ref[first + h] = (
            acc_ref[which, h, :, 0:VD] / acc_ref[which, h, :, VD : 2 * VD]
        ).astype(BF)


def squares(att_ref, first, count):
    total = jnp.zeros((ROWS, VD), F32)
    for h in range(count):
        at = att_ref[first + h].astype(F32)
        total = total + at * at
    return total


def finish(att_ref, total, mixed_ref, ogain_ref, wo_ref, out_ref):
    scale = lax.rsqrt(jnp.sum(total, axis=1, keepdims=True) * (1.0 / (HEADS * VD)) + EPS)
    for h in range(HEADS):
        cols = slice(h * VD, (h + 1) * VD)
        mixed_ref[:, cols] = (att_ref[h].astype(F32) * scale * ogain_ref[:, cols]).astype(BF)

    def one(j, _):
        cols = pl.ds(pl.multiple_of(j * 512, 512), 512)
        w = wo_ref[:, :, :, :, :, cols].reshape(HEADS * VD, 512)
        out_ref[:, cols] = dot(mixed_ref[...], w).astype(BF)
        return 0

    lax.fori_loop(0, D // 512, one, 0)


def rms_rows(values, scaling):
    return values * lax.rsqrt(jnp.mean(values * values, axis=-1, keepdims=True) + EPS) * scaling


SLOTS = 128
SPLIT = 4


def kernel(
    tok_in, ing_ref, wqd_in, wld_in, wrt_in, qlg_ref, klg_ref, wqu_in, wku_in, wvu_in,
    qg_ref, kg_ref, ogain_ref, wo_in, lowq_in, highq_in, lowk_in, highk_in,
    out_ref,
    wd, us, wo, kvb, lq, normed, sums, wq_ref, wkt_ref, wv_ref, q_ref, kt_ref, v_ref, kt_keep, v_keep,
    m_ref, acc_ref, att_ref, mixed_ref, qgain_ref, gk_ref, gr_ref,
    tok_ref, wrt_ref, wqu_ref, lowq_ref, highq_ref, lowk_ref, highk_ref, lsem, ssem, rsem,
):
    sp, dp = lax.axis_index("sp"), lax.axis_index("dp")
    z, y = sp // 4, sp % 4
    x, c = dp // 2, dp % 2
    xl, xr, xo = (x + 3) % 4, (x + 1) % 4, (x + 2) % 4
    yl, yr, yo = (y + 3) % 4, (y + 1) % 4, (y + 2) % 4
    zl, zr, zo = (z + 3) % 4, (z + 1) % 4, (z + 2) % 4
    co = 1 - c
    zb = z % 2
    zpair = z + 1 - 2 * zb
    zmate = 3 - z

    def dev(xx=x, yy=y, zz=z, cc=c):
        return {"sp": zz * 4 + yy, "dp": xx * 2 + cc}

    X_R, X_L, Y_R, Y_L, Z_R, Z_L, CORE = (
        dev(xx=xr), dev(xx=xl), dev(yy=yr), dev(yy=yl), dev(zz=zr), dev(zz=zl), dev(cc=co)
    )
    zn, zm = zpair, (z + 3 + 2 * zb) % 4
    Z_N, Z_M = dev(zz=zn), dev(zz=zm)
    names, sent = {}, []

    def number(name):
        return names.setdefault(name, len(names))

    def push(name, view, to, dst=None):
        i = number(name)
        again = view if callable(view) else functools.partial(lambda v: v, view)
        view = again()
        pltpu.make_async_remote_copy(
            src_ref=view, dst_ref=view if dst is None else dst, send_sem=ssem.at[i],
            recv_sem=rsem.at[i], device_id=to, device_id_type=pl.DeviceIdType.MESH,
        ).start()
        sent.append((i, again))

    def got(name, view):
        pltpu.make_async_copy(view, view, rsem.at[number(name)]).wait()

    barrier = pltpu.get_barrier_semaphore()
    X_O, Y_O = dev(xx=xo), dev(yy=yo)
    for to in (X_R, X_L, X_O, Y_R, Y_L, Y_O, Z_R, Z_L, CORE):
        pl.semaphore_signal(barrier, 1, device_id=to, device_id_type=pl.DeviceIdType.MESH)

    hl = zb * 4 + y
    loads = [
        pltpu.make_async_copy(src, dst, lsem.at[i])
        for i, (src, dst) in enumerate((
            (wqu_in, wqu_ref), (wku_in, us.at[c, hl, x, 96:128]),
            (wvu_in, us.at[c, hl, x, 128:160]), (wo_in, wo.at[z, y, x, c]),
            (wqd_in, wd.at[dp, :, 0:QR]), (wld_in, wd.at[dp, :, QR : QR + KR]),
            (tok_in, tok_ref), (wrt_in, wrt_ref), (lowq_in, lowq_ref), (highq_in, highq_ref),
            (lowk_in, lowk_ref), (highk_in, highk_ref),
        ))
    ]
    for load in loads:
        load.start()
    loads[0].wait()
    us[c, hl, x, 0:64] = wqu_ref[:, 0:NOPE]
    us[c, hl, x, 64:96] = jnp.concatenate(
        [wqu_ref[0:32, NOPE:QK], wqu_ref[32:64, NOPE:QK]], axis=1
    )
    for load in loads[1:4]:
        load.wait()
    pl.semaphore_wait(barrier, 9)

    uown = us.at[c, hl, x]
    push("u_r", uown, X_R)
    push("u_l", uown, X_L)
    push("u_o", uown, X_O)
    wown = wo.at[z, y, x, c]
    push("w_yr", wown, Y_R)
    push("w_yl", wown, Y_L)
    push("w_yo", wown, Y_O)
    loads[4].wait()
    loads[5].wait()
    down = wd.at[dp]
    push("d_ra", wd.at[dp, 0:128], X_R)
    push("d_la", wd.at[dp, 128:256], X_L)
    push("d_rb", wd.at[dp, 128:256], X_R)
    push("d_lb", wd.at[dp, 0:128], X_L)
    push("d_c", down, CORE)

    for load in loads[6:]:
        load.wait()
    for r in range(0, ROWS, 64):
        rows = slice(r, r + 64)
        n = rms_rows(tok_ref[rows].astype(F32), ing_ref[...]).astype(BF)
        for k in range(8):
            normed[k, rows] = n[:, k * 256 : (k + 1) * 256]

    qgain_ref[:, 0:NOPE] = qg_ref[:, 0:NOPE]
    qgain_ref[:, NOPE:256] = jnp.concatenate(
        [qg_ref[:, NOPE:QK], jnp.zeros((1, 256 - QK), F32)], axis=1
    )
    kg = jnp.concatenate([kg_ref[...], jnp.zeros((1, 256 - QK), F32)], axis=1)
    column = jnp.broadcast_to(kg[:, 0:NOPE], (NOPE, NOPE)).T
    gk_ref[...] = jnp.concatenate([column, column], axis=1)
    column = jnp.broadcast_to(kg[:, NOPE:256], (NOPE, NOPE)).T[0:ROPE]
    gr_ref[...] = jnp.concatenate([column, column], axis=1)

    got("u_r", us.at[c, hl, xl])
    got("u_l", us.at[c, hl, xr])
    got("u_o", us.at[c, hl, xo])
    block0 = us.at[c, hl]
    push("u_z", block0, dev(zz=zpair))
    push("u_y0r", block0, Y_R)
    push("u_y0l", block0, Y_L)
    push("u_c0", block0, CORE)
    got("w_yr", wo.at[z, yl, x, c])
    got("w_yl", wo.at[z, yr, x, c])
    got("w_yo", wo.at[z, yo, x, c])
    push("w_zr", wo.at[z, :, x, c], Z_R)
    push("w_zl", wo.at[z, :, x, c], Z_L)

    def add(d, first=False):
        part = dot(normed[d], wd[d])
        if first:
            sums[...] = part
        else:
            sums[...] += part

    add(dp, True)
    got("d_c", wd.at[2 * x + co])
    add(2 * x + co)
    m_ref[...] = jnp.full(m_ref.shape, NEG_BIG, F32)
    acc_ref[...] = jnp.zeros(acc_ref.shape, F32)
    wq_ref[:, :, QK:256] = jnp.zeros((LOCAL, QR, 256 - QK), BF)
    kt_ref[:, :, QK:256, :] = jnp.zeros((2, SPLIT, 256 - QK, 256), BF)
    v_ref[:, :, :, VD:256] = jnp.ones((2, SPLIT, ROWS, 256 - VD), BF)

    def blank(i, _):
        kt_keep[i, :, QK:256, :] = jnp.zeros((LOCAL - SPLIT, 256 - QK, 256), BF)
        v_keep[i, :, :, VD:256] = jnp.ones((LOCAL - SPLIT, ROWS, 256 - VD), BF)
        return 0

    lax.fori_loop(0, 16, blank, 0)
    rope_t = jnp.zeros((ROPE, ROWS), F32)
    for k in range(8):
        rope_t = rope_t + dot_nt(wrt_ref[:, k * 256 : (k + 1) * 256], normed[k])
    kvb[y, z, 256:320] = rope_t.astype(BF)
    base0, base1 = zb * 4, 4 - zb * 4
    block1 = us.at[c, base1 + y]

    def ring_y(j, base):
        got(f"u_y{j}r", us.at[c, base + yl])
        push(f"u_y{j}or", us.at[c, base + yl, 0:2], Y_R)
        push(f"u_c{j}l", us.at[c, base + yl], CORE)
        got(f"u_y{j}l", us.at[c, base + yr])
        push(f"u_y{j}ol", us.at[c, base + yr, 2:4], Y_L)
        push(f"u_c{j}r", us.at[c, base + yr], CORE)

    got("d_ra", wd.at[2 * xl + c, 0:128])
    push("d_or", wd.at[2 * xl + c, 0:128], X_R)
    got("d_la", wd.at[2 * xr + c, 128:256])
    push("d_ol", wd.at[2 * xr + c, 128:256], X_L)
    got("u_z", us.at[c, base1 + y])
    push("u_y1r", block1, Y_R)
    push("u_y1l", block1, Y_L)
    push("u_c1", block1, CORE)
    ring_y(0, base0)
    got("d_rb", wd.at[2 * xl + c, 128:256])
    push("d_cl", wd.at[2 * xl + c], CORE)
    got("d_lb", wd.at[2 * xr + c, 0:128])
    push("d_cr", wd.at[2 * xr + c], CORE)
    add(2 * xl + c)
    add(2 * xr + c)
    got("d_cl", wd.at[2 * xl + co])
    add(2 * xl + co)
    got("d_cr", wd.at[2 * xr + co])
    add(2 * xr + co)
    zrow = (z, zl, zr, zo)

    def row(k):
        push(f"w_xr{k}", wo.at[zrow[k], :, x, c], X_R)
        push(f"w_xl{k}", wo.at[zrow[k], :, x, c], X_L)

    row(0)
    got("w_zr", wo.at[zl, :, x, c])
    push("w_ozr", wo.at[zl, 0:2, x, c], Z_R)
    got("w_zl", wo.at[zr, :, x, c])
    push("w_ozl", wo.at[zr, 2:4, x, c], Z_L)
    row(1)
    row(2)
    got("u_c0", us.at[co, base0 + y])
    got("u_c1", us.at[co, base1 + y])
    got("u_c0l", us.at[co, base0 + yl])
    got("u_c0r", us.at[co, base0 + yr])
    for h in (base0 + y, base1 + y, base0 + yl, base0 + yr):
        prepare_head(us, h, wq_ref, wkt_ref, wv_ref)
    ring_y(1, base1)
    got("d_or", wd.at[2 * xo + c, 0:128])
    push("d_coa", wd.at[2 * xo + c, 0:128], CORE)
    got("d_ol", wd.at[2 * xo + c, 128:256])
    push("d_cob", wd.at[2 * xo + c, 128:256], CORE)
    add(2 * xo + c)
    got("d_coa", wd.at[2 * xo + co, 0:128])
    got("d_cob", wd.at[2 * xo + co, 128:256])
    add(2 * xo + co)

    lq[0] = rms_rows(sums[:, 0:QR], qlg_ref[...]).astype(BF)
    push("q", lq.at[0], dev(zz=zmate), lq.at[1])
    kvb[y, z, 0:256] = rms_rows(sums[:, QR : QR + KR], klg_ref[...]).astype(BF)
    own = kvb.at[y, z]
    push("k_yr", own, Y_R)
    push("k_yl", own, Y_L)
    push("k_zn", own, Z_N)
    push("k_zm", own, Z_M)

    def queries_own(heads):
        make_queries(lq[0], sp, wq_ref, qgain_ref[...], lowq_ref, highq_ref, q_ref, 0, heads)

    queries_own((base0 + y, base1 + y, base0 + yl, base0 + yr))

    for j, base in ((0, base0), (1, base1)):
        got(f"u_y{j}or", us.at[c, base + yo, 0:2])
        got(f"u_y{j}ol", us.at[c, base + yo, 2:4])
        push(f"u_c{j}o", us.at[c, base + yo], CORE)
    got("w_ozr", wo.at[zo, 0:2, x, c])
    got("w_ozl", wo.at[zo, 2:4, x, c])
    row(3)
    got("u_c1l", us.at[co, base1 + yl])
    got("u_c1r", us.at[co, base1 + yr])
    got("u_c0o", us.at[co, base0 + yo])
    got("u_c1o", us.at[co, base1 + yo])
    push("w_c", wo.at[:, :, x, c], CORE)
    for h in (base0 + yo, base1 + yl, base1 + yr, base1 + yo):
        prepare_head(us, h, wq_ref, wkt_ref, wv_ref)
    queries_own((base0 + yo, base1 + yl, base1 + yr, base1 + yo))
    def k_y():
        got("k_yr", kvb.at[yl, z])
        push("k_oyr", lambda: kvb.at[yl, z, 0:160], Y_R)
        got("k_yl", kvb.at[yr, z])
        push("k_oyl", lambda: kvb.at[yr, z, 160:320], Y_L)

    def k_zn():
        got("k_zn", kvb.at[y, zn])
        push("k_ozm", lambda: kvb.at[y, zn, 0:160], Z_M)
        push("k_ynr", lambda: kvb.at[y, zn], Y_R)
        push("k_ynl", lambda: kvb.at[y, zn], Y_L)

    def k_zm():
        got("k_zm", kvb.at[y, zm])
        push("k_ozn", lambda: kvb.at[y, zm, 160:320], Z_N)
        push("k_ymr", lambda: kvb.at[y, zm], Y_R)
        push("k_yml", lambda: kvb.at[y, zm], Y_L)

    def k_oy():
        got("k_oyr", kvb.at[yo, z, 0:160])
        got("k_oyl", kvb.at[yo, z, 160:320])
        push("k_pzn", lambda: kvb.at[yo, z], Z_N)
        push("k_pzm", lambda: kvb.at[yo, z], Z_M)

    def k_oz():
        got("k_ozm", kvb.at[y, zo, 0:160])
        got("k_ozn", kvb.at[y, zo, 160:320])
        push("k_yor", lambda: kvb.at[y, zo], Y_R)
        push("k_yol", lambda: kvb.at[y, zo], Y_L)

    def k_pz():
        got("k_pzn", kvb.at[yo, zn])
        push("k_pozm", lambda: kvb.at[yo, zn, 0:160], Z_M)
        got("k_pzm", kvb.at[yo, zm])
        push("k_pozn", lambda: kvb.at[yo, zm, 160:320], Z_N)

    def k_yn():
        got("k_ynr", kvb.at[yl, zn])
        got("k_ynl", kvb.at[yr, zn])

    def k_ym():
        got("k_ymr", kvb.at[yl, zm])
        got("k_yml", kvb.at[yr, zm])

    def k_yo():
        got("k_yor", kvb.at[yl, zo])
        got("k_yol", kvb.at[yr, zo])

    def k_poz():
        got("k_pozm", kvb.at[yo, zo, 0:160])
        got("k_pozn", kvb.at[yo, zo, 160:320])

    def queries_mate():
        got("q", lq.at[1])
        make_queries(
            lq[1], zmate * 4 + y, wq_ref, qgain_ref[...], lowq_ref, highq_ref, q_ref, 1,
            range(LOCAL),
        )

    def wx(k):
        def go():
            r = zrow[k]
            got(f"w_xr{k}", wo.at[r, :, xl, c])
            push(f"w_oxr{k}", lambda: wo.at[r, 0:2, xl, c], X_R)
            push(f"w_cl{k}", lambda: wo.at[r, :, xl, c], CORE)
            got(f"w_xl{k}", wo.at[r, :, xr, c])
            push(f"w_oxl{k}", lambda: wo.at[r, 2:4, xr, c], X_L)
            push(f"w_cr{k}", lambda: wo.at[r, :, xr, c], CORE)

        return go

    def wxo(k):
        r = zrow[k]
        got(f"w_oxr{k}", wo.at[r, 0:2, xo, c])
        got(f"w_oxl{k}", wo.at[r, 2:4, xo, c])
        push(f"w_co{k}", lambda: wo.at[r, :, xo, c], CORE)

    hfirst = (z // 2) * LOCAL
    b_own, b_mate = sp, zmate * 4 + y

    low, high = range(SPLIT), range(SPLIT, LOCAL)

    def send_mate(heads):
        close_heads(acc_ref, 1, att_ref, HEADS, heads)
        push(
            f"att{heads[0]}", lambda: att_ref.at[HEADS + heads[0] : HEADS + heads[-1] + 1],
            dev(zz=zmate), att_ref.at[pl.ds(hfirst + heads[0], SPLIT)],
        )

    def place(slot, step):
        def of(h):
            if h < SPLIT:
                return kt_ref.at[slot, h], v_ref.at[slot, h]
            return kt_keep.at[step, h - SPLIT], v_keep.at[step, h - SPLIT]

        return of

    def pick(test, yes, no):
        return no + test.astype(jnp.int32) * (yes - no)

    def source(step):
        dy = pick(step < 3, step, pick(step < 5, 0, pick(step < 7, step - 4, pick(
            step == 7, 0, pick(step == 8, 3, pick(step < 11, step - 8, pick(
                step < 13, 3, pick(step < 15, step - 12, 3))))))))
        dz = pick(step < 3, 0, pick(step < 5, step - 2, pick(step < 7, 1, pick(
            step == 7, 3, pick(step == 8, 0, pick(step < 11, 2, pick(
                step < 13, step - 10, 3)))))))
        yy = pick(dy == 0, y, pick(dy == 1, yl, pick(dy == 2, yr, yo)))
        zz = pick(dz == 0, z, pick(dz == 1, zn, pick(dz == 2, zm, zo)))
        return yy, zz, zz * 4 + yy

    b_last = jnp.maximum(b_own, b_mate)

    def expand_step(step, slot, count=LOCAL):
        yy, zz, b = source(step)
        expand(
            kvb[yy, zz], b, wkt_ref, wv_ref, gk_ref, gr_ref, lowk_ref, highk_ref,
            place(slot, step), count,
        )

    def attend_to(which, slot, step, diagonal=False):
        attend(diagonal, q_ref, place(slot, step), m_ref, acc_ref, which)

    def attend_both(which, first, second, heads):
        attend_pair(
            q_ref, place(0, first), place(1, second), m_ref, acc_ref, which, heads
        )

    def singles(first, second, b0, b1, own0, own1, skip_own, skip_mate):
        def single(j, _):
            which, slot = j // 2, j % 2
            step = pick(slot == 0, first, second)
            b = pick(slot == 0, b0, b1)
            mine = pick(slot == 0, own0.astype(jnp.int32), own1.astype(jnp.int32)) * (1 - skip_own)
            mates = (b < b_mate).astype(jnp.int32) * (1 - skip_mate)

            @pl.when(pick(which == 0, mine, mates) == 1)
            def _():
                attend_to(which, slot, step)

            @pl.when((b == b_mate) & (which == 1))
            def _():
                attend_to(which, slot, step, True)

            return 0

        lax.fori_loop(0, 4, single, 0)

    zero = z - z
    expand_step(zero, 0)
    attend_to(0, 0, zero, True)
    k_y()
    k_zn()
    expand_step(zero + 1, 0)
    expand_step(zero + 2, 1)
    queries_mate()
    mate_both = (source(zero + 1)[2] < b_mate) & (source(zero + 2)[2] < b_mate)

    @pl.when(mate_both)
    def _():
        attend_both(1, zero + 1, zero + 2, low)

    def units(i):
        first = pick(i == 7, 0, 2 * i + 1)
        second = pick(i == 7, 15, 2 * i + 2)
        return first, second, source(first)[2], source(second)[2]

    at_pair = {1: (k_zm, k_oy, wx(0)), 2: (k_yn,), 3: (k_oz, wx(1)), 4: (k_ym, k_pz, wx(2)),
               5: (wx(3),), 6: (k_yo,), 7: (k_poz, lambda: wxo(0), lambda: wxo(1))}
    i_send = pick(z == 3, 6, 8)

    def rest(i, _):
        first, second, b0, b1 = units(i)

        @pl.when((b0 < b_mate) & (b1 < b_mate))
        def _():
            attend_both(1, first, second, high)

        return 0


    def pair(i, _):
        for when, todo in at_pair.items():
            @pl.when(i == when)
            def _(todo=todo):
                for f in todo:
                    f()

        @pl.when(i == i_send)
        def _():
            send_mate(low)
            lax.fori_loop(0, 8, rest, 0)
            send_mate(high)

        @pl.when(i < 8)
        def _():
            pair_work(i)

        return 0

    def pair_work(i):
        first, second, b0, b1 = units(i)
        now = (i > 0) & jnp.logical_not((z == 2) & (i > 5))
        own0 = (b0 < b_own) & now & (first > 0)
        own1 = (b1 < b_own) & now & (second != 8)
        own_both = own0 & own1
        mate_both = (b0 < b_mate) & (b1 < b_mate)
        needed = ((b0 <= b_last) | (b1 <= b_last)) & (i > 0)
        mate_first = mate_both & jnp.logical_not(own_both)

        @pl.when(own_both)
        def _():
            expand_step(first, 0)
            expand_step(second, 1)
            attend_both(0, first, second, range(LOCAL))

        @pl.when(mate_first & (i > 0))
        def _():
            expand_step(first, 0)
            expand_step(second, 1)
            attend_both(1, first, second, low)

        @pl.when(jnp.logical_not(own_both | mate_both) & needed)
        def _():
            expand_step(first, 0)
            expand_step(second, 1)

        @pl.when(own_both & mate_both)
        def _():
            attend_both(1, first, second, low)

        @pl.when(jnp.logical_not(own_both & mate_both))
        def _():
            singles(
                first, second, b0, b1, own0, own1, own_both.astype(jnp.int32), mate_both.astype(jnp.int32),
            )

    lax.fori_loop(0, 9, pair, 0)
    for k in (2, 3):
        wxo(k)

    def last(j, _):
        step = pick(j == 2, 8, pick(j < 2, j + 1, j + 10))

        @pl.when((source(step)[2] < b_own) & ((j < 3) | (z == 2)))
        def _():
            expand_step(step, 0, SPLIT)
            attend_to(0, 0, step)

        return 0

    lax.fori_loop(0, 6, last, 0)
    close_heads(acc_ref, 0, att_ref, hfirst)
    got("w_c", wo.at[:, :, x, co])
    for k in range(4):
        got(f"w_cl{k}", wo.at[zrow[k], :, xl, co])
        got(f"w_cr{k}", wo.at[zrow[k], :, xr, co])
        got(f"w_co{k}", wo.at[zrow[k], :, xo, co])
    total = squares(att_ref, hfirst, LOCAL)
    for heads in (low, high):
        first = LOCAL - hfirst + heads[0]
        got(f"att{heads[0]}", att_ref.at[pl.ds(first, SPLIT)])
        total = total + squares(att_ref, first, SPLIT)
    finish(att_ref, total, mixed_ref, ogain_ref, wo, out_ref)
    for i, again in sent:
        view = again()
        pltpu.make_async_copy(view, view, ssem.at[i]).wait()
    assert len(names) <= SLOTS


def per_device(
    tokens, in_gain, w_query_down, w_latent_down, w_rope_key, query_latent_gain, latent_gain,
    w_query_up, w_key_up, w_value_up, query_gain, key_gain, out_gain, w_out,
):
    blocks = lax.axis_size("sp")
    tables = [jnp.asarray(t) for t in rope_tables(blocks)]
    vm = pl.BlockSpec(memory_space=pltpu.VMEM)
    hbm = pl.BlockSpec(memory_space=pl.ANY)
    args = (
        tokens.reshape(ROWS, D), in_gain.reshape(1, D), w_query_down, w_latent_down, w_rope_key.T,
        query_latent_gain.reshape(1, QR), latent_gain.reshape(1, KR), w_query_up, w_key_up,
        w_value_up, query_gain.reshape(1, QK), key_gain.reshape(1, QK), out_gain.reshape(1, D), w_out, *tables,
    )
    out = pl.pallas_call(
        kernel,
        out_shape=pltpu.VMEM((ROWS, D), BF),
        in_specs=[hbm if i in (0, 2, 3, 4, 7, 8, 9) or i > 12 else vm for i in range(len(args))],
        out_specs=vm,
        scratch_shapes=[
            pltpu.VMEM((8, 256, QR + KR), BF),
            pltpu.VMEM((2, LOCAL, 4, 160, 128), BF),
            pltpu.VMEM((4, 4, 4, 2, 16, D), BF),
            pltpu.VMEM((4, 4, 320, 256), BF),
            pltpu.VMEM((2, ROWS, QR), BF),
            pltpu.VMEM((8, ROWS, 256), BF),
            pltpu.VMEM((ROWS, QR + KR), F32),
            pltpu.VMEM((LOCAL, QR, 256), BF),
            pltpu.VMEM((LOCAL, NOPE, KR), BF),
            pltpu.VMEM((LOCAL // 2, KR, 2 * VD), BF),
            pltpu.VMEM((2, LOCAL, ROWS, 256), BF),
            pltpu.VMEM((2, SPLIT, 256, 256), BF),
            pltpu.VMEM((2, SPLIT, 256, 256), BF),
            pltpu.VMEM((16, LOCAL - SPLIT, 256, 256), BF),
            pltpu.VMEM((16, LOCAL - SPLIT, 256, 256), BF),
            pltpu.VMEM((2, LOCAL, ROWS, 128), F32),
            pltpu.VMEM((2, LOCAL, ROWS, 256), F32),
            pltpu.VMEM((HEADS + LOCAL, ROWS, VD), BF),
            pltpu.VMEM((ROWS, D), BF),
            pltpu.VMEM((1, 256), F32),
            pltpu.VMEM((NOPE, 256), F32),
            pltpu.VMEM((ROPE, 256), F32),
            pltpu.VMEM((ROWS, D), BF),
            pltpu.VMEM((ROPE, D), BF),
            pltpu.VMEM((64, QK), BF),
        ]
        + [pltpu.VMEM(t.shape, F32) for t in tables]
        + [
            pltpu.SemaphoreType.DMA((12,)),
            pltpu.SemaphoreType.DMA((SLOTS,)),
            pltpu.SemaphoreType.DMA((SLOTS,)),
        ],
        compiler_params=pltpu.CompilerParams(
            vmem_limit_bytes=60 * 1024 * 1024, collective_id=0, has_side_effects=True
        ),
    )(*args)
    return out.reshape(1, ROWS, D)


def solution(mesh):
    in_specs = (
        P("dp", "sp", None), P(), P("dp", None), P("dp", None), P(), P(), P(),
        P("dp", "sp"), P("dp", "sp"), P("dp", "sp"), P(), P(), P(), P(("sp", "dp"), None),
    )
    return jax.shard_map(
        per_device, mesh=mesh, in_specs=in_specs, out_specs=P("dp", "sp", None), check_vma=False
    )
```
